32 devices in a mesh: ep: 8 (over z, core), tp: 4 (over y, x).
Axes of the slice: x: 2, y: 2, z: 4, core: 2. Of those that a mesh axis runs over, the one named last changes fastest.
Arguments:
- tokens: bfloat16 [384, 2048], P('ep'), may hold values from -6 to 6
- retention_state: float32 [384, 16, 64, 64], P('ep', 'tp'), may hold values from -1.5 to 1.5
- lengths: int32 [384], P('ep'), may hold values from 1024 to 16383
- query_weight: bfloat16 [2048, 1024], P(None, 'tp'), may hold values from -0.125 to 0.125
- key_weight: bfloat16 [2048, 1024], P(None, 'tp'), may hold values from -0.125 to 0.125
- value_weight: bfloat16 [2048, 1024], P(None, 'tp'), may hold values from -0.125 to 0.125
- gate_weight: bfloat16 [2048, 1024], P(None, 'tp'), may hold values from -0.125 to 0.125
- out_weight: bfloat16 [1024, 2048], P(None, 'tp'), may hold values from -0.1875 to 0.1875
- first_gain: float32 [2048], replicated, may hold values from 0.1 to 1.9
- routing: int32 [384, 4], P('ep'), may hold values from 0 to 31, all different within a row; in each aligned block of 48 rows (0 to 47, 48 to 95, ...) at most 18 rows name the same one
- route_weight: float32 [384, 4], P('ep'), may hold values from 0.1 to 1
- expert_gate: bfloat16 [32, 2048, 512], P('ep', None, 'tp'), may hold values from -0.125 to 0.125
- expert_up: bfloat16 [32, 2048, 512], P('ep', None, 'tp'), may hold values from -0.125 to 0.125
- expert_down: bfloat16 [32, 512, 2048], P('ep', None, 'tp'), may hold values from -0.25 to 0.25
- shared_gate: bfloat16 [2048, 512], P(None, 'tp'), may hold values from -0.125 to 0.125
- shared_up: bfloat16 [2048, 512], P(None, 'tp'), may hold values from -0.125 to 0.125
- shared_down: bfloat16 [512, 2048], P(None, 'tp'), may hold values from -0.25 to 0.25
- side_gate: bfloat16 [2048, 256], P('ep', 'tp'), may hold values from -0.125 to 0.125
- side_up: bfloat16 [2048, 256], P('ep', 'tp'), may hold values from -0.125 to 0.125
- side_down: bfloat16 [256, 2048], P(None, 'tp'), may hold values from -0.375 to 0.375
- side_switch: bfloat16 [2048], replicated, may hold values from -0.125 to 0.125
- second_gain: float32 [2048], P('tp'), may hold values from 0.1 to 1.9
Outputs:
- output: bfloat16 [384, 2048], P('ep', 'tp')
- new_state: float32 [384, 16, 64, 64], P('ep', 'tp')
The draws below stay inside these ranges and needn't reach their ends.
Inputs may be any that keep to these rules, and one draw needn't show every extreme that they name: `routing`: each row names 4 different experts. Among the rows of one ep index (aligned blocks of 48 rows) no expert is named by more than 18 rows, a bound that some block reaches.
All inputs are finite; a program needn't handle non-finite values.
Results may differ from the reference program's by a relative error of at most 0.013.
Values may be sent and summed in bfloat16 or wider, within the bound.
A program may use at most 64 MiB of HBM per device.

```python
import math
import jax
import jax.numpy as jnp
import numpy as np
from jax import lax

D = 2048
HEADS = 16
HEAD_SIZE = 64
FE = 512
SHARED_F = 512
DENSE_F = 256
TOPK = 4
SEQ_DEV = 48
BATCH = 384
EXPERTS = 32
CAP = 18
N_EP = 8


def touch_ends(array, own_key, low, largest):
    longest = array.shape.index(max(array.shape))
    spots = []
    for shift in (0, 1):
        where = [jax.random.randint(jax.random.fold_in(own_key, axis), (), 0, length) for axis, length in enumerate(array.shape)]
        where[longest] = (where[longest] + shift) % array.shape[longest]
        spots.append(tuple(where))
    return array.at[spots[0]].set(low).at[spots[1]].set(largest)


def levels(rng, extent, cuts, low, largest):
    level, own = 1.0, jax.random.fold_in(rng, 6)
    for dim, shards_of in cuts:
        steps = jnp.exp(jax.random.uniform(jax.random.fold_in(own, dim), (shards_of,), jnp.float32, low / len(cuts), largest / len(cuts)))
        level = level * jnp.repeat(steps, extent[dim] // shards_of).reshape([-1 if axis == dim else 1 for axis in range(len(extent))])
    return level


def assign_block(key, own, number, rows, number_of, top, bound, slope):
    ranking = jax.random.permutation(key, number_of)
    crowded, ordinary = portions_of(number_of, rows * top, bound, slope, True), portions_of(number_of, rows * top, bound, slope, False)
    places = jnp.arange(number_of)

    def named(sizes, offset_by):
        used = int((sizes > 0).sum())
        fixed = max(1, used // 4)
        shifted = fixed + (places - fixed + offset_by * (used - fixed)) % max(1, number_of - fixed)
        return jnp.zeros((number_of,), jnp.int32).at[ranking[jnp.where(places < fixed, places, shifted)]].set(jnp.asarray(sizes, jnp.int32))

    sizes = jnp.where(number % 4 == 0, named(crowded, number // 4), named(ordinary, number - number // 4 - 1))
    mixed = jax.random.permutation(jax.random.fold_in(own, 3), number_of)
    giver, receiver = mixed[0:number_of // 2 * 2:2], mixed[1:number_of // 2 * 2:2]
    room = jnp.minimum(sizes[giver] - 1, bound - sizes[receiver]) // 2
    room = jnp.where((giver == ranking[0]) | (receiver == ranking[0]) | (sizes[receiver] == 0), 0, jnp.maximum(room, 0))
    shifted = jax.random.randint(jax.random.fold_in(own, 4), (number_of // 2,), 0, 1 << 20) % (room + 1)
    sizes = sizes.at[giver].add(-shifted).at[receiver].add(shifted)
    items = jnp.searchsorted(jnp.cumsum(sizes), jnp.arange(rows * top), side="right").astype(jnp.int32)
    listing = items.reshape(top, rows).T
    listing = listing[jax.random.permutation(jax.random.fold_in(own, 1), rows)]
    offset_by = jax.random.randint(jax.random.fold_in(own, 2), (rows, 1), 0, top)
    return jnp.take_along_axis(listing, (jnp.arange(top)[None, :] + offset_by) % top, axis=1)


def portions_of(count, total, most, lean, full):
    weights = [(1 << 20) // math.isqrt(standing ** lean) + 1 for standing in range(1, count + 1)]
    largest = most if full else min(most, max(-(-total // count), total * weights[0] // sum(weights)))
    least = 1 if total - largest >= count - 1 else 0
    given, rest = [largest] + [least] * (count - 1), total - largest - least * (count - 1)
    while rest > 0:
        movable = [i for i in range(1, count) if given[i] < largest] or [i for i in range(1, count) if given[i] < most]
        whole, left = sum([weights[i] for i in movable]), rest
        for i in movable:
            addition = min(most - given[i], max(1, left * weights[i] // whole), rest)
            given[i] = given[i] + addition
            rest = rest - addition
    return np.array(given)


def bell_draw(stream_key, shape, deviation, bound, shards=(), kind=jnp.bfloat16):
    array = jax.random.normal(stream_key, shape, jnp.float32) * deviation
    if len(shards) > 0:
        array = levels(stream_key, shape, shards, -0.22, 0.18) * array
    return jnp.clip(array, min=-bound, max=bound).astype(kind)


def setup_inputs(seed: int = 0) -> dict:
    key_list = jax.random.split(jax.random.key(seed), 23)
    tokens = bell_draw(key_list[0], (BATCH, D), 1.0, 6.0, ((0, 8),))
    retention_state = bell_draw(key_list[1], (BATCH, HEADS, HEAD_SIZE, HEAD_SIZE), 0.25, 1.5, ((0, 8), (1, 4)), jnp.float32)
    lengths = touch_ends(jax.random.randint(key_list[2], (BATCH,), 1024, 16384), jax.random.fold_in(key_list[2], 1), 1024, 16383).astype(jnp.int32)
    query_weight = bell_draw(key_list[3], (D, HEADS * HEAD_SIZE), D ** -0.5, 0.125, ((1, 4),))
    key_weight = bell_draw(key_list[4], (D, HEADS * HEAD_SIZE), D ** -0.5, 0.125, ((1, 4),))
    value_weight = bell_draw(key_list[5], (D, HEADS * HEAD_SIZE), D ** -0.5, 0.125, ((1, 4),))
    gate_weight = bell_draw(key_list[6], (D, HEADS * HEAD_SIZE), D ** -0.5, 0.125, ((1, 4),))
    out_weight = bell_draw(key_list[7], (HEADS * HEAD_SIZE, D), (HEADS * HEAD_SIZE) ** -0.5, 0.1875, ((1, 4),))
    first_gain = jnp.clip(1.0 + 0.18 * jax.random.normal(key_list[8], (D,), jnp.float32), 0.1, 1.9)
    routing_keys = jax.random.split(jax.random.fold_in(key_list[9], 1), BATCH // SEQ_DEV)
    routing_turns = jax.random.permutation(jax.random.fold_in(key_list[9], 3), BATCH // SEQ_DEV)
    routing = jax.vmap(lambda own, number: assign_block(jax.random.fold_in(key_list[9], 2), own, number, SEQ_DEV, EXPERTS, TOPK, CAP, 2))(routing_keys, routing_turns).reshape((BATCH, TOPK))
    route_weight = jnp.clip(0.1 + 0.9 * jax.random.uniform(key_list[10], (BATCH, TOPK), jnp.float32) ** levels(key_list[10], (BATCH, TOPK), ((0, 8),), -0.2, 0.2), 0.1, 1.0)
    expert_gate = bell_draw(key_list[11], (EXPERTS, D, FE), D ** -0.5, 0.125, ((0, 8), (2, 4)))
    expert_up = bell_draw(key_list[12], (EXPERTS, D, FE), D ** -0.5, 0.125, ((0, 8), (2, 4)))
    expert_down = bell_draw(key_list[13], (EXPERTS, FE, D), FE ** -0.5, 0.25, ((0, 8), (2, 4)))
    shared_gate = bell_draw(key_list[14], (D, SHARED_F), D ** -0.5, 0.125, ((1, 4),))
    shared_up = bell_draw(key_list[15], (D, SHARED_F), D ** -0.5, 0.125, ((1, 4),))
    shared_down = bell_draw(key_list[16], (SHARED_F, D), SHARED_F ** -0.5, 0.25, ((1, 4),))
    side_gate = bell_draw(key_list[17], (D, DENSE_F), D ** -0.5, 0.125, ((0, 8), (1, 4)))
    side_up = bell_draw(key_list[18], (D, DENSE_F), D ** -0.5, 0.125, ((0, 8), (1, 4)))
    side_down = bell_draw(key_list[19], (DENSE_F, D), DENSE_F ** -0.5, 0.375, ((1, 4),))
    side_switch = bell_draw(key_list[20], (D,), D ** -0.5, 0.125)
    second_gain = jnp.clip(1.0 + 0.18 * jax.random.normal(key_list[21], (D,), jnp.float32), 0.1, 1.9)
    return {"tokens": tokens, "retention_state": retention_state, "lengths": lengths, "query_weight": query_weight, "key_weight": key_weight, "value_weight": value_weight, "gate_weight": gate_weight, "out_weight": out_weight, "first_gain": first_gain, "routing": routing, "route_weight": route_weight, "expert_gate": expert_gate, "expert_up": expert_up, "expert_down": expert_down, "shared_gate": shared_gate, "shared_up": shared_up, "shared_down": shared_down, "side_gate": side_gate, "side_up": side_up, "side_down": side_down, "side_switch": side_switch, "second_gain": second_gain}


RESIDUAL_SCALE = 2.0 ** 0.25
NORM_EPS = 1e-05
GROUP_EPS = 1e-06
ROPE_BASE = 10000.0

def rotate(vector, positions):
    half_width = vector.shape[-1] // 2
    frequency = ROPE_BASE ** (-jnp.arange(half_width, dtype=jnp.float32) / half_width)
    angles = positions.astype(jnp.float32)[:, None, None] * frequency[None, None, :]
    cosine = jnp.cos(angles)
    sine_part = jnp.sin(angles)
    first_half = vector[..., :half_width]
    second_half = vector[..., half_width:]
    return jnp.concatenate([first_half * cosine - second_half * sine_part, second_half * cosine + first_half * sine_part], -1)

def retain(tokens, retention_state, lengths, query_weight, key_weight, value_weight, gate_weight, first_head):
    row_count = tokens.shape[0]
    head_count = retention_state.shape[1]
    head_width = retention_state.shape[2]

    def project(weight):
        rounded = jnp.dot(tokens, weight, preferred_element_type=jnp.float32).astype(jnp.bfloat16)
        return lax.optimization_barrier(rounded).astype(jnp.float32)
    queries = rotate(project(query_weight).reshape(row_count, head_count, head_width), lengths)
    key_rows = rotate(project(key_weight).reshape(row_count, head_count, head_width), lengths) * head_width ** (-0.5)
    values = project(value_weight).reshape(row_count, head_count, head_width)
    gate_act = project(gate_weight)
    head_index = (first_head + jnp.arange(head_count)).astype(jnp.float32)
    decays = 1.0 - 2.0 ** (-5.0 - 7.0 * head_index / (HEADS - 1))
    own_term = lax.optimization_barrier(jnp.sum(queries * key_rows, -1, keepdims=True)) * values
    carried = decays[None, :, None] * jnp.einsum('bhd,bhde->bhe', queries, retention_state, precision=lax.Precision.HIGHEST)
    result = own_term + carried
    new_state = decays[None, :, None, None] * retention_state + key_rows[:, :, :, None] * values[:, :, None, :]
    normed = result * lax.rsqrt(lax.optimization_barrier(jnp.mean(result * result, -1, keepdims=True)) + GROUP_EPS)
    mixed_heads = (normed.reshape(row_count, head_count * head_width) * jax.nn.silu(gate_act)).astype(jnp.bfloat16)
    return (mixed_heads, new_state)

def layer_norm(values, gain):
    row_mean = lax.optimization_barrier(jnp.mean(values, -1, keepdims=True))
    square = lax.optimization_barrier(jnp.mean(values * values, -1, keepdims=True))
    return ((values - row_mean) * lax.rsqrt(square - row_mean * row_mean + NORM_EPS) * gain).astype(jnp.bfloat16)

def slot_numbers(route_ids, expert_count, capacity):
    onehot = (route_ids[..., None] == jnp.arange(expert_count, dtype=jnp.int32)).astype(jnp.int32)
    position = lax.optimization_barrier(jnp.sum(jnp.cumsum(onehot, -2) * onehot, -1)) - 1
    return route_ids * capacity + position

def take_rows(source_rows, row_index):
    return source_rows[row_index]

def one_expert(operands):
    rows_in, gate_mat, up_mat, down_mat = operands
    gate_part = jnp.dot(rows_in, gate_mat, preferred_element_type=jnp.float32)
    up_part = jnp.dot(rows_in, up_mat, preferred_element_type=jnp.float32)
    hidden = (jax.nn.silu(gate_part) * up_part).astype(jnp.bfloat16)
    return jnp.dot(hidden, down_mat, preferred_element_type=jnp.float32).astype(jnp.bfloat16)

def reference(tokens, retention_state, lengths, query_weight, key_weight, value_weight, gate_weight, out_weight, first_gain, routing, route_weight, expert_gate, expert_up, expert_down, shared_gate, shared_up, shared_down, side_gate, side_up, side_down, side_switch, second_gain):
    mixed_heads, new_state = retain(tokens, retention_state, lengths, query_weight, key_weight, value_weight, gate_weight, 0)
    mixing = jnp.dot(mixed_heads, out_weight, preferred_element_type=jnp.float32)
    normed = layer_norm(RESIDUAL_SCALE * tokens.astype(jnp.float32) + mixing, first_gain)
    shared_hidden = (jax.nn.silu(jnp.dot(normed, shared_gate, preferred_element_type=jnp.float32)) * jnp.dot(normed, shared_up, preferred_element_type=jnp.float32)).astype(jnp.bfloat16)
    shared_out = jnp.dot(shared_hidden, shared_down, preferred_element_type=jnp.float32)
    side_hidden = (jax.nn.silu(jnp.dot(normed, side_gate, preferred_element_type=jnp.float32)) * jnp.dot(normed, side_up, preferred_element_type=jnp.float32)).astype(jnp.bfloat16)
    side_out = jnp.dot(side_hidden, side_down, preferred_element_type=jnp.float32)
    switch = jax.nn.sigmoid(jnp.dot(normed, side_switch, preferred_element_type=jnp.float32))
    assigned = SEQ_DEV * TOPK
    groups = routing.reshape(N_EP, assigned)
    slot_ids = slot_numbers(groups, EXPERTS, CAP)
    owners = jnp.arange(assigned, dtype=jnp.int32) // TOPK
    table = jnp.full((N_EP, EXPERTS * CAP), SEQ_DEV, jnp.int32)
    table = table.at[jnp.arange(N_EP, dtype=jnp.int32)[:, None], slot_ids].set(jnp.broadcast_to(owners[None, :], (N_EP, assigned)))
    padded = jnp.concatenate([normed.reshape(N_EP, SEQ_DEV, D), jnp.zeros((N_EP, 1, D), jnp.bfloat16)], 1)
    slot_rows = jax.vmap(take_rows)(padded, table)
    per_expert = jnp.transpose(slot_rows.reshape(N_EP, EXPERTS, CAP, D), (1, 0, 2, 3)).reshape(EXPERTS, N_EP * CAP, D)
    outputs = lax.map(one_expert, (per_expert, expert_gate, expert_up, expert_down))
    back = jnp.transpose(outputs.reshape(EXPERTS, N_EP, CAP, D), (1, 0, 2, 3)).reshape(N_EP, EXPERTS * CAP, D)
    picked = jax.vmap(take_rows)(back, slot_ids).reshape(BATCH, TOPK, D)
    routed = lax.optimization_barrier(jnp.sum(picked.astype(jnp.float32) * route_weight[:, :, None], 1))
    pre_second = RESIDUAL_SCALE * normed.astype(jnp.float32) + routed + shared_out + switch[:, None] * side_out
    output = layer_norm(pre_second, second_gain)
    return (output, new_state)
```

```python
import functools

import jax
import jax.numpy as jnp
import numpy as np
from jax import lax
from jax.experimental import pallas as pl
from jax.experimental.pallas import tpu as pltpu
from jax.sharding import PartitionSpec as P

HEADS = 16


RESIDUAL_SCALE = 2.0**0.25
NORM_EPS = 1e-05
GROUP_EPS = 1e-06
ROPE_BASE = 10000.0


def rotate(vector, positions):
    half_width = vector.shape[-1] // 2
    frequency = ROPE_BASE ** (-jnp.arange(half_width, dtype=jnp.float32) / half_width)
    angles = positions.astype(jnp.float32)[:, None, None] * frequency[None, None, :]
    cosine = jnp.cos(angles)
    sine_part = jnp.sin(angles)
    first_half = vector[..., :half_width]
    second_half = vector[..., half_width:]
    return jnp.concatenate(
        [
            first_half * cosine - second_half * sine_part,
            second_half * cosine + first_half * sine_part,
        ],
        -1,
    )


def retain(
    retention_state,
    lengths,
    projections,
    first_head,
):
    row_count = retention_state.shape[0]
    head_count = retention_state.shape[1]
    head_width = retention_state.shape[2]

    query_rows, key_part, value_part, gate_part = [part.astype(jnp.float32) for part in projections]
    queries = rotate(query_rows.reshape(row_count, head_count, head_width), lengths)
    key_rows = rotate(
        key_part.reshape(row_count, head_count, head_width), lengths
    ) * head_width ** (-0.5)
    values = value_part.reshape(row_count, head_count, head_width)
    gate_act = gate_part
    head_index = (first_head + jnp.arange(head_count)).astype(jnp.float32)
    decays = 1.0 - 2.0 ** (-5.0 - 7.0 * head_index / (HEADS - 1))
    own_term = jnp.sum(queries * key_rows, -1, keepdims=True) * values
    carried = decays[None, :, None] * jnp.sum(queries[:, :, :, None] * retention_state, 2)
    result = own_term + carried
    new_state = (
        decays[None, :, None, None] * retention_state
        + key_rows[:, :, :, None] * values[:, :, None, :]
    )
    normed = result * lax.rsqrt(jnp.mean(result * result, -1, keepdims=True) + GROUP_EPS)
    mixed_heads = (
        normed.reshape(row_count, head_count * head_width) * jax.nn.silu(gate_act)
    ).astype(jnp.bfloat16)
    return (mixed_heads, new_state)


VMEM = pl.BlockSpec(memory_space=pltpu.VMEM)
DEVICE = pl.DeviceIdType.MESH


def enter(peers):
    barrier = pltpu.get_barrier_semaphore()
    for peer in peers:
        pl.semaphore_signal(barrier, inc=1, device_id=peer, device_id_type=DEVICE)
    pl.semaphore_wait(barrier, len(peers))


def send(source, target, send_sem, recv_sem, peer):
    copy = pltpu.make_async_remote_copy(
        src_ref=source,
        dst_ref=target,
        send_sem=send_sem,
        recv_sem=recv_sem,
        device_id=peer,
        device_id_type=DEVICE,
    )
    copy.start()
    return copy


def on_axis(axis, index):
    if axis == "ep":
        return (index, lax.axis_index("tp"))
    return (lax.axis_index("ep"), index)


def gather_body(axis, count, parts, *refs):
    sources, targets = refs[:parts], refs[parts : 2 * parts]
    send_sem, recv_sem, local_sem = refs[2 * parts :]
    me = lax.axis_index(axis)
    others = [lax.rem(me + step, count) for step in range(1, count)]
    locals_ = []
    for part in range(parts):
        own = pltpu.make_async_copy(sources[part], targets[part].at[me], local_sem.at[part])
        own.start()
        locals_.append(own)
    enter([on_axis(axis, other) for other in others])
    copies = []
    for step, other in enumerate(others):
        for part in range(parts):
            copies.append(
                send(
                    sources[part],
                    targets[part].at[me],
                    send_sem.at[step, part],
                    recv_sem.at[step, part],
                    on_axis(axis, other),
                )
            )
    for copy in locals_:
        copy.wait()
    for copy in copies:
        copy.wait()


def gather(arrays, axis, ident):
    count, parts = lax.axis_size(axis), len(arrays)
    return pl.pallas_call(
        functools.partial(gather_body, axis, count, parts),
        out_shape=[jax.ShapeDtypeStruct((count,) + a.shape, a.dtype) for a in arrays],
        in_specs=[VMEM] * parts,
        out_specs=[VMEM] * parts,
        scratch_shapes=[
            pltpu.SemaphoreType.DMA((count - 1, parts)),
            pltpu.SemaphoreType.DMA((count - 1, parts)),
            pltpu.SemaphoreType.DMA((parts,)),
        ],
        compiler_params=pltpu.CompilerParams(collective_id=ident, has_side_effects=True),
    )(*arrays)


def scatter_body(count, source, target, send_sem, recv_sem, local_sem):
    me = lax.axis_index("ep")
    others = [lax.rem(me + step, count) for step in range(1, count)]
    own = pltpu.make_async_copy(source.at[me], target.at[me], local_sem)
    own.start()
    enter([on_axis("ep", other) for other in others])
    copies = [
        send(
            source.at[other],
            target.at[me],
            send_sem.at[step],
            recv_sem.at[step],
            on_axis("ep", other),
        )
        for step, other in enumerate(others)
    ]
    own.wait()
    for copy in copies:
        copy.wait()


def scatter(array, ident):
    count = array.shape[0]
    return pl.pallas_call(
        functools.partial(scatter_body, count),
        out_shape=jax.ShapeDtypeStruct(array.shape, array.dtype),
        in_specs=[VMEM],
        out_specs=VMEM,
        scratch_shapes=[
            pltpu.SemaphoreType.DMA((count - 1,)),
            pltpu.SemaphoreType.DMA((count - 1,)),
            pltpu.SemaphoreType.DMA,
        ],
        compiler_params=pltpu.CompilerParams(collective_id=ident, has_side_effects=True),
    )(array)


def first_body(count, *refs):
    parts = 3
    sources, (tokens, *weights) = refs[:parts], refs[parts : parts + 5]
    targets = refs[parts + 5 : 2 * parts + 5]
    results = refs[2 * parts + 5 : 2 * parts + 9]
    send_sem, recv_sem, local_sem = refs[2 * parts + 9 :]
    chips = count // 2
    me = lax.axis_index("ep")
    chip, core = me // 2, lax.rem(me, 2)
    partner = on_axis("ep", chip * 2 + 1 - core)
    line = [lax.rem(chip + step, chips) * 2 + core for step in range(1, chips)]
    senders = [lax.rem(chip + chips - step, chips) * 2 + core for step in range(1, chips)]
    locals_ = []
    for part in range(parts):
        own = pltpu.make_async_copy(sources[part], targets[part].at[me], local_sem.at[part])
        own.start()
        locals_.append(own)
    enter([on_axis("ep", other) for other in line] + [partner])
    direct, copies = [], []
    for step, other in enumerate(line):
        for part in range(parts):
            direct.append(
                send(
                    sources[part],
                    targets[part].at[me],
                    send_sem.at[step, part],
                    recv_sem.at[step, part],
                    on_axis("ep", other),
                )
            )
    for part in range(parts):
        copies.append(
            send(
                sources[part],
                targets[part].at[me],
                send_sem.at[chips - 1, part],
                recv_sem.at[chips - 1, part],
                partner,
            )
        )
    for weight, result in zip(weights, results):
        result[...] = jnp.dot(
            tokens[...], weight[...], preferred_element_type=jnp.float32
        ).astype(result.dtype)
    for step, sender in enumerate(senders):
        for part in range(parts):
            direct[step * parts + part].wait_recv()
            copies.append(
                send(
                    targets[part].at[sender],
                    targets[part].at[sender],
                    send_sem.at[chips + step, part],
                    recv_sem.at[chips + step, part],
                    partner,
                )
            )
    for copy in locals_:
        copy.wait()
    for copy in direct:
        copy.wait_send()
    for copy in copies:
        copy.wait()


def first(arrays, tokens, weights, ident):
    count, parts = lax.axis_size("ep"), len(arrays)
    rows = tokens.shape[0]
    return pl.pallas_call(
        functools.partial(first_body, count),
        out_shape=[jax.ShapeDtypeStruct((count,) + a.shape, a.dtype) for a in arrays]
        + [jax.ShapeDtypeStruct((rows, w.shape[1]), jnp.bfloat16) for w in weights],
        in_specs=[VMEM] * (parts + 5),
        out_specs=[VMEM] * (parts + 4),
        scratch_shapes=[
            pltpu.SemaphoreType.DMA((count - 1, parts)),
            pltpu.SemaphoreType.DMA((count - 1, parts)),
            pltpu.SemaphoreType.DMA((parts,)),
        ],
        compiler_params=pltpu.CompilerParams(collective_id=ident, has_side_effects=True),
    )(*arrays, tokens, *weights)


def spread_body(count, tp_count, source, target, send_sem, recv_sem, local_sem):
    chips, width = count // 2, source.shape[1]
    me, own_tp = lax.axis_index("ep"), lax.axis_index("tp")
    chip, core = me // 2, lax.rem(me, 2)
    partner = (chip * 2 + 1 - core, own_tp)

    def place(row, col):
        return target.at[row, :, pl.ds(pl.multiple_of(col * width, width), width)]

    def chip_at(step):
        return lax.rem(chip + chips + step, chips) * 2 + core

    def tp_at(step):
        return lax.rem(own_tp + tp_count + step, tp_count)

    own = pltpu.make_async_copy(source, place(me, own_tp), local_sem)
    own.start()
    line = [(chip_at(step), own_tp) for step in range(1, chips)]
    plane = [(me, tp_at(step)) for step in range(1, tp_count)]
    enter(line + plane + [partner])

    def pair(line_step, plane_step, to_partner):
        return (
            send_sem.at[to_partner, line_step, plane_step],
            recv_sem.at[to_partner, line_step, plane_step],
        )

    direct, planar, copies = [], {}, []
    for step in range(1, chips):
        direct.append(send(source, place(me, own_tp), *pair(step, 0, 0), line[step - 1]))
    for step in range(1, tp_count):
        planar[(0, step)] = send(source, place(me, own_tp), *pair(0, step, 0), plane[step - 1])
    copies.append(send(source, place(me, own_tp), *pair(0, 0, 1), partner))
    for line_step in range(1, chips):
        direct[line_step - 1].wait_recv()
        block = place(chip_at(-line_step), own_tp)
        for step in range(1, tp_count):
            planar[(line_step, step)] = send(
                block, block, *pair(line_step, step, 0), plane[step - 1]
            )
        copies.append(send(block, block, *pair(line_step, 0, 1), partner))
    for line_step in range(chips):
        for step in range(1, tp_count):
            planar[(line_step, step)].wait_recv()
            block = place(chip_at(-line_step), tp_at(-step))
            copies.append(send(block, block, *pair(line_step, step, 1), partner))
    own.wait()
    for copy in direct:
        copy.wait_send()
    for copy in planar.values():
        copy.wait_send()
    for copy in copies:
        copy.wait()


def spread(block, ident):
    count, tp_count = lax.axis_size("ep"), lax.axis_size("tp")
    rows, width = block.shape
    return pl.pallas_call(
        functools.partial(spread_body, count, tp_count),
        out_shape=jax.ShapeDtypeStruct((count, rows, width * tp_count), block.dtype),
        in_specs=[VMEM],
        out_specs=VMEM,
        scratch_shapes=[
            pltpu.SemaphoreType.DMA((2, count // 2, tp_count)),
            pltpu.SemaphoreType.DMA((2, count // 2, tp_count)),
            pltpu.SemaphoreType.DMA,
        ],
        compiler_params=pltpu.CompilerParams(collective_id=ident, has_side_effects=True),
    )(block)


def side_by_side(gathered):
    return jnp.concatenate([gathered[i] for i in range(gathered.shape[0])], -1)


def row_moments(values, ident):
    sums = jnp.stack([jnp.sum(values, -1), jnp.sum(values * values, -1)])
    (every,) = gather([sums], "tp", ident)
    totals = jnp.sum(every, 0)
    return totals[0][:, None], totals[1][:, None]


ANY = pl.BlockSpec(memory_space=pl.ANY)


def dot(a, b):
    return jnp.dot(a, b, preferred_element_type=jnp.float32)


def silu(x):
    return x / (1.0 + jnp.exp(-x))


def fetch(source, target, sem):
    copy = pltpu.make_async_copy(source, target, sem)
    copy.start()
    return copy


def rotated(x, cosine, sine, half):
    width = x.shape[1]
    lane = lax.broadcasted_iota(jnp.int32, x.shape, 1)
    first = (lane & (2 * half - 1)) < half
    later = pltpu.roll(x, width - half, 1)
    sooner = pltpu.roll(x, half, 1)
    return x * cosine + jnp.where(first, -later, sooner) * sine


def retain_body(
    chunk,
    tokens_in,
    lengths,
    frequency,
    query_in,
    key_in,
    value_in,
    gate_in,
    state_in,
    mixed,
    state_out,
    tokens,
    weights,
    state,
    queries,
    keys,
    values,
    carried,
    weight_sem,
    state_sem,
    out_sem,
):
    rows, heads, width = state.shape[0], state.shape[1], state.shape[2]
    chunks = rows // chunk
    tokens_copy = fetch(tokens_in, tokens, weight_sem.at[4])
    copies = [
        fetch(source, weights.at[i], weight_sem.at[i])
        for i, source in enumerate([query_in, key_in, value_in, gate_in])
    ]
    for i in range(chunks):
        piece = pl.ds(i * chunk, chunk)
        fetch(state_in.at[piece], state.at[piece], state_sem.at[i])

    row = lax.broadcasted_iota(jnp.int32, (rows, rows), 0)
    col = lax.broadcasted_iota(jnp.int32, (rows, rows), 1)
    position = jnp.sum(
        jnp.where(row == col, lengths[...].astype(jnp.float32), 0.0), 1, keepdims=True
    )
    angles = position * frequency[...]
    cosine, sine = jnp.cos(angles), jnp.sin(angles)
    first_head = lax.axis_index("tp") * heads

    tokens_copy.wait()

    def project(i):
        copies[i].wait()
        return dot(tokens[...], weights[i]).astype(jnp.bfloat16).astype(jnp.float32)

    def head_of(x, head):
        return x[:, head * width : (head + 1) * width]

    query = rotated(project(0), cosine, sine, width // 2)
    queries[...] = query
    key = rotated(project(1), cosine, sine, width // 2) * width ** (-0.5)
    keys[...] = key
    value = project(2)
    for head in range(heads):
        values[head] = head_of(value, head)
    gate = project(3)
    decays = []
    for head in range(heads):
        index = jnp.full((1, width), first_head + head, jnp.int32).astype(jnp.float32)
        decays.append(1.0 - jnp.exp2(-5.0 - 7.0 * index / (HEADS - 1)))

    def step(i, carry):
        base = pl.multiple_of(i * chunk, chunk)
        piece = pl.ds(base, chunk)
        pltpu.make_async_copy(state_in.at[piece], state.at[piece], state_sem.at[i]).wait()
        query_cols = jnp.transpose(queries[piece, :])
        key_cols = jnp.transpose(keys[piece, :])
        for at in range(chunk):
            for head in range(heads):
                span = slice(head * width, (head + 1) * width)
                old = state[base + at, head]
                q_col = query_cols[span, at : at + 1]
                k_col = key_cols[span, at : at + 1]
                v_row = values[head, pl.ds(base + at, 1), :]
                carried[head, pl.ds(base + at, 1), :] = jnp.sum(q_col * old, 0, keepdims=True)
                state[base + at, head] = decays[head] * old + k_col * v_row
        pltpu.make_async_copy(state.at[piece], state_out.at[piece], out_sem.at[i]).start()
        return carry

    lax.fori_loop(0, chunks, step, 0)
    both = query * key
    parts = []
    for head in range(heads):
        own = jnp.sum(head_of(both, head), -1, keepdims=True) * values[head]
        result = own + decays[head] * carried[head]
        scale = lax.rsqrt(jnp.mean(result * result, -1, keepdims=True) + GROUP_EPS)
        parts.append(result * scale)
    mixed[...] = (jnp.concatenate(parts, 1) * silu(gate)).astype(mixed.dtype)
    for i in range(chunks):
        piece = pl.ds(i * chunk, chunk)
        pltpu.make_async_copy(state.at[piece], state_out.at[piece], out_sem.at[i]).wait()


def retain_kernel(tokens, lengths, frequency, weights, state):
    rows, heads, width = state.shape[0], state.shape[1], state.shape[2]
    chunk = 8
    cols = heads * width
    return pl.pallas_call(
        functools.partial(retain_body, chunk),
        out_shape=[
            jax.ShapeDtypeStruct((rows, cols), jnp.bfloat16),
            jax.ShapeDtypeStruct(state.shape, state.dtype),
        ],
        in_specs=[ANY, VMEM, VMEM] + [ANY] * 5,
        out_specs=[VMEM, ANY],
        scratch_shapes=[
            pltpu.VMEM(tokens.shape, tokens.dtype),
            pltpu.VMEM((4,) + weights[0].shape, weights[0].dtype),
            pltpu.VMEM(state.shape, state.dtype),
            pltpu.VMEM((rows, cols), jnp.float32),
            pltpu.VMEM((rows, cols), jnp.float32),
            pltpu.VMEM((heads, rows, width), jnp.float32),
            pltpu.VMEM((heads, rows, width), jnp.float32),
            pltpu.SemaphoreType.DMA((5,)),
            pltpu.SemaphoreType.DMA((rows // chunk,)),
            pltpu.SemaphoreType.DMA((rows // chunk,)),
        ],
    )(tokens, lengths, frequency, *weights, state)


def mixer_body(
    dims,
    mixed,
    tokens,
    routes,
    route_weights,
    first_gain,
    second_gain,
    side_switch,
    out_in,
    gate_in,
    up_in,
    down_in,
    shared_gate_in,
    shared_up_in,
    shared_down_in,
    side_gate_in,
    side_up_in,
    side_down_in,
    output,
    mixed_all,
    route_all,
    weight_all,
    rows_all,
    normed,
    own_normed,
    info,
    info_cols,
    hidden_all,
    pair_out,
    pair_in,
    line_out,
    line_in,
    total,
    side_out,
    side_in,
    late_all,
    stats,
    out_w,
    gate_up_w,
    down_w,
    shared_w,
    shared_down_w,
    side_w,
    side_down_w,
    weight_sem,
    head_sems,
    route_sems,
    row_sems,
    hidden_sems,
    back_sems,
    side_sems,
    late_sems,
    stat_sems,
):
    chips, tps, capacity = dims
    steps = chips
    rows, model = tokens.shape
    cols = model // tps
    half = cols // 2
    experts, hidden_width = gate_in.shape[0], gate_in.shape[2]
    slots = hidden_all.shape[3]
    side_width = side_gate_in.shape[0]
    side_rows = side_gate_in.shape[1]
    tp = lax.axis_index("tp")
    ep = lax.axis_index("ep")
    chip, core = ep // 2, lax.rem(ep, 2)
    partner = (chip * 2 + 1 - core, tp)
    low, high = lax.rem(tp, 2), tp // 2
    tp_x = high * 2 + 1 - low
    tp_y = (1 - high) * 2 + low
    tp_d = (1 - high) * 2 + 1 - low
    plane = [(ep, tp_x), (ep, tp_y), (ep, tp_d)]

    def chip_at(step):
        if step == 0:
            return chip
        if step == 1:
            return chip + 1 - 2 * lax.rem(chip, 2)
        if step == 2:
            return lax.rem(chip + 2, 4)
        return 3 - chip

    others = []
    for step in range(1, steps):
        others += [(chip_at(step) * 2 + core, tp), (chip_at(step) * 2 + 1 - core, tp)]
    others.append(partner)

    loads = {}

    def load(name, source, target, index):
        loads.setdefault(name, []).append(fetch(source, target, weight_sem.at[index]))

    def ready(name):
        for copy in loads.pop(name):
            copy.wait()

    load("out", out_in, out_w, 0)
    for e in range(experts):
        load("gate_up", gate_in.at[e], gate_up_w.at[e, :, pl.ds(0, hidden_width)], 1 + 2 * e)
        load(
            "gate_up",
            up_in.at[e],
            gate_up_w.at[e, :, pl.ds(hidden_width, hidden_width)],
            2 + 2 * e,
        )
    base = 1 + 2 * experts
    shared_width = shared_gate_in.shape[1]
    load("side", side_gate_in, side_w.at[pl.ds(0, side_width)], base)
    load("side", side_up_in, side_w.at[pl.ds(side_width, side_width)], base + 1)
    load("shared", shared_gate_in, shared_w.at[:, pl.ds(0, shared_width)], base + 2)
    load("shared", shared_up_in, shared_w.at[:, pl.ds(shared_width, shared_width)], base + 3)
    load("down", down_in, down_w, base + 4)
    load("late", shared_down_in, shared_down_w, base + 5)
    load("late", side_down_in, side_down_w, base + 6)

    pending = []

    def push(source, target, sems, index, peer):
        copy = send(source, target, sems.at[(0,) + index], sems.at[(1,) + index], peer)
        pending.append(copy)
        return copy

    enter(plane + others)

    mixed_copies = [push(mixed, mixed_all.at[tp], head_sems, (i,), p) for i, p in enumerate(plane)]
    route_copies = []
    for i, other in enumerate(others):
        route_copies.append(push(routes, route_all.at[ep], route_sems, (i, 0), other))
        route_copies.append(push(route_weights, weight_all.at[ep], route_sems, (i, 1), other))
    route_all[ep] = routes[...]
    weight_all[ep] = route_weights[...]

    def head_rows(index):
        width = mixed.shape[1]
        return out_w[pl.ds(pl.multiple_of(index * width, width), width), :]

    ready("out")
    own_cols = tokens[:, pl.ds(pl.multiple_of(tp * cols, cols), cols)].astype(jnp.float32)
    pre_first = RESIDUAL_SCALE * own_cols + dot(mixed[...], head_rows(tp))
    for copy, index in zip(mixed_copies, [tp_x, tp_y, tp_d]):
        copy.wait_recv()
        pre_first = pre_first + dot(mixed_all[index], head_rows(index))
    for part in range(2):
        rows_all[ep, 2 * tp + part] = pre_first[:, part * half : (part + 1) * half].astype(
            jnp.bfloat16
        )

    def block(step, index):
        return rows_all.at[chip_at(step) * 2 + core, pl.ds(2 * index, 2)]

    def piece(step, index, part):
        return rows_all.at[chip_at(step) * 2 + core, 2 * index + part]

    line = {}
    flat = {}
    across = {}
    shared_rows = {}

    def push_rows(ref, step, kind, peer):
        return push(ref, ref, row_sems, (step, kind), peer)

    def spread(step):
        if step > 0:
            line[step].wait_recv()
        ref = block(step, tp)
        flat[step] = (push_rows(ref, step, 1, plane[0]), push_rows(ref, step, 2, plane[1]))
        shared_rows[step] = [push_rows(ref, step, 3, partner)]

    def relay(step):
        by_x, by_y = flat[step]
        by_x.wait_recv()
        first_half = push_rows(piece(step, tp_x, 0), step, 4, plane[1])
        shared_rows[step].append(push_rows(block(step, tp_x), step, 5, partner))
        by_y.wait_recv()
        second_half = push_rows(piece(step, tp_y, 1), step, 6, plane[0])
        shared_rows[step].append(push_rows(block(step, tp_y), step, 7, partner))
        across[step] = (first_half, second_half)

    def corner(step):
        for part in range(2):
            across[step][part].wait_recv()
            shared_rows[step].append(push_rows(piece(step, tp_d, part), step, 8 + part, partner))

    def arrive(step):
        for copy in shared_rows[step]:
            copy.wait_recv()

    for step in range(1, steps):
        line[step] = push(
            block(0, tp), block(0, tp), row_sems, (step, 0), (chip_at(step) * 2 + core, tp)
        )
    spread(0)

    for copy in route_copies:
        copy.wait_recv()
    wide = experts * rows

    def expert_of(index):
        return sum(jnp.where(index >= e * rows, 1, 0) for e in range(1, experts))

    group_lane = expert_of(lax.broadcasted_iota(jnp.int32, (1, wide), 1))
    expert_lane = ep * experts + group_lane
    info[...] = jnp.zeros_like(info)
    eps = route_all.shape[0]
    for g in range(eps):
        ids = jnp.concatenate([route_all[g]] * experts, 1)
        hits = ids == expert_lane
        scales = jnp.concatenate([weight_all[g]] * experts, 1)
        info[g : g + 1, 0:wide] = jnp.sum(jnp.where(hits, 1.0, 0.0), 0, keepdims=True)
        info[eps + g : eps + g + 1, 0:wide] = jnp.sum(
            jnp.where(hits, scales, 0.0), 0, keepdims=True
        )
    member = info[0:eps, 0:wide]
    sooner = lax.broadcasted_iota(jnp.int32, (wide, wide), 0)
    later = lax.broadcasted_iota(jnp.int32, (wide, wide), 1)
    earlier = jnp.where(
        (sooner < later) & (expert_of(sooner) == expert_of(later)), 1.0, 0.0
    ).astype(jnp.bfloat16)
    before = dot(member.astype(jnp.bfloat16), earlier)
    start = (group_lane * capacity).astype(jnp.float32)
    info[0:eps, 0:wide] = jnp.where(member > 0.5, before + start, -1.0)
    info_cols[...] = jnp.transpose(info[...])

    def column(index):
        lane = lax.broadcasted_iota(jnp.int32, (wide, info_cols.shape[1]), 1)
        picked = jnp.where(lane == index, info_cols[0:wide, :], 0.0)
        return jnp.sum(picked, 1, keepdims=True)

    def groups(step):
        return chip_at(step) * 2 + core, chip_at(step) * 2 + 1 - core

    hidden_copies = {}
    side_copies = {}
    side_span = pl.ds(pl.multiple_of(ep * side_rows, side_rows), side_rows)

    def expert_step(step):
        for at, g in enumerate(groups(step)):
            sums = jnp.zeros((rows, half), jnp.float32)
            squares = jnp.zeros((rows, half), jnp.float32)
            for part in range(2 * tps):
                x = rows_all[g, part].astype(jnp.float32)
                sums = sums + x
                squares = squares + x * x
            mean = jnp.sum(sums, 1, keepdims=True) / model
            square = jnp.sum(squares, 1, keepdims=True) / model
            scale = lax.rsqrt(square - mean * mean + NORM_EPS)
            for part in range(2 * tps):
                span = slice(part * half, (part + 1) * half)
                x = rows_all[g, part].astype(jnp.float32)
                y = ((x - mean) * scale * first_gain[:, span]).astype(jnp.bfloat16)
                normed[at * rows : (at + 1) * rows, span] = y
                if step == 0 and at == 0:
                    own_normed[:, span] = y
        if step == 0:
            ready("side")
        side_part = lax.dot_general(
            normed[:, side_span],
            side_w[...],
            (((1,), (1,)), ((), ())),
            preferred_element_type=jnp.float32,
        ).astype(jnp.bfloat16)
        side_copies[step] = []
        for at, g in enumerate(groups(step)):
            side_out[step, at] = side_part[at * rows : (at + 1) * rows]
            if step > 0 or at > 0:
                side_copies[step].append(
                    push(side_out.at[step, at], side_in.at[step, at], side_sems, (step, at), (g, tp))
                )
        if step == 0:
            ready("gate_up")
        stacks = [[], []]
        scales = [column(eps + g) for g in groups(step)]
        for e in range(experts):
            both = dot(normed[...], gate_up_w[e])
            hidden = silu(both[:, :hidden_width]) * both[:, hidden_width:]
            for at in range(2):
                mine = hidden[at * rows : (at + 1) * rows] * scales[at][e * rows : (e + 1) * rows]
                stacks[at].append(mine.astype(jnp.bfloat16))
        for at, g in enumerate(groups(step)):
            slot_row = info[pl.ds(g, 1), 0:wide]
            number = lax.broadcasted_iota(jnp.int32, (slots, wide), 0).astype(jnp.float32)
            table = jnp.where(number == slot_row, 1.0, 0.0).astype(jnp.bfloat16)
            packed = dot(table, jnp.concatenate(stacks[at], 0)).astype(jnp.bfloat16)
            hidden_all[step, tp, at] = packed
        hidden_copies[step] = [
            push(hidden_all.at[step, tp], hidden_all.at[step, tp], hidden_sems, (step, i), p)
            for i, p in enumerate(plane)
        ]

    pair_copies = {}
    line_copies = {}

    def down_step(step):
        for copy in hidden_copies[step]:
            copy.wait_recv()
        if step == 0:
            ready("down")
        spread_rows = []
        for at, g in enumerate(groups(step)):
            number = lax.broadcasted_iota(jnp.int32, (wide, slots), 1).astype(jnp.float32)
            table = jnp.where(number == column(g), 1.0, 0.0).astype(jnp.bfloat16)
            packed = jnp.concatenate([hidden_all[step, t, at] for t in range(tps)], 1)
            spread_rows.append(dot(table, packed).astype(jnp.bfloat16))
        result = None
        for e in range(experts):
            mine = jnp.concatenate([r[e * rows : (e + 1) * rows] for r in spread_rows], 0)
            term = dot(mine, down_w[e])
            result = term if result is None else result + term
        total[step] = result[:rows]
        pair_out[step] = result[rows:].astype(jnp.bfloat16)
        pair_copies[step] = push(
            pair_out.at[step], pair_in.at[step], back_sems, (step, 0), partner
        )

    def return_step(step):
        pair_copies[step].wait_recv()
        mine = total[step] + pair_in[step].astype(jnp.float32)
        if step == 0:
            total[step] = mine
            return
        line_out[step] = mine.astype(jnp.bfloat16)
        line_copies[step] = push(
            line_out.at[step],
            line_in.at[step],
            back_sems,
            (step, 1),
            (chip_at(step) * 2 + core, tp),
        )

    def own_shared():
        ready("shared")
        both = dot(own_normed[...], shared_w[...])
        hidden = silu(both[:, :shared_width]) * both[:, shared_width:]
        late_all[tp, :, 0:shared_width] = hidden.astype(jnp.bfloat16)

    late_copies = []

    def own_side():
        pre = side_out[0, 0].astype(jnp.float32)
        for step in range(steps):
            for at, copy in enumerate(side_copies[step]):
                place = at + 1 if step == 0 else at
                copy.wait_recv()
                pre = pre + side_in[step, place].astype(jnp.float32)
        act = silu(pre[:, :side_width]) * pre[:, side_width:]
        act = jnp.concatenate([act, jnp.zeros_like(act)], 1)
        late_all[tp, :, shared_width : shared_width + 2 * side_width] = act.astype(jnp.bfloat16)
        late_copies.extend(
            push(late_all.at[tp], late_all.at[tp], late_sems, (i,), p) for i, p in enumerate(plane)
        )

    def own_extra():
        product = own_normed[...].astype(jnp.float32) * side_switch[...].astype(jnp.float32)
        logit = jnp.sum(product, 1, keepdims=True)
        switch = 1.0 / (1.0 + jnp.exp(-logit))
        ready("late")
        for copy in late_copies:
            copy.wait_recv()
        shared = jnp.concatenate([late_all[t, :, :shared_width] for t in range(tps)], 1)
        shared = dot(shared, shared_down_w[...])
        side = None
        for t in range(tps):
            mine = late_all[t, :, shared_width : shared_width + side_width]
            term = dot(mine, side_down_w[t * side_width : (t + 1) * side_width, :])
            side = term if side is None else side + term
        return shared + switch * side

    relay(0)
    corner(0)
    spread(1)
    arrive(0)
    relay(1)
    expert_step(0)
    spread(2)
    corner(1)
    arrive(1)
    relay(2)
    expert_step(1)
    spread(3)
    corner(2)
    arrive(2)
    relay(3)
    down_step(0)
    expert_step(2)
    corner(3)
    arrive(3)
    return_step(0)
    expert_step(3)
    down_step(1)
    own_shared()
    return_step(1)
    down_step(2)
    own_side()
    return_step(2)
    down_step(3)
    extra = own_extra()
    return_step(3)

    routed = total[0]
    for step in range(1, steps):
        line_copies[step].wait_recv()
        routed = routed + line_in[step].astype(jnp.float32)
    own = own_normed[:, pl.ds(pl.multiple_of(tp * cols, cols), cols)].astype(jnp.float32)
    pre_second = RESIDUAL_SCALE * own + routed + extra
    lane = lax.broadcasted_iota(jnp.int32, (rows, stats.shape[2]), 1)
    sums = jnp.sum(pre_second, 1, keepdims=True)
    squares = jnp.sum(pre_second * pre_second, 1, keepdims=True)
    stats[tp] = jnp.where(lane == 0, sums, squares)
    stat_copies = [push(stats.at[tp], stats.at[tp], stat_sems, (i,), p) for i, p in enumerate(plane)]
    for copy in stat_copies:
        copy.wait_recv()
    totals = stats[0]
    for t in range(1, tps):
        totals = totals + stats[t]
    mean = jnp.sum(jnp.where(lane == 0, totals, 0.0), 1, keepdims=True) / model
    square = jnp.sum(jnp.where(lane == 1, totals, 0.0), 1, keepdims=True) / model
    scale = lax.rsqrt(square - mean * mean + NORM_EPS)
    output[...] = ((pre_second - mean) * scale * second_gain[...]).astype(output.dtype)
    for copy in pending:
        copy.wait_send()


def mixer(
    mixed,
    tokens,
    routes,
    route_weights,
    first_gain,
    second_gain,
    side_switch,
    weights,
):
    out_w, gate_w, up_w, down_w, shared_gate, shared_up, shared_down, side_gate, side_up, side_down = weights
    eps, tps = lax.axis_size("ep"), lax.axis_size("tp")
    chips = eps // 2
    rows, model = tokens.shape
    cols = model // tps
    experts, _, hidden = gate_w.shape
    top = routes.shape[0]
    total = experts * eps
    capacity = (3 * rows * top + total - 1) // total
    slots = -(-experts * capacity // 16) * 16
    wide = -(-experts * rows // 128) * 128
    side_width, side_rows = side_gate.shape
    shared = shared_gate.shape[1]
    bf16, f32 = jnp.bfloat16, jnp.float32
    dma = pltpu.SemaphoreType.DMA
    return pl.pallas_call(
        functools.partial(mixer_body, (chips, tps, capacity)),
        out_shape=jax.ShapeDtypeStruct((rows, cols), bf16),
        in_specs=[VMEM] * 7 + [ANY] * 10,
        out_specs=VMEM,
        scratch_shapes=[
            pltpu.VMEM((tps,) + mixed.shape, bf16),
            pltpu.VMEM((eps, top, rows), jnp.int32),
            pltpu.VMEM((eps, top, rows), f32),
            pltpu.VMEM((eps, 2 * tps, rows, cols // 2), bf16),
            pltpu.VMEM((2 * rows, model), bf16),
            pltpu.VMEM((rows, model), bf16),
            pltpu.VMEM((128, wide), f32),
            pltpu.VMEM((wide, 128), f32),
            pltpu.VMEM((chips, tps, 2, slots, hidden), bf16),
            pltpu.VMEM((chips, rows, cols), bf16),
            pltpu.VMEM((chips, rows, cols), bf16),
            pltpu.VMEM((chips, rows, cols), bf16),
            pltpu.VMEM((chips, rows, cols), bf16),
            pltpu.VMEM((chips, rows, cols), f32),
            pltpu.VMEM((chips, 2, rows, 2 * side_width), bf16),
            pltpu.VMEM((chips, 2, rows, 2 * side_width), bf16),
            pltpu.VMEM((tps, rows, shared + 2 * side_width), bf16),
            pltpu.VMEM((tps, rows, 128), f32),
            pltpu.VMEM(out_w.shape, bf16),
            pltpu.VMEM((experts, model, 2 * hidden), bf16),
            pltpu.VMEM(down_w.shape, bf16),
            pltpu.VMEM((model, 2 * shared), bf16),
            pltpu.VMEM(shared_down.shape, bf16),
            pltpu.VMEM((2 * side_width, side_rows), bf16),
            pltpu.VMEM(side_down.shape, bf16),
            dma((2 * experts + 8,)),
            dma((2, tps - 1)),
            dma((2, eps - 1, 2)),
            dma((2, chips, 10)),
            dma((2, chips, tps - 1)),
            dma((2, chips, 2)),
            dma((2, chips, 2)),
            dma((2, tps - 1)),
            dma((2, tps - 1)),
        ],
        compiler_params=pltpu.CompilerParams(collective_id=0, has_side_effects=True),
    )(mixed, tokens, routes, route_weights, first_gain, second_gain, side_switch, *weights)


def streamed_device(
    tokens,
    retention_state,
    lengths,
    query_weight,
    key_weight,
    value_weight,
    gate_weight,
    out_weight,
    first_gain,
    routing,
    route_weight,
    expert_gate,
    expert_up,
    expert_down,
    shared_gate,
    shared_up,
    shared_down,
    side_gate,
    side_up,
    side_down,
    side_switch,
    second_gain,
):
    rows, heads, width = retention_state.shape[:3]
    exponent = np.arange(width // 2, dtype=np.float64) / (width // 2)
    frequency = np.tile((ROPE_BASE**-exponent).astype(np.float32), 2 * heads)[None, :]
    mixed, new_state = retain_kernel(
        tokens,
        lengths.reshape(1, rows),
        jnp.asarray(frequency),
        [query_weight, key_weight, value_weight, gate_weight],
        retention_state,
    )
    output = mixer(
        mixed,
        tokens,
        routing.T,
        route_weight.T,
        first_gain.reshape(1, -1),
        second_gain.reshape(1, -1),
        side_switch.reshape(1, -1),
        [
            out_weight,
            expert_gate,
            expert_up,
            expert_down,
            shared_gate,
            shared_up,
            shared_down,
            side_gate.T,
            side_up.T,
            side_down,
        ],
    )
    return (output, new_state)


def staged_device(
    tokens,
    retention_state,
    lengths,
    query_weight,
    key_weight,
    value_weight,
    gate_weight,
    out_weight,
    first_gain,
    routing,
    route_weight,
    expert_gate,
    expert_up,
    expert_down,
    shared_gate,
    shared_up,
    shared_down,
    side_gate,
    side_up,
    side_down,
    side_switch,
    second_gain,
):
    seq_rows = tokens.shape[0]
    model_width = tokens.shape[1]
    head_count = retention_state.shape[1]
    col_count = out_weight.shape[1]
    ep_count = lax.axis_size("ep")
    tp_rank = lax.axis_index("tp")
    ep_rank = lax.axis_index("ep")
    col_start = tp_rank * col_count
    side_width = side_gate.shape[1]
    side_part = jnp.concatenate([side_gate, side_up], 1)
    side_both, every_route, every_weight, *projections = first(
        [side_part, routing.T, route_weight.T],
        tokens,
        [query_weight, key_weight, value_weight, gate_weight],
        0,
    )
    side_both = side_both.reshape(model_width, 2 * side_width)
    mixed_heads, new_state = retain(
        retention_state, lengths, projections, tp_rank * head_count
    )
    (every_mixed,) = gather([mixed_heads], "tp", 1)
    mixing = jnp.dot(
        side_by_side(every_mixed),
        out_weight,
        preferred_element_type=jnp.float32,
    )
    own_cols = lax.dynamic_slice_in_dim(tokens, col_start, col_count, 1).astype(jnp.float32)
    pre_first = RESIDUAL_SCALE * own_cols + mixing
    first_sum, first_square = row_moments(pre_first, 2)
    row_mean = first_sum / model_width
    square = first_square / model_width
    own_gain = lax.dynamic_slice_in_dim(first_gain, col_start, col_count, 0)
    normed_cols = (
        (pre_first - row_mean) * lax.rsqrt(square - row_mean * row_mean + NORM_EPS) * own_gain
    ).astype(jnp.bfloat16)
    every_rows = spread(normed_cols, 3)
    normed_full = lax.dynamic_index_in_dim(every_rows, ep_rank, 0, keepdims=False)
    every_rows = every_rows.reshape(ep_count * seq_rows, model_width)

    local_experts = expert_gate.shape[0]
    top_count = routing.shape[1]
    expert_count = local_experts * ep_count
    capacity = (3 * seq_rows * top_count + expert_count - 1) // expert_count
    total_rows = ep_count * seq_rows
    route_all = jnp.transpose(every_route, (1, 0, 2)).reshape(top_count, total_rows)
    weight_all = jnp.transpose(every_weight, (1, 0, 2)).reshape(top_count, total_rows)
    local_ids = ep_rank * local_experts + jnp.arange(local_experts, dtype=jnp.int32)
    named = route_all[None, :, :] == local_ids[:, None, None]
    member = jnp.any(named, 1)
    pair_weight = jnp.sum(jnp.where(named, weight_all[None, :, :], 0.0), 1)
    index = jnp.arange(total_rows, dtype=jnp.int32)
    group = index // seq_rows
    earlier = ((index[:, None] < index[None, :]) & (group[:, None] == group[None, :])).astype(
        jnp.bfloat16
    )
    before = jnp.dot(
        member.astype(jnp.bfloat16), earlier, preferred_element_type=jnp.float32
    ).astype(jnp.int32)
    slot = jnp.where(member, group[None, :] * capacity + before, -1)
    slot_total = ep_count * capacity
    hit = slot[:, None, :] == jnp.arange(slot_total, dtype=jnp.int32)[None, :, None]
    table = hit.astype(jnp.bfloat16).reshape(local_experts * slot_total, total_rows)
    slot_weight = jnp.sum(jnp.where(hit, pair_weight[:, None, :], 0.0), -1, keepdims=True)
    chosen = (
        jnp.dot(table, every_rows, preferred_element_type=jnp.float32)
        .astype(jnp.bfloat16)
        .reshape(local_experts, slot_total, model_width)
    )
    gate_part = jnp.einsum("jcd,jdf->jcf", chosen, expert_gate, preferred_element_type=jnp.float32)
    up_part = jnp.einsum("jcd,jdf->jcf", chosen, expert_up, preferred_element_type=jnp.float32)
    hidden = (jax.nn.silu(gate_part) * up_part * slot_weight).astype(jnp.bfloat16)

    side_pre = jnp.dot(normed_full, side_both, preferred_element_type=jnp.float32)
    side_hidden = (jax.nn.silu(side_pre[:, :side_width]) * side_pre[:, side_width:]).astype(
        jnp.bfloat16
    )
    shared_hidden = (
        jax.nn.silu(jnp.dot(normed_full, shared_gate, preferred_element_type=jnp.float32))
        * jnp.dot(normed_full, shared_up, preferred_element_type=jnp.float32)
    ).astype(jnp.bfloat16)
    hidden_blocks, shared_blocks, side_blocks = gather(
        [hidden.reshape(local_experts * slot_total, -1), shared_hidden, side_hidden], "tp", 4
    )
    hidden_all = side_by_side(hidden_blocks).reshape(local_experts, slot_total, -1)
    result = (
        jnp.einsum("jcf,jfd->jcd", hidden_all, expert_down, preferred_element_type=jnp.float32)
        .astype(jnp.bfloat16)
        .reshape(local_experts * slot_total, col_count)
    )
    summed = (
        lax.dot_general(
            table, result, (((0,), (0,)), ((), ())), preferred_element_type=jnp.float32
        )
        .astype(jnp.bfloat16)
        .reshape(ep_count, seq_rows, col_count)
    )
    returned = scatter(summed, 5)
    routed = jnp.sum(returned.astype(jnp.float32), 0)
    shared_out = jnp.dot(
        side_by_side(shared_blocks), shared_down, preferred_element_type=jnp.float32
    )
    side_out = jnp.dot(side_by_side(side_blocks), side_down, preferred_element_type=jnp.float32)
    switch = jax.nn.sigmoid(
        jnp.sum(normed_full.astype(jnp.float32) * side_switch.astype(jnp.float32)[None, :], -1)
    )
    pre_second = (
        RESIDUAL_SCALE * normed_cols.astype(jnp.float32)
        + routed
        + shared_out
        + switch[:, None] * side_out
    )
    second_sum, second_square = row_moments(pre_second, 6)
    mean_second = second_sum / model_width
    square_second = second_square / model_width
    output = (
        (pre_second - mean_second)
        * lax.rsqrt(square_second - mean_second * mean_second + NORM_EPS)
        * second_gain
    ).astype(jnp.bfloat16)
    return (output, new_state)


def on_device(*arrays):
    tokens, state, expert_gate, side_gate = arrays[0], arrays[1], arrays[11], arrays[17]
    eps, tps = lax.axis_size("ep"), lax.axis_size("tp")
    rows, model = tokens.shape
    fits = (
        eps == 8
        and tps == 4
        and rows % 16 == 0
        and model % (256 * tps) == 0
        and state.shape[1] * state.shape[2] % 128 == 0
        and expert_gate.shape[2] % 128 == 0
        and side_gate.shape[0] % 128 == 0
        and side_gate.shape[1] == 64
    )
    return (streamed_device if fits else staged_device)(*arrays)


def solution(mesh):
    return jax.shard_map(
        on_device,
        mesh=mesh,
        in_specs=(
            P("ep", None),
            P("ep", "tp", None, None),
            P("ep"),
            P(None, "tp"),
            P(None, "tp"),
            P(None, "tp"),
            P(None, "tp"),
            P(None, "tp"),
            P(),
            P("ep", None),
            P("ep", None),
            P("ep", None, "tp"),
            P("ep", None, "tp"),
            P("ep", None, "tp"),
            P(None, "tp"),
            P(None, "tp"),
            P(None, "tp"),
            P("ep", "tp"),
            P("ep", "tp"),
            P(None, "tp"),
            P(),
            P("tp"),
        ),
        out_specs=(P("ep", "tp"), P("ep", "tp", None, None)),
        check_vma=False,
    )
```

```python
import functools

import jax
import jax.numpy as jnp
import numpy as np
from jax import lax
from jax.experimental import pallas as pl
from jax.experimental.pallas import tpu as pltpu
from jax.sharding import PartitionSpec as P

HEADS = 16


RESIDUAL_SCALE = 2.0**0.25
NORM_EPS = 1e-05
GROUP_EPS = 1e-06
ROPE_BASE = 10000.0


def rotate(vector, positions):
    half_width = vector.shape[-1] // 2
    frequency = ROPE_BASE ** (-jnp.arange(half_width, dtype=jnp.float32) / half_width)
    angles = positions.astype(jnp.float32)[:, None, None] * frequency[None, None, :]
    cosine = jnp.cos(angles)
    sine_part = jnp.sin(angles)
    first_half = vector[..., :half_width]
    second_half = vector[..., half_width:]
    return jnp.concatenate(
        [
            first_half * cosine - second_half * sine_part,
            second_half * cosine + first_half * sine_part,
        ],
        -1,
    )


def retain(
    retention_state,
    lengths,
    projections,
    first_head,
):
    row_count = retention_state.shape[0]
    head_count = retention_state.shape[1]
    head_width = retention_state.shape[2]

    query_rows, key_part, value_part, gate_part = [part.astype(jnp.float32) for part in projections]
    queries = rotate(query_rows.reshape(row_count, head_count, head_width), lengths)
    key_rows = rotate(
        key_part.reshape(row_count, head_count, head_width), lengths
    ) * head_width ** (-0.5)
    values = value_part.reshape(row_count, head_count, head_width)
    gate_act = gate_part
    head_index = (first_head + jnp.arange(head_count)).astype(jnp.float32)
    decays = 1.0 - 2.0 ** (-5.0 - 7.0 * head_index / (HEADS - 1))
    own_term = jnp.sum(queries * key_rows, -1, keepdims=True) * values
    carried = decays[None, :, None] * jnp.sum(queries[:, :, :, None] * retention_state, 2)
    result = own_term + carried
    new_state = (
        decays[None, :, None, None] * retention_state
        + key_rows[:, :, :, None] * values[:, :, None, :]
    )
    normed = result * lax.rsqrt(jnp.mean(result * result, -1, keepdims=True) + GROUP_EPS)
    mixed_heads = (
        normed.reshape(row_count, head_count * head_width) * jax.nn.silu(gate_act)
    ).astype(jnp.bfloat16)
    return (mixed_heads, new_state)


VMEM = pl.BlockSpec(memory_space=pltpu.VMEM)
DEVICE = pl.DeviceIdType.MESH


def enter(peers):
    barrier = pltpu.get_barrier_semaphore()
    for peer in peers:
        pl.semaphore_signal(barrier, inc=1, device_id=peer, device_id_type=DEVICE)
    pl.semaphore_wait(barrier, len(peers))


def send(source, target, send_sem, recv_sem, peer):
    copy = pltpu.make_async_remote_copy(
        src_ref=source,
        dst_ref=target,
        send_sem=send_sem,
        recv_sem=recv_sem,
        device_id=peer,
        device_id_type=DEVICE,
    )
    copy.start()
    return copy


def on_axis(axis, index):
    if axis == "ep":
        return (index, lax.axis_index("tp"))
    return (lax.axis_index("ep"), index)


def gather_body(axis, count, parts, *refs):
    sources, targets = refs[:parts], refs[parts : 2 * parts]
    send_sem, recv_sem, local_sem = refs[2 * parts :]
    me = lax.axis_index(axis)
    others = [lax.rem(me + step, count) for step in range(1, count)]
    locals_ = []
    for part in range(parts):
        own = pltpu.make_async_copy(sources[part], targets[part].at[me], local_sem.at[part])
        own.start()
        locals_.append(own)
    enter([on_axis(axis, other) for other in others])
    copies = []
    for step, other in enumerate(others):
        for part in range(parts):
            copies.append(
                send(
                    sources[part],
                    targets[part].at[me],
                    send_sem.at[step, part],
                    recv_sem.at[step, part],
                    on_axis(axis, other),
                )
            )
    for copy in locals_:
        copy.wait()
    for copy in copies:
        copy.wait()


def gather(arrays, axis, ident):
    count, parts = lax.axis_size(axis), len(arrays)
    return pl.pallas_call(
        functools.partial(gather_body, axis, count, parts),
        out_shape=[jax.ShapeDtypeStruct((count,) + a.shape, a.dtype) for a in arrays],
        in_specs=[VMEM] * parts,
        out_specs=[VMEM] * parts,
        scratch_shapes=[
            pltpu.SemaphoreType.DMA((count - 1, parts)),
            pltpu.SemaphoreType.DMA((count - 1, parts)),
            pltpu.SemaphoreType.DMA((parts,)),
        ],
        compiler_params=pltpu.CompilerParams(collective_id=ident, has_side_effects=True),
    )(*arrays)


def scatter_body(count, source, target, send_sem, recv_sem, local_sem):
    me = lax.axis_index("ep")
    others = [lax.rem(me + step, count) for step in range(1, count)]
    own = pltpu.make_async_copy(source.at[me], target.at[me], local_sem)
    own.start()
    enter([on_axis("ep", other) for other in others])
    copies = [
        send(
            source.at[other],
            target.at[me],
            send_sem.at[step],
            recv_sem.at[step],
            on_axis("ep", other),
        )
        for step, other in enumerate(others)
    ]
    own.wait()
    for copy in copies:
        copy.wait()


def scatter(array, ident):
    count = array.shape[0]
    return pl.pallas_call(
        functools.partial(scatter_body, count),
        out_shape=jax.ShapeDtypeStruct(array.shape, array.dtype),
        in_specs=[VMEM],
        out_specs=VMEM,
        scratch_shapes=[
            pltpu.SemaphoreType.DMA((count - 1,)),
            pltpu.SemaphoreType.DMA((count - 1,)),
            pltpu.SemaphoreType.DMA,
        ],
        compiler_params=pltpu.CompilerParams(collective_id=ident, has_side_effects=True),
    )(array)


def first_body(count, *refs):
    parts = 3
    sources, (tokens, *weights) = refs[:parts], refs[parts : parts + 5]
    targets = refs[parts + 5 : 2 * parts + 5]
    results = refs[2 * parts + 5 : 2 * parts + 9]
    send_sem, recv_sem, local_sem = refs[2 * parts + 9 :]
    chips = count // 2
    me = lax.axis_index("ep")
    chip, core = me // 2, lax.rem(me, 2)
    partner = on_axis("ep", chip * 2 + 1 - core)
    line = [lax.rem(chip + step, chips) * 2 + core for step in range(1, chips)]
    senders = [lax.rem(chip + chips - step, chips) * 2 + core for step in range(1, chips)]
    locals_ = []
    for part in range(parts):
        own = pltpu.make_async_copy(sources[part], targets[part].at[me], local_sem.at[part])
        own.start()
        locals_.append(own)
    enter([on_axis("ep", other) for other in line] + [partner])
    direct, copies = [], []
    for step, other in enumerate(line):
        for part in range(parts):
            direct.append(
                send(
                    sources[part],
                    targets[part].at[me],
                    send_sem.at[step, part],
                    recv_sem.at[step, part],
                    on_axis("ep", other),
                )
            )
    for part in range(parts):
        copies.append(
            send(
                sources[part],
                targets[part].at[me],
                send_sem.at[chips - 1, part],
                recv_sem.at[chips - 1, part],
                partner,
            )
        )
    for weight, result in zip(weights, results):
        result[...] = jnp.dot(
            tokens[...], weight[...], preferred_element_type=jnp.float32
        ).astype(result.dtype)
    for step, sender in enumerate(senders):
        for part in range(parts):
            direct[step * parts + part].wait_recv()
            copies.append(
                send(
                    targets[part].at[sender],
                    targets[part].at[sender],
                    send_sem.at[chips + step, part],
                    recv_sem.at[chips + step, part],
                    partner,
                )
            )
    for copy in locals_:
        copy.wait()
    for copy in direct:
        copy.wait_send()
    for copy in copies:
        copy.wait()


def first(arrays, tokens, weights, ident):
    count, parts = lax.axis_size("ep"), len(arrays)
    rows = tokens.shape[0]
    return pl.pallas_call(
        functools.partial(first_body, count),
        out_shape=[jax.ShapeDtypeStruct((count,) + a.shape, a.dtype) for a in arrays]
        + [jax.ShapeDtypeStruct((rows, w.shape[1]), jnp.bfloat16) for w in weights],
        in_specs=[VMEM] * (parts + 5),
        out_specs=[VMEM] * (parts + 4),
        scratch_shapes=[
            pltpu.SemaphoreType.DMA((count - 1, parts)),
            pltpu.SemaphoreType.DMA((count - 1, parts)),
            pltpu.SemaphoreType.DMA((parts,)),
        ],
        compiler_params=pltpu.CompilerParams(collective_id=ident, has_side_effects=True),
    )(*arrays, tokens, *weights)


def spread_body(count, tp_count, source, target, send_sem, recv_sem, local_sem):
    chips, width = count // 2, source.shape[1]
    me, own_tp = lax.axis_index("ep"), lax.axis_index("tp")
    chip, core = me // 2, lax.rem(me, 2)
    partner = (chip * 2 + 1 - core, own_tp)

    def place(row, col):
        return target.at[row, :, pl.ds(pl.multiple_of(col * width, width), width)]

    def chip_at(step):
        return lax.rem(chip + chips + step, chips) * 2 + core

    def tp_at(step):
        return lax.rem(own_tp + tp_count + step, tp_count)

    own = pltpu.make_async_copy(source, place(me, own_tp), local_sem)
    own.start()
    line = [(chip_at(step), own_tp) for step in range(1, chips)]
    plane = [(me, tp_at(step)) for step in range(1, tp_count)]
    enter(line + plane + [partner])

    def pair(line_step, plane_step, to_partner):
        return (
            send_sem.at[to_partner, line_step, plane_step],
            recv_sem.at[to_partner, line_step, plane_step],
        )

    direct, planar, copies = [], {}, []
    for step in range(1, chips):
        direct.append(send(source, place(me, own_tp), *pair(step, 0, 0), line[step - 1]))
    for step in range(1, tp_count):
        planar[(0, step)] = send(source, place(me, own_tp), *pair(0, step, 0), plane[step - 1])
    copies.append(send(source, place(me, own_tp), *pair(0, 0, 1), partner))
    for line_step in range(1, chips):
        direct[line_step - 1].wait_recv()
        block = place(chip_at(-line_step), own_tp)
        for step in range(1, tp_count):
            planar[(line_step, step)] = send(
                block, block, *pair(line_step, step, 0), plane[step - 1]
            )
        copies.append(send(block, block, *pair(line_step, 0, 1), partner))
    for line_step in range(chips):
        for step in range(1, tp_count):
            planar[(line_step, step)].wait_recv()
            block = place(chip_at(-line_step), tp_at(-step))
            copies.append(send(block, block, *pair(line_step, step, 1), partner))
    own.wait()
    for copy in direct:
        copy.wait_send()
    for copy in planar.values():
        copy.wait_send()
    for copy in copies:
        copy.wait()


def spread(block, ident):
    count, tp_count = lax.axis_size("ep"), lax.axis_size("tp")
    rows, width = block.shape
    return pl.pallas_call(
        functools.partial(spread_body, count, tp_count),
        out_shape=jax.ShapeDtypeStruct((count, rows, width * tp_count), block.dtype),
        in_specs=[VMEM],
        out_specs=VMEM,
        scratch_shapes=[
            pltpu.SemaphoreType.DMA((2, count // 2, tp_count)),
            pltpu.SemaphoreType.DMA((2, count // 2, tp_count)),
            pltpu.SemaphoreType.DMA,
        ],
        compiler_params=pltpu.CompilerParams(collective_id=ident, has_side_effects=True),
    )(block)


def side_by_side(gathered):
    return jnp.concatenate([gathered[i] for i in range(gathered.shape[0])], -1)


def row_moments(values, ident):
    sums = jnp.stack([jnp.sum(values, -1), jnp.sum(values * values, -1)])
    (every,) = gather([sums], "tp", ident)
    totals = jnp.sum(every, 0)
    return totals[0][:, None], totals[1][:, None]


ANY = pl.BlockSpec(memory_space=pl.ANY)


def dot(a, b):
    return jnp.dot(a, b, preferred_element_type=jnp.float32)


def silu(x):
    return x / (1.0 + jnp.exp(-x))


def fetch(source, target, sem):
    copy = pltpu.make_async_copy(source, target, sem)
    copy.start()
    return copy


def settle(ref, sem):
    pltpu.make_async_copy(ref, ref, sem).wait()


def on_diagonal(rows):
    row = lax.broadcasted_iota(jnp.int32, (rows, rows), 0)
    return row == lax.broadcasted_iota(jnp.int32, (rows, rows), 1)


def column_of(line):
    return jnp.sum(jnp.where(on_diagonal(line.shape[1]), line, 0.0), 1, keepdims=True)


def line_of(column):
    return jnp.sum(jnp.where(on_diagonal(column.shape[0]), column, 0.0), 0, keepdims=True)


def rotated(x, cosine, sine, half):
    width = x.shape[1]
    lane = lax.broadcasted_iota(jnp.int32, x.shape, 1)
    first = (lane & (2 * half - 1)) < half
    later = pltpu.roll(x, width - half, 1)
    sooner = pltpu.roll(x, half, 1)
    return x * cosine + jnp.where(first, -later, sooner) * sine


def retain_body(
    chunk,
    tokens_in,
    lengths_in,
    frequency_in,
    query_in,
    key_in,
    value_in,
    gate_in,
    state_in,
    mixed,
    state_out,
    tokens,
    lengths,
    frequency,
    weights,
    state,
    columns,
    spread_even,
    spread_odd,
    values,
    carried,
    small_sem,
    weight_sem,
    state_sem,
    out_sem,
):
    rows, heads, width = state.shape[0], state.shape[1], state.shape[2]
    total = heads * width
    chunks = rows // chunk
    small = [
        fetch(source, target, small_sem.at[i])
        for i, (source, target) in enumerate(
            [(lengths_in, lengths), (frequency_in, frequency), (tokens_in, tokens)]
        )
    ]
    for i, source in enumerate([query_in, key_in, value_in, gate_in]):
        fetch(source, weights.at[:, pl.ds(i * total, total)], weight_sem.at[i // 2])
    for i in range(chunks):
        piece = pl.ds(i * chunk, chunk)
        fetch(state_in.at[piece], state.at[piece], state_sem.at[i])

    with jax.named_scope("small_wait"):
        small[0].wait()
        small[1].wait()
    position = column_of(lengths[...].astype(jnp.float32))
    angles = position * frequency[...]
    cosine, sine = jnp.cos(angles), jnp.sin(angles)
    first_head = lax.axis_index("tp") * heads
    decays = []
    for head in range(heads):
        index = jnp.full((1, width), first_head + head, jnp.int32).astype(jnp.float32)
        decays.append(1.0 - jnp.exp2(-5.0 - 7.0 * index / (HEADS - 1)))

    def project(i):
        span = pl.ds(2 * i * total, 2 * total)
        with jax.named_scope("weight_wait"):
            settle(weights.at[:, span], weight_sem.at[i])
        both = dot(tokens[...], weights[:, span]).astype(jnp.bfloat16).astype(jnp.float32)
        return both[:, :total], both[:, total:]

    with jax.named_scope("small_wait"):
        small[2].wait()
    query, key = project(0)
    lanes = columns.shape[1] // 2
    for i, (x, scale) in enumerate([(query, 1.0), (key, width ** (-0.5))]):
        turned = rotated(x, cosine, sine, width // 2) * scale
        padded = jnp.concatenate([turned, jnp.zeros((lanes - rows, total), jnp.float32)], 0)
        flipped = jnp.transpose(padded)
        high = flipped.astype(jnp.bfloat16)
        columns[i * total : (i + 1) * total, :lanes] = high
        columns[i * total : (i + 1) * total, lanes:] = (
            flipped - high.astype(jnp.float32)
        ).astype(jnp.bfloat16)
    value, gate = project(1)
    for head in range(heads):
        values[head] = value[:, head * width : (head + 1) * width]

    source_lane = lax.broadcasted_iota(jnp.int32, (2 * lanes, 2 * lanes), 0) & (lanes - 1)
    target_lane = lax.broadcasted_iota(jnp.int32, (2 * lanes, 2 * lanes), 1)
    offset = jnp.where(target_lane >= lanes, 1, 0)
    buffers = [spread_even, spread_odd]

    def widen(i):
        for pair in range(chunk // 2):
            pick = jnp.where(source_lane == offset + (i * chunk + 2 * pair), 1.0, 0.0)
            buffers[i % 2][pair] = dot(columns[...], pick.astype(jnp.bfloat16))

    widen(0)
    for i in range(chunks):
        base = i * chunk
        piece = pl.ds(base, chunk)
        with jax.named_scope("state_wait"):
            pltpu.make_async_copy(state_in.at[piece], state.at[piece], state_sem.at[i]).wait()
        if i + 1 < chunks:
            widen(i + 1)
        wide = buffers[i % 2]
        for at in range(chunk):
            lane = (at % 2) * lanes
            for head in range(heads):
                low, high = head * width, (head + 1) * width
                q_cols = wide[at // 2, low:high, lane : lane + width]
                k_cols = wide[at // 2, total + low : total + high, lane : lane + width]
                v_row = values[head, base + at : base + at + 1, :]
                new = decays[head] * state[base + at, head] + k_cols * v_row
                state[base + at, head] = new
                carried[head, base + at : base + at + 1, :] = jnp.sum(
                    q_cols * new, 0, keepdims=True
                )
        fetch(state.at[piece], state_out.at[piece], out_sem)
    parts = []
    for head in range(heads):
        result = carried[head]
        scale = lax.rsqrt(jnp.mean(result * result, -1, keepdims=True) + GROUP_EPS)
        parts.append(result * scale)
    mixed[...] = (jnp.concatenate(parts, 1) * silu(gate)).astype(mixed.dtype)
    with jax.named_scope("state_drain"):
        settle(state, out_sem)


def retain_kernel(tokens, lengths, frequency, weights, state):
    rows, heads, width = state.shape[0], state.shape[1], state.shape[2]
    chunk, lanes = 8, 128
    cols = heads * width
    wide = pltpu.VMEM((chunk // 2, 2 * cols, 2 * lanes), jnp.float32)
    return pl.pallas_call(
        functools.partial(retain_body, chunk),
        out_shape=[
            jax.ShapeDtypeStruct((rows, cols), jnp.bfloat16),
            jax.ShapeDtypeStruct(state.shape, state.dtype),
        ],
        in_specs=[ANY] * 8,
        out_specs=[VMEM, ANY],
        scratch_shapes=[
            pltpu.VMEM(tokens.shape, tokens.dtype),
            pltpu.VMEM(lengths.shape, lengths.dtype),
            pltpu.VMEM(frequency.shape, frequency.dtype),
            pltpu.VMEM((tokens.shape[1], 4 * cols), jnp.bfloat16),
            pltpu.VMEM(state.shape, state.dtype),
            pltpu.VMEM((2 * cols, 2 * lanes), jnp.bfloat16),
            wide,
            wide,
            pltpu.VMEM((heads, rows, width), jnp.float32),
            pltpu.VMEM((heads, rows, width), jnp.float32),
            pltpu.SemaphoreType.DMA((3,)),
            pltpu.SemaphoreType.DMA((2,)),
            pltpu.SemaphoreType.DMA((rows // chunk,)),
            pltpu.SemaphoreType.DMA,
        ],
    )(tokens, lengths, frequency, *weights, state)


def mixer_body(
    dims,
    mixed_in,
    tokens_in,
    routes_in,
    route_weights_in,
    first_gain_in,
    side_switch_in,
    out_in,
    gate_in,
    up_in,
    down_in,
    shared_gate_in,
    shared_up_in,
    shared_down_in,
    side_gate_in,
    side_up_in,
    side_down_in,
    output,
    own_tokens,
    first_gain,
    side_switch,
    mixed_all,
    route_all,
    weight_all,
    rows_all,
    normed,
    info,
    info_cols,
    hidden_all,
    pair_out,
    pair_in,
    line_out,
    line_in,
    total,
    side_out,
    side_in,
    late_all,
    stats,
    out_w,
    gate_up_w,
    down_w,
    shared_w,
    shared_down_w,
    side_w,
    side_down_w,
    small_sem,
    weight_sem,
    send_sem,
    recv_sem,
    row_sem,
    back_sem,
):
    chips, tps, capacity = dims
    steps = chips
    rows, cols = own_tokens.shape
    model = cols * tps
    half = cols // 2
    experts, hidden_width = gate_in.shape[0], gate_in.shape[2]
    slots = hidden_all.shape[3]
    side_width = side_gate_in.shape[0]
    side_rows = side_gate_in.shape[1]
    shared_width = shared_gate_in.shape[1]
    tp = lax.axis_index("tp")
    ep = lax.axis_index("ep")
    eps = 2 * chips
    chip, core = ep // 2, lax.rem(ep, 2)
    partner = (chip * 2 + 1 - core, tp)
    low, high = lax.rem(tp, 2), tp // 2
    tp_x = high * 2 + 1 - low
    tp_y = (1 - high) * 2 + low
    tp_d = (1 - high) * 2 + 1 - low
    plane = [(ep, tp_x), (ep, tp_y), (ep, tp_d)]

    def chip_at(step):
        if step == 0:
            return chip
        if step == 1:
            return chip + 1 - 2 * lax.rem(chip, 2)
        if step == 2:
            return lax.rem(chip + 2, 4)
        return 3 - chip

    def group_at(step, at):
        return chip_at(step) * 2 + (core if at == 0 else 1 - core)

    line = [(group_at(step, 0), tp) for step in range(steps)]
    others = [(group_at(s, at), tp) for s in range(steps) for at in range(2) if s + at > 0]
    peers = plane + others
    barrier = pltpu.get_barrier_semaphore()
    for peer in peers:
        pl.semaphore_signal(barrier, inc=1, device_id=peer, device_id_type=DEVICE)

    own_mixed = mixed_all.at[tp]
    own_slice = pl.ds(pl.multiple_of(tp * cols, cols), cols)
    fetch(mixed_in, own_mixed, small_sem.at[0])
    fetch(routes_in, route_all.at[ep], small_sem.at[1])
    fetch(route_weights_in, weight_all.at[ep], small_sem.at[2])
    fetch(tokens_in.at[:, own_slice], own_tokens, small_sem.at[3])
    fetch(out_in, out_w, weight_sem.at[0])
    fetch(first_gain_in, first_gain, small_sem.at[4])
    fetch(side_switch_in, side_switch, small_sem.at[5])
    for e in range(experts):
        fetch(gate_in.at[e], gate_up_w.at[e, :, pl.ds(0, hidden_width)], weight_sem.at[1])
        fetch(up_in.at[e], gate_up_w.at[e, :, pl.ds(hidden_width, hidden_width)], weight_sem.at[1])
    fetch(side_gate_in, side_w.at[pl.ds(0, side_width)], weight_sem.at[2])
    fetch(side_up_in, side_w.at[pl.ds(side_width, side_width)], weight_sem.at[2])
    fetch(shared_gate_in, shared_w.at[:, pl.ds(0, shared_width)], weight_sem.at[3])
    fetch(shared_up_in, shared_w.at[:, pl.ds(shared_width, shared_width)], weight_sem.at[3])
    fetch(down_in, down_w, weight_sem.at[4])
    fetch(shared_down_in, shared_down_w, weight_sem.at[5])
    fetch(side_down_in, side_down_w, weight_sem.at[6])

    MIXED, ROUTE, WEIGHT, SIDE, LATE, STAT, HIDDEN = 0, 1, 2, 3, 4, 5, 6

    def push(source, target, sent, received, peer):
        send(source, target, sent, received, peer)

    with jax.named_scope("small_wait"):
        settle(own_mixed, small_sem.at[0])
        settle(route_all.at[ep], small_sem.at[1])
        settle(weight_all.at[ep], small_sem.at[2])
    with jax.named_scope("enter"):
        pl.semaphore_wait(barrier, len(peers))

    for peer in plane:
        push(own_mixed, own_mixed, send_sem.at[MIXED], recv_sem.at[MIXED], peer)
    for peer in others:
        own = route_all.at[ep]
        push(own, own, send_sem.at[ROUTE], recv_sem.at[ROUTE], peer)
        own = weight_all.at[ep]
        push(own, own, send_sem.at[WEIGHT], recv_sem.at[WEIGHT], peer)

    with jax.named_scope("out_wait"):
        settle(own_tokens, small_sem.at[3])
        settle(out_w, weight_sem.at[0])
    with jax.named_scope("mixed_wait"):
        settle(mixed_all.at[pl.ds(0, tps - 1)], recv_sem.at[MIXED])
    heads_all = jnp.concatenate([mixed_all[t] for t in range(tps)], 1)
    pre_first = RESIDUAL_SCALE * own_tokens[...].astype(jnp.float32) + dot(heads_all, out_w[...])
    for part in range(2):
        rows_all[ep, 2 * tp + part] = pre_first[:, part * half : (part + 1) * half].astype(
            jnp.bfloat16
        )

    def block(step, index):
        return rows_all.at[group_at(step, 0), pl.ds(2 * index, 2)]

    def piece(step, index, part):
        return rows_all.at[group_at(step, 0), 2 * index + part]

    def push_rows(ref, step, kind, peer):
        sent = send_sem.at[8] if kind == 5 else send_sem.at[7]
        push(ref, ref, sent, row_sem.at[step, kind], peer)

    def came(ref, step, kind):
        settle(ref, row_sem.at[step, kind])

    def spread(step):
        ref = block(step, tp)
        if step > 0:
            came(ref, step, 0)
        push_rows(ref, step, 1, plane[0])
        push_rows(ref, step, 2, plane[1])
        push_rows(ref, step, 5, partner)

    def relay(step):
        came(block(step, tp_x), step, 1)
        push_rows(piece(step, tp_x, 0), step, 3, plane[1])
        push_rows(block(step, tp_x), step, 5, partner)
        came(block(step, tp_y), step, 2)
        push_rows(piece(step, tp_y, 1), step, 4, plane[0])
        push_rows(block(step, tp_y), step, 5, partner)

    def corner(step):
        for part in range(2):
            came(piece(step, tp_d, part), step, 3 + part)
            push_rows(piece(step, tp_d, part), step, 5, partner)

    def arrive(step):
        came(rows_all.at[group_at(step, 1)], step, 5)

    with jax.named_scope("spread0"):
        spread(0)
        for step in range(1, steps):
            push_rows_to = line[step]
            push(block(0, tp), block(0, tp), send_sem.at[7], row_sem.at[step, 0], push_rows_to)

    with jax.named_scope("route_wait"):
        settle(route_all.at[pl.ds(0, eps - 1)], recv_sem.at[ROUTE])
        settle(weight_all.at[pl.ds(0, eps - 1)], recv_sem.at[WEIGHT])
    wide = experts * rows

    def expert_of(index):
        return sum(jnp.where(index >= e * rows, 1, 0) for e in range(1, experts))

    group_lane = expert_of(lax.broadcasted_iota(jnp.int32, (1, wide), 1))
    expert_lane = ep * experts + group_lane
    info[...] = jnp.zeros_like(info)
    for g in range(eps):
        ids = jnp.concatenate([route_all[g]] * experts, 1)
        hits = ids == expert_lane
        scales = jnp.concatenate([weight_all[g]] * experts, 1)
        info[g : g + 1, 0:wide] = jnp.sum(jnp.where(hits, 1.0, 0.0), 0, keepdims=True)
        info[eps + g : eps + g + 1, 0:wide] = jnp.sum(
            jnp.where(hits, scales, 0.0), 0, keepdims=True
        )
    member = info[0:eps, 0:wide]
    sooner = lax.broadcasted_iota(jnp.int32, (wide, wide), 0)
    later = lax.broadcasted_iota(jnp.int32, (wide, wide), 1)
    earlier = jnp.where(
        (sooner < later) & (expert_of(sooner) == expert_of(later)), 1.0, 0.0
    ).astype(jnp.bfloat16)
    before = dot(member.astype(jnp.bfloat16), earlier)
    start = (group_lane * capacity).astype(jnp.float32)
    info[0:eps, 0:wide] = jnp.where(member > 0.5, before + start, -1.0)
    info_cols[...] = jnp.transpose(info[...])
    settle(first_gain, small_sem.at[4])

    def column(index):
        lane = lax.broadcasted_iota(jnp.int32, (wide, info_cols.shape[1]), 1)
        picked = jnp.where(lane == index, info_cols[0:wide, :], 0.0)
        return jnp.sum(picked, 1, keepdims=True)

    side_span = pl.ds(pl.multiple_of(ep * side_rows, side_rows), side_rows)

    def blocks(group):
        return [(step, at) for step in (2 * group, 2 * group + 1) for at in range(2)]

    def norm_step(step, at):
        g, base = group_at(step, at), (2 * step + at) * rows
        sums = jnp.zeros((rows, half), jnp.float32)
        squares = jnp.zeros((rows, half), jnp.float32)
        for part in range(2 * tps):
            x = rows_all[g, part].astype(jnp.float32)
            sums = sums + x
            squares = squares + x * x
        mean = jnp.sum(sums, 1, keepdims=True) / model
        square = jnp.sum(squares, 1, keepdims=True) / model
        scale = lax.rsqrt(square - mean * mean + NORM_EPS)
        for part in range(2 * tps):
            span = slice(part * half, (part + 1) * half)
            x = rows_all[g, part].astype(jnp.float32)
            y = (x - mean) * scale * first_gain[:, span]
            normed[base : base + rows, span] = y.astype(jnp.bfloat16)

    def side_step(group):
        if group == 0:
            settle(side_w, weight_sem.at[2])
        first = 4 * group * rows
        partial = lax.dot_general(
            normed[first : first + 4 * rows, side_span],
            side_w[...],
            (((1,), (1,)), ((), ())),
            preferred_element_type=jnp.float32,
        ).astype(jnp.bfloat16)
        for i, (step, at) in enumerate(blocks(group)):
            n = 2 * step + at
            side_out[n] = partial[i * rows : (i + 1) * rows]
            if n > 0:
                peer = (group_at(step, at), tp)
                push(
                    side_out.at[n],
                    side_in.at[n],
                    send_sem.at[SIDE],
                    recv_sem.at[SIDE],
                    peer,
                )

    def expert_step(group):
        if group == 0:
            settle(gate_up_w, weight_sem.at[1])
        first = 4 * group * rows
        stacks = [[] for _ in range(4)]
        scales = [column(eps + group_at(step, at)) for step, at in blocks(group)]
        for e in range(experts):
            both = dot(normed[first : first + 4 * rows, :], gate_up_w[e])
            hidden = silu(both[:, :hidden_width]) * both[:, hidden_width:]
            for i in range(4):
                mine = hidden[i * rows : (i + 1) * rows] * scales[i][e * rows : (e + 1) * rows]
                stacks[i].append(mine.astype(jnp.bfloat16))
        for i, (step, at) in enumerate(blocks(group)):
            slot_row = info[pl.ds(group_at(step, at), 1), 0:wide]
            number = lax.broadcasted_iota(jnp.int32, (slots, wide), 0).astype(jnp.float32)
            table = jnp.where(number == slot_row, 1.0, 0.0).astype(jnp.bfloat16)
            packed = dot(table, jnp.concatenate(stacks[i], 0)).astype(jnp.bfloat16)
            hidden_all[group, tp, i] = packed
        own = hidden_all.at[group, tp]
        for peer in plane:
            push(own, own, send_sem.at[HIDDEN], recv_sem.at[HIDDEN + group], peer)

    def down_step(group):
        with jax.named_scope("hidden_wait"):
            settle(hidden_all.at[group, pl.ds(0, tps - 1)], recv_sem.at[HIDDEN + group])
        if group == 0:
            settle(down_w, weight_sem.at[4])
        spread_rows = []
        for i, (step, at) in enumerate(blocks(group)):
            number = lax.broadcasted_iota(jnp.int32, (wide, slots), 1).astype(jnp.float32)
            table = jnp.where(number == column(group_at(step, at)), 1.0, 0.0).astype(jnp.bfloat16)
            packed = jnp.concatenate([hidden_all[group, t, i] for t in range(tps)], 1)
            spread_rows.append(dot(table, packed).astype(jnp.bfloat16))
        result = None
        for e in range(experts):
            mine = jnp.concatenate([r[e * rows : (e + 1) * rows] for r in spread_rows], 0)
            term = dot(mine, down_w[e])
            result = term if result is None else result + term
        for i, (step, at) in enumerate(blocks(group)):
            part = result[i * rows : (i + 1) * rows]
            if at == 0:
                total[step] = part
            else:
                pair_out[step] = part.astype(jnp.bfloat16)
        both = pl.ds(2 * group, 2)
        push(
            pair_out.at[both],
            pair_in.at[both],
            send_sem.at[9],
            back_sem.at[group],
            partner,
        )

    def return_step(group):
        both = pl.ds(2 * group, 2)
        with jax.named_scope("pair_wait"):
            settle(pair_in.at[both], back_sem.at[group])
        for step in (2 * group, 2 * group + 1):
            mine = total[step] + pair_in[step].astype(jnp.float32)
            if step == 0:
                total[step] = mine
                continue
            line_out[step] = mine.astype(jnp.bfloat16)
            push(
                line_out.at[step],
                line_in.at[step],
                send_sem.at[10],
                back_sem.at[1 + step],
                line[step],
            )

    def own_shared():
        settle(shared_w, weight_sem.at[3])
        both = dot(normed[0:rows, :], shared_w[...])
        hidden = silu(both[:, :shared_width]) * both[:, shared_width:]
        late_all[tp, :, 0:shared_width] = hidden.astype(jnp.bfloat16)

    def own_side():
        with jax.named_scope("side_wait"):
            settle(side_in.at[pl.ds(0, eps - 1)], recv_sem.at[SIDE])
        pre = side_out[0].astype(jnp.float32)
        for n in range(1, eps):
            pre = pre + side_in[n].astype(jnp.float32)
        act = silu(pre[:, :side_width]) * pre[:, side_width:]
        act = jnp.concatenate([act, jnp.zeros_like(act)], 1)
        late_all[tp, :, shared_width : shared_width + 2 * side_width] = act.astype(jnp.bfloat16)
        for peer in plane:
            push(late_all.at[tp], late_all.at[tp], send_sem.at[LATE], recv_sem.at[LATE], peer)

    def own_switch():
        settle(side_switch, small_sem.at[5])
        row = side_switch[...].astype(jnp.float32)
        product = normed[0:rows, :].astype(jnp.float32) * row
        logit = jnp.sum(product, 1, keepdims=True)
        return 1.0 / (1.0 + jnp.exp(-logit))

    def own_extra():
        settle(shared_down_w, weight_sem.at[5])
        settle(side_down_w, weight_sem.at[6])
        with jax.named_scope("late_wait"):
            settle(late_all.at[pl.ds(0, tps - 1)], recv_sem.at[LATE])
        shared = jnp.concatenate([late_all[t, :, :shared_width] for t in range(tps)], 1)
        shared = dot(shared, shared_down_w[...])
        side = None
        for t in range(tps):
            mine = late_all[t, :, shared_width : shared_width + side_width]
            term = dot(mine, side_down_w[t * side_width : (t + 1) * side_width, :])
            side = term if side is None else side + term
        return shared + switch * side

    with jax.named_scope("relay0"):
        relay(0)
    with jax.named_scope("spread1"):
        spread(1)
    with jax.named_scope("spread2"):
        spread(2)
    with jax.named_scope("corner0"):
        corner(0)
    with jax.named_scope("relay1"):
        relay(1)
    with jax.named_scope("spread3"):
        spread(3)
    with jax.named_scope("arrive0"):
        arrive(0)
    with jax.named_scope("norm_step0_0"):
        norm_step(0, 0)
    with jax.named_scope("norm_step0_1"):
        norm_step(0, 1)
    with jax.named_scope("relay2"):
        relay(2)
    with jax.named_scope("corner1"):
        corner(1)
    with jax.named_scope("relay3"):
        relay(3)
    with jax.named_scope("arrive1"):
        arrive(1)
    with jax.named_scope("norm_step1_0"):
        norm_step(1, 0)
    with jax.named_scope("norm_step1_1"):
        norm_step(1, 1)
    with jax.named_scope("side_step0"):
        side_step(0)
    with jax.named_scope("expert_step0"):
        expert_step(0)
    with jax.named_scope("corner2"):
        corner(2)
    with jax.named_scope("corner3"):
        corner(3)
    with jax.named_scope("arrive2"):
        arrive(2)
    with jax.named_scope("norm_step2_0"):
        norm_step(2, 0)
    with jax.named_scope("norm_step2_1"):
        norm_step(2, 1)
    with jax.named_scope("own_shared"):
        own_shared()
    with jax.named_scope("arrive3"):
        arrive(3)
    with jax.named_scope("norm_step3_0"):
        norm_step(3, 0)
    with jax.named_scope("norm_step3_1"):
        norm_step(3, 1)
    with jax.named_scope("side_step1"):
        side_step(1)
    with jax.named_scope("expert_step1"):
        expert_step(1)
    with jax.named_scope("down_step0"):
        down_step(0)
    with jax.named_scope("return_step0"):
        return_step(0)
    with jax.named_scope("own_switch"):
        switch = own_switch()
    with jax.named_scope("own_side"):
        own_side()
    with jax.named_scope("down_step1"):
        down_step(1)
    with jax.named_scope("own_extra"):
        extra = own_extra()
    with jax.named_scope("return_step1"):
        return_step(1)

    routed = total[0]
    for step in range(1, steps):
        with jax.named_scope("line_wait"):
            settle(line_in.at[step], back_sem.at[1 + step])
        routed = routed + line_in[step].astype(jnp.float32)
    own = normed[0:rows, own_slice].astype(jnp.float32)
    pre_second = RESIDUAL_SCALE * own + routed + extra
    stats[tp, 0:1, 0:rows] = line_of(jnp.sum(pre_second, 1, keepdims=True))
    stats[tp, 1:2, 0:rows] = line_of(jnp.sum(pre_second * pre_second, 1, keepdims=True))
    for peer in plane:
        push(stats.at[tp], stats.at[tp], send_sem.at[STAT], recv_sem.at[STAT], peer)
    with jax.named_scope("stat_wait"):
        settle(stats.at[pl.ds(0, tps - 1)], recv_sem.at[STAT])
    totals = stats[0]
    for t in range(1, tps):
        totals = totals + stats[t]
    mean = column_of(totals[0:1, 0:rows]) / model
    square = column_of(totals[1:2, 0:rows]) / model
    output[...] = (pre_second - mean) * lax.rsqrt(square - mean * mean + NORM_EPS)
    with jax.named_scope("drain"):
        settle(mixed_all.at[pl.ds(0, tps - 1)], send_sem.at[MIXED])
        settle(route_all.at[pl.ds(0, eps - 1)], send_sem.at[ROUTE])
        settle(weight_all.at[pl.ds(0, eps - 1)], send_sem.at[WEIGHT])
        settle(side_out.at[pl.ds(0, eps - 1)], send_sem.at[SIDE])
        settle(late_all.at[pl.ds(0, tps - 1)], send_sem.at[LATE])
        settle(stats.at[pl.ds(0, tps - 1)], send_sem.at[STAT])
        settle(hidden_all.at[:, pl.ds(0, tps - 1)], send_sem.at[HIDDEN])
        settle(rows_all.at[pl.ds(0, 5), pl.ds(0, 6)], send_sem.at[7])
        settle(rows_all.at[pl.ds(0, 4)], send_sem.at[8])
        settle(pair_out, send_sem.at[9])
        settle(line_out.at[pl.ds(0, steps - 1)], send_sem.at[10])


def mixer(mixed, tokens, routes, route_weights, first_gain, side_switch, weights):
    out_w, gate_w, up_w, down_w, shared_gate, _, shared_down, side_gate, _, side_down = weights
    eps, tps = lax.axis_size("ep"), lax.axis_size("tp")
    chips = eps // 2
    rows, model = tokens.shape
    cols = model // tps
    experts, _, hidden = gate_w.shape
    top = routes.shape[0]
    total = experts * eps
    capacity = (3 * rows * top + total - 1) // total
    slots = -(-experts * capacity // 16) * 16
    wide = -(-experts * rows // 128) * 128
    side_width, side_rows = side_gate.shape
    shared = shared_gate.shape[1]
    bf16, f32 = jnp.bfloat16, jnp.float32
    dma = pltpu.SemaphoreType.DMA
    line = pltpu.VMEM((chips, rows, cols), bf16)
    sides = pltpu.VMEM((eps, rows, 2 * side_width), bf16)
    return pl.pallas_call(
        functools.partial(mixer_body, (chips, tps, capacity)),
        out_shape=jax.ShapeDtypeStruct((rows, cols), f32),
        in_specs=[ANY] * 16,
        out_specs=VMEM,
        scratch_shapes=[
            pltpu.VMEM((rows, cols), bf16),
            pltpu.VMEM(first_gain.shape, f32),
            pltpu.VMEM(side_switch.shape, bf16),
            pltpu.VMEM((tps,) + mixed.shape, bf16),
            pltpu.VMEM((eps, top, rows), jnp.int32),
            pltpu.VMEM((eps, top, rows), f32),
            pltpu.VMEM((eps, 2 * tps, rows, cols // 2), bf16),
            pltpu.VMEM((eps * rows, model), bf16),
            pltpu.VMEM((128, wide), f32),
            pltpu.VMEM((wide, 128), f32),
            pltpu.VMEM((2, tps, 4, slots, hidden), bf16),
            line,
            line,
            line,
            line,
            pltpu.VMEM((chips, rows, cols), f32),
            sides,
            sides,
            pltpu.VMEM((tps, rows, shared + 2 * side_width), bf16),
            pltpu.VMEM((tps, 8, 128), f32),
            pltpu.VMEM(out_w.shape, bf16),
            pltpu.VMEM((experts, model, 2 * hidden), bf16),
            pltpu.VMEM(down_w.shape, bf16),
            pltpu.VMEM((model, 2 * shared), bf16),
            pltpu.VMEM(shared_down.shape, bf16),
            pltpu.VMEM((2 * side_width, side_rows), bf16),
            pltpu.VMEM(side_down.shape, bf16),
            dma((6,)),
            dma((7,)),
            dma((11,)),
            dma((8,)),
            dma((chips, 6)),
            dma((5,)),
        ],
        compiler_params=pltpu.CompilerParams(collective_id=0, has_side_effects=True),
    )(mixed, tokens, routes, route_weights, first_gain, side_switch, *weights)


def streamed_device(
    tokens,
    retention_state,
    lengths,
    query_weight,
    key_weight,
    value_weight,
    gate_weight,
    out_weight,
    first_gain,
    routing,
    route_weight,
    expert_gate,
    expert_up,
    expert_down,
    shared_gate,
    shared_up,
    shared_down,
    side_gate,
    side_up,
    side_down,
    side_switch,
    second_gain,
):
    rows, heads, width = retention_state.shape[:3]
    exponent = np.arange(width // 2, dtype=np.float64) / (width // 2)
    frequency = np.tile((ROPE_BASE**-exponent).astype(np.float32), 2 * heads)[None, :]
    mixed, new_state = retain_kernel(
        tokens,
        lengths.reshape(1, rows),
        jnp.asarray(frequency),
        [query_weight, key_weight, value_weight, gate_weight],
        retention_state,
    )
    normed = mixer(
        mixed,
        tokens,
        routing.T,
        route_weight.T,
        first_gain.reshape(1, -1),
        side_switch,
        [
            out_weight,
            expert_gate,
            expert_up,
            expert_down,
            shared_gate,
            shared_up,
            shared_down,
            side_gate.T,
            side_up.T,
            side_down,
        ],
    )
    output = (normed * second_gain[None, :]).astype(jnp.bfloat16)
    return (output, new_state)


def staged_device(
    tokens,
    retention_state,
    lengths,
    query_weight,
    key_weight,
    value_weight,
    gate_weight,
    out_weight,
    first_gain,
    routing,
    route_weight,
    expert_gate,
    expert_up,
    expert_down,
    shared_gate,
    shared_up,
    shared_down,
    side_gate,
    side_up,
    side_down,
    side_switch,
    second_gain,
):
    seq_rows = tokens.shape[0]
    model_width = tokens.shape[1]
    head_count = retention_state.shape[1]
    col_count = out_weight.shape[1]
    ep_count = lax.axis_size("ep")
    tp_rank = lax.axis_index("tp")
    ep_rank = lax.axis_index("ep")
    col_start = tp_rank * col_count
    side_width = side_gate.shape[1]
    side_part = jnp.concatenate([side_gate, side_up], 1)
    side_both, every_route, every_weight, *projections = first(
        [side_part, routing.T, route_weight.T],
        tokens,
        [query_weight, key_weight, value_weight, gate_weight],
        0,
    )
    side_both = side_both.reshape(model_width, 2 * side_width)
    mixed_heads, new_state = retain(
        retention_state, lengths, projections, tp_rank * head_count
    )
    (every_mixed,) = gather([mixed_heads], "tp", 1)
    mixing = jnp.dot(
        side_by_side(every_mixed),
        out_weight,
        preferred_element_type=jnp.float32,
    )
    own_cols = lax.dynamic_slice_in_dim(tokens, col_start, col_count, 1).astype(jnp.float32)
    pre_first = RESIDUAL_SCALE * own_cols + mixing
    first_sum, first_square = row_moments(pre_first, 2)
    row_mean = first_sum / model_width
    square = first_square / model_width
    own_gain = lax.dynamic_slice_in_dim(first_gain, col_start, col_count, 0)
    normed_cols = (
        (pre_first - row_mean) * lax.rsqrt(square - row_mean * row_mean + NORM_EPS) * own_gain
    ).astype(jnp.bfloat16)
    every_rows = spread(normed_cols, 3)
    normed_full = lax.dynamic_index_in_dim(every_rows, ep_rank, 0, keepdims=False)
    every_rows = every_rows.reshape(ep_count * seq_rows, model_width)

    local_experts = expert_gate.shape[0]
    top_count = routing.shape[1]
    expert_count = local_experts * ep_count
    capacity = (3 * seq_rows * top_count + expert_count - 1) // expert_count
    total_rows = ep_count * seq_rows
    route_all = jnp.transpose(every_route, (1, 0, 2)).reshape(top_count, total_rows)
    weight_all = jnp.transpose(every_weight, (1, 0, 2)).reshape(top_count, total_rows)
    local_ids = ep_rank * local_experts + jnp.arange(local_experts, dtype=jnp.int32)
    named = route_all[None, :, :] == local_ids[:, None, None]
    member = jnp.any(named, 1)
    pair_weight = jnp.sum(jnp.where(named, weight_all[None, :, :], 0.0), 1)
    index = jnp.arange(total_rows, dtype=jnp.int32)
    group = index // seq_rows
    earlier = ((index[:, None] < index[None, :]) & (group[:, None] == group[None, :])).astype(
        jnp.bfloat16
    )
    before = jnp.dot(
        member.astype(jnp.bfloat16), earlier, preferred_element_type=jnp.float32
    ).astype(jnp.int32)
    slot = jnp.where(member, group[None, :] * capacity + before, -1)
    slot_total = ep_count * capacity
    hit = slot[:, None, :] == jnp.arange(slot_total, dtype=jnp.int32)[None, :, None]
    table = hit.astype(jnp.bfloat16).reshape(local_experts * slot_total, total_rows)
    slot_weight = jnp.sum(jnp.where(hit, pair_weight[:, None, :], 0.0), -1, keepdims=True)
    chosen = (
        jnp.dot(table, every_rows, preferred_element_type=jnp.float32)
        .astype(jnp.bfloat16)
        .reshape(local_experts, slot_total, model_width)
    )
    gate_part = jnp.einsum("jcd,jdf->jcf", chosen, expert_gate, preferred_element_type=jnp.float32)
    up_part = jnp.einsum("jcd,jdf->jcf", chosen, expert_up, preferred_element_type=jnp.float32)
    hidden = (jax.nn.silu(gate_part) * up_part * slot_weight).astype(jnp.bfloat16)

    side_pre = jnp.dot(normed_full, side_both, preferred_element_type=jnp.float32)
    side_hidden = (jax.nn.silu(side_pre[:, :side_width]) * side_pre[:, side_width:]).astype(
        jnp.bfloat16
    )
    shared_hidden = (
        jax.nn.silu(jnp.dot(normed_full, shared_gate, preferred_element_type=jnp.float32))
        * jnp.dot(normed_full, shared_up, preferred_element_type=jnp.float32)
    ).astype(jnp.bfloat16)
    hidden_blocks, shared_blocks, side_blocks = gather(
        [hidden.reshape(local_experts * slot_total, -1), shared_hidden, side_hidden], "tp", 4
    )
    hidden_all = side_by_side(hidden_blocks).reshape(local_experts, slot_total, -1)
    result = (
        jnp.einsum("jcf,jfd->jcd", hidden_all, expert_down, preferred_element_type=jnp.float32)
        .astype(jnp.bfloat16)
        .reshape(local_experts * slot_total, col_count)
    )
    summed = (
        lax.dot_general(
            table, result, (((0,), (0,)), ((), ())), preferred_element_type=jnp.float32
        )
        .astype(jnp.bfloat16)
        .reshape(ep_count, seq_rows, col_count)
    )
    returned = scatter(summed, 5)
    routed = jnp.sum(returned.astype(jnp.float32), 0)
    shared_out = jnp.dot(
        side_by_side(shared_blocks), shared_down, preferred_element_type=jnp.float32
    )
    side_out = jnp.dot(side_by_side(side_blocks), side_down, preferred_element_type=jnp.float32)
    switch = jax.nn.sigmoid(
        jnp.sum(normed_full.astype(jnp.float32) * side_switch.astype(jnp.float32)[None, :], -1)
    )
    pre_second = (
        RESIDUAL_SCALE * normed_cols.astype(jnp.float32)
        + routed
        + shared_out
        + switch[:, None] * side_out
    )
    second_sum, second_square = row_moments(pre_second, 6)
    mean_second = second_sum / model_width
    square_second = second_square / model_width
    output = (
        (pre_second - mean_second)
        * lax.rsqrt(square_second - mean_second * mean_second + NORM_EPS)
        * second_gain
    ).astype(jnp.bfloat16)
    return (output, new_state)


def on_device(*arrays):
    tokens, state, expert_gate, side_gate = arrays[0], arrays[1], arrays[11], arrays[17]
    eps, tps = lax.axis_size("ep"), lax.axis_size("tp")
    rows, model = tokens.shape
    fits = (
        eps == 8
        and tps == 4
        and rows % 16 == 0
        and model % (256 * tps) == 0
        and state.shape[1] * state.shape[2] % 128 == 0
        and expert_gate.shape[2] % 128 == 0
        and side_gate.shape[0] % 128 == 0
        and side_gate.shape[1] == 64
    )
    return (streamed_device if fits else staged_device)(*arrays)


def solution(mesh):
    return jax.shard_map(
        on_device,
        mesh=mesh,
        in_specs=(
            P("ep", None),
            P("ep", "tp", None, None),
            P("ep"),
            P(None, "tp"),
            P(None, "tp"),
            P(None, "tp"),
            P(None, "tp"),
            P(None, "tp"),
            P(),
            P("ep", None),
            P("ep", None),
            P("ep", None, "tp"),
            P("ep", None, "tp"),
            P("ep", None, "tp"),
            P(None, "tp"),
            P(None, "tp"),
            P(None, "tp"),
            P("ep", "tp"),
            P("ep", "tp"),
            P(None, "tp"),
            P(),
            P("tp"),
        ),
        out_specs=(P("ep", "tp"), P("ep", "tp", None, None)),
        check_vma=False,
    )
```

```python
import functools

import jax
import jax.numpy as jnp
from jax import lax
from jax.experimental import pallas as pl
from jax.experimental.pallas import tpu as pltpu
from jax.sharding import PartitionSpec as P

HEADS = 16


RESIDUAL_SCALE = 2.0**0.25
NORM_EPS = 1e-05
GROUP_EPS = 1e-06
ROPE_BASE = 10000.0


def rotate(vector, positions):
    half_width = vector.shape[-1] // 2
    frequency = ROPE_BASE ** (-jnp.arange(half_width, dtype=jnp.float32) / half_width)
    angles = positions.astype(jnp.float32)[:, None, None] * frequency[None, None, :]
    cosine = jnp.cos(angles)
    sine_part = jnp.sin(angles)
    first_half = vector[..., :half_width]
    second_half = vector[..., half_width:]
    return jnp.concatenate(
        [
            first_half * cosine - second_half * sine_part,
            second_half * cosine + first_half * sine_part,
        ],
        -1,
    )


def retain(
    retention_state,
    lengths,
    projections,
    first_head,
):
    row_count = retention_state.shape[0]
    head_count = retention_state.shape[1]
    head_width = retention_state.shape[2]

    query_rows, key_part, value_part, gate_part = [part.astype(jnp.float32) for part in projections]
    queries = rotate(query_rows.reshape(row_count, head_count, head_width), lengths)
    key_rows = rotate(
        key_part.reshape(row_count, head_count, head_width), lengths
    ) * head_width ** (-0.5)
    values = value_part.reshape(row_count, head_count, head_width)
    gate_act = gate_part
    head_index = (first_head + jnp.arange(head_count)).astype(jnp.float32)
    decays = 1.0 - 2.0 ** (-5.0 - 7.0 * head_index / (HEADS - 1))
    own_term = jnp.sum(queries * key_rows, -1, keepdims=True) * values
    carried = decays[None, :, None] * jnp.sum(queries[:, :, :, None] * retention_state, 2)
    result = own_term + carried
    new_state = (
        decays[None, :, None, None] * retention_state
        + key_rows[:, :, :, None] * values[:, :, None, :]
    )
    normed = result * lax.rsqrt(jnp.mean(result * result, -1, keepdims=True) + GROUP_EPS)
    mixed_heads = (
        normed.reshape(row_count, head_count * head_width) * jax.nn.silu(gate_act)
    ).astype(jnp.bfloat16)
    return (mixed_heads, new_state)


VMEM = pl.BlockSpec(memory_space=pltpu.VMEM)
DEVICE = pl.DeviceIdType.MESH


def enter(peers):
    barrier = pltpu.get_barrier_semaphore()
    for peer in peers:
        pl.semaphore_signal(barrier, inc=1, device_id=peer, device_id_type=DEVICE)
    pl.semaphore_wait(barrier, len(peers))


def send(source, target, send_sem, recv_sem, peer):
    copy = pltpu.make_async_remote_copy(
        src_ref=source,
        dst_ref=target,
        send_sem=send_sem,
        recv_sem=recv_sem,
        device_id=peer,
        device_id_type=DEVICE,
    )
    copy.start()
    return copy


def on_axis(axis, index):
    if axis == "ep":
        return (index, lax.axis_index("tp"))
    return (lax.axis_index("ep"), index)


def gather_body(axis, count, parts, *refs):
    sources, targets = refs[:parts], refs[parts : 2 * parts]
    send_sem, recv_sem, local_sem = refs[2 * parts :]
    me = lax.axis_index(axis)
    others = [lax.rem(me + step, count) for step in range(1, count)]
    locals_ = []
    for part in range(parts):
        own = pltpu.make_async_copy(sources[part], targets[part].at[me], local_sem.at[part])
        own.start()
        locals_.append(own)
    enter([on_axis(axis, other) for other in others])
    copies = []
    for step, other in enumerate(others):
        for part in range(parts):
            copies.append(
                send(
                    sources[part],
                    targets[part].at[me],
                    send_sem.at[step, part],
                    recv_sem.at[step, part],
                    on_axis(axis, other),
                )
            )
    for copy in locals_:
        copy.wait()
    for copy in copies:
        copy.wait()


def gather(arrays, axis, ident):
    count, parts = lax.axis_size(axis), len(arrays)
    return pl.pallas_call(
        functools.partial(gather_body, axis, count, parts),
        out_shape=[jax.ShapeDtypeStruct((count,) + a.shape, a.dtype) for a in arrays],
        in_specs=[VMEM] * parts,
        out_specs=[VMEM] * parts,
        scratch_shapes=[
            pltpu.SemaphoreType.DMA((count - 1, parts)),
            pltpu.SemaphoreType.DMA((count - 1, parts)),
            pltpu.SemaphoreType.DMA((parts,)),
        ],
        compiler_params=pltpu.CompilerParams(collective_id=ident, has_side_effects=True),
    )(*arrays)


def scatter_body(count, source, target, send_sem, recv_sem, local_sem):
    me = lax.axis_index("ep")
    others = [lax.rem(me + step, count) for step in range(1, count)]
    own = pltpu.make_async_copy(source.at[me], target.at[me], local_sem)
    own.start()
    enter([on_axis("ep", other) for other in others])
    copies = [
        send(
            source.at[other],
            target.at[me],
            send_sem.at[step],
            recv_sem.at[step],
            on_axis("ep", other),
        )
        for step, other in enumerate(others)
    ]
    own.wait()
    for copy in copies:
        copy.wait()


def scatter(array, ident):
    count = array.shape[0]
    return pl.pallas_call(
        functools.partial(scatter_body, count),
        out_shape=jax.ShapeDtypeStruct(array.shape, array.dtype),
        in_specs=[VMEM],
        out_specs=VMEM,
        scratch_shapes=[
            pltpu.SemaphoreType.DMA((count - 1,)),
            pltpu.SemaphoreType.DMA((count - 1,)),
            pltpu.SemaphoreType.DMA,
        ],
        compiler_params=pltpu.CompilerParams(collective_id=ident, has_side_effects=True),
    )(array)


def first_body(count, *refs):
    parts = 3
    sources, (tokens, *weights) = refs[:parts], refs[parts : parts + 5]
    targets = refs[parts + 5 : 2 * parts + 5]
    results = refs[2 * parts + 5 : 2 * parts + 9]
    send_sem, recv_sem, local_sem = refs[2 * parts + 9 :]
    chips = count // 2
    me = lax.axis_index("ep")
    chip, core = me // 2, lax.rem(me, 2)
    partner = on_axis("ep", chip * 2 + 1 - core)
    line = [lax.rem(chip + step, chips) * 2 + core for step in range(1, chips)]
    senders = [lax.rem(chip + chips - step, chips) * 2 + core for step in range(1, chips)]
    locals_ = []
    for part in range(parts):
        own = pltpu.make_async_copy(sources[part], targets[part].at[me], local_sem.at[part])
        own.start()
        locals_.append(own)
    enter([on_axis("ep", other) for other in line] + [partner])
    direct, copies = [], []
    for step, other in enumerate(line):
        for part in range(parts):
            direct.append(
                send(
                    sources[part],
                    targets[part].at[me],
                    send_sem.at[step, part],
                    recv_sem.at[step, part],
                    on_axis("ep", other),
                )
            )
    for part in range(parts):
        copies.append(
            send(
                sources[part],
                targets[part].at[me],
                send_sem.at[chips - 1, part],
                recv_sem.at[chips - 1, part],
                partner,
            )
        )
    for weight, result in zip(weights, results):
        result[...] = jnp.dot(
            tokens[...], weight[...], preferred_element_type=jnp.float32
        ).astype(result.dtype)
    for step, sender in enumerate(senders):
        for part in range(parts):
            direct[step * parts + part].wait_recv()
            copies.append(
                send(
                    targets[part].at[sender],
                    targets[part].at[sender],
                    send_sem.at[chips + step, part],
                    recv_sem.at[chips + step, part],
                    partner,
                )
            )
    for copy in locals_:
        copy.wait()
    for copy in direct:
        copy.wait_send()
    for copy in copies:
        copy.wait()


def first(arrays, tokens, weights, ident):
    count, parts = lax.axis_size("ep"), len(arrays)
    rows = tokens.shape[0]
    return pl.pallas_call(
        functools.partial(first_body, count),
        out_shape=[jax.ShapeDtypeStruct((count,) + a.shape, a.dtype) for a in arrays]
        + [jax.ShapeDtypeStruct((rows, w.shape[1]), jnp.bfloat16) for w in weights],
        in_specs=[VMEM] * (parts + 5),
        out_specs=[VMEM] * (parts + 4),
        scratch_shapes=[
            pltpu.SemaphoreType.DMA((count - 1, parts)),
            pltpu.SemaphoreType.DMA((count - 1, parts)),
            pltpu.SemaphoreType.DMA((parts,)),
        ],
        compiler_params=pltpu.CompilerParams(collective_id=ident, has_side_effects=True),
    )(*arrays, tokens, *weights)


def spread_body(count, tp_count, source, target, send_sem, recv_sem, local_sem):
    chips, width = count // 2, source.shape[1]
    me, own_tp = lax.axis_index("ep"), lax.axis_index("tp")
    chip, core = me // 2, lax.rem(me, 2)
    partner = (chip * 2 + 1 - core, own_tp)

    def place(row, col):
        return target.at[row, :, pl.ds(pl.multiple_of(col * width, width), width)]

    def chip_at(step):
        return lax.rem(chip + chips + step, chips) * 2 + core

    def tp_at(step):
        return lax.rem(own_tp + tp_count + step, tp_count)

    own = pltpu.make_async_copy(source, place(me, own_tp), local_sem)
    own.start()
    line = [(chip_at(step), own_tp) for step in range(1, chips)]
    plane = [(me, tp_at(step)) for step in range(1, tp_count)]
    enter(line + plane + [partner])

    def pair(line_step, plane_step, to_partner):
        return (
            send_sem.at[to_partner, line_step, plane_step],
            recv_sem.at[to_partner, line_step, plane_step],
        )

    direct, planar, copies = [], {}, []
    for step in range(1, chips):
        direct.append(send(source, place(me, own_tp), *pair(step, 0, 0), line[step - 1]))
    for step in range(1, tp_count):
        planar[(0, step)] = send(source, place(me, own_tp), *pair(0, step, 0), plane[step - 1])
    copies.append(send(source, place(me, own_tp), *pair(0, 0, 1), partner))
    for line_step in range(1, chips):
        direct[line_step - 1].wait_recv()
        block = place(chip_at(-line_step), own_tp)
        for step in range(1, tp_count):
            planar[(line_step, step)] = send(
                block, block, *pair(line_step, step, 0), plane[step - 1]
            )
        copies.append(send(block, block, *pair(line_step, 0, 1), partner))
    for line_step in range(chips):
        for step in range(1, tp_count):
            planar[(line_step, step)].wait_recv()
            block = place(chip_at(-line_step), tp_at(-step))
            copies.append(send(block, block, *pair(line_step, step, 1), partner))
    own.wait()
    for copy in direct:
        copy.wait_send()
    for copy in planar.values():
        copy.wait_send()
    for copy in copies:
        copy.wait()


def spread(block, ident):
    count, tp_count = lax.axis_size("ep"), lax.axis_size("tp")
    rows, width = block.shape
    return pl.pallas_call(
        functools.partial(spread_body, count, tp_count),
        out_shape=jax.ShapeDtypeStruct((count, rows, width * tp_count), block.dtype),
        in_specs=[VMEM],
        out_specs=VMEM,
        scratch_shapes=[
            pltpu.SemaphoreType.DMA((2, count // 2, tp_count)),
            pltpu.SemaphoreType.DMA((2, count // 2, tp_count)),
            pltpu.SemaphoreType.DMA,
        ],
        compiler_params=pltpu.CompilerParams(collective_id=ident, has_side_effects=True),
    )(block)


def side_by_side(gathered):
    return jnp.concatenate([gathered[i] for i in range(gathered.shape[0])], -1)


def row_moments(values, ident):
    sums = jnp.stack([jnp.sum(values, -1), jnp.sum(values * values, -1)])
    (every,) = gather([sums], "tp", ident)
    totals = jnp.sum(every, 0)
    return totals[0][:, None], totals[1][:, None]


ANY = pl.BlockSpec(memory_space=pl.ANY)


def dot(a, b):
    return jnp.dot(a, b, preferred_element_type=jnp.float32)


def silu(x):
    return x / (1.0 + jnp.exp(-x))


def fetch(source, target, sem):
    copy = pltpu.make_async_copy(source, target, sem)
    copy.start()
    return copy


def settle(ref, sem):
    pltpu.make_async_copy(ref, ref, sem).wait()


def on_diagonal(rows):
    row = lax.broadcasted_iota(jnp.int32, (rows, rows), 0)
    return row == lax.broadcasted_iota(jnp.int32, (rows, rows), 1)


def column_of(line):
    return jnp.sum(jnp.where(on_diagonal(line.shape[1]), line, 0.0), 1, keepdims=True)


def line_of(column):
    return jnp.sum(jnp.where(on_diagonal(column.shape[0]), column, 0.0), 0, keepdims=True)


def rotated(x, cosine, sine, half):
    width = x.shape[1]
    lane = lax.broadcasted_iota(jnp.int32, x.shape, 1)
    first = (lane & (2 * half - 1)) < half
    later = pltpu.roll(x, width - half, 1)
    sooner = pltpu.roll(x, half, 1)
    return x * cosine + jnp.where(first, -later, sooner) * sine


def retain_body(
    chunk,
    tokens_in,
    lengths_in,
    query_in,
    key_in,
    value_in,
    gate_in,
    state_in,
    mixed,
    state_out,
    tokens,
    lengths,
    weights,
    state,
    columns,
    spread_even,
    spread_odd,
    values,
    carried,
    small_sem,
    weight_sem,
    state_sem,
    out_sem,
):
    rows, heads, width = state.shape[0], state.shape[1], state.shape[2]
    total = heads * width
    chunks = rows // chunk
    small = [
        fetch(source, target, small_sem.at[i])
        for i, (source, target) in enumerate(
            [(lengths_in, lengths), (tokens_in, tokens)]
        )
    ]
    for i, source in enumerate([query_in, key_in, value_in, gate_in]):
        fetch(source, weights.at[:, pl.ds(i * total, total)], weight_sem.at[i // 2])

    with jax.named_scope("small_wait"):
        small[0].wait()
    for i in range(chunks):
        piece = pl.ds(i * chunk, chunk)
        fetch(state_in.at[piece], state.at[piece], state_sem.at[i])
    position = column_of(lengths[...].astype(jnp.float32))
    lane = lax.broadcasted_iota(jnp.int32, (1, total), 1) & (width // 2 - 1)
    frequency = jnp.zeros((1, total), jnp.float32)
    for i in range(width // 2):
        frequency = jnp.where(lane == i, ROPE_BASE ** (-i / (width // 2)), frequency)
    angles = position * frequency
    cosine, sine = jnp.cos(angles), jnp.sin(angles)
    first_head = lax.axis_index("tp") * heads
    decays = []
    for head in range(heads):
        index = jnp.full((1, width), first_head + head, jnp.int32).astype(jnp.float32)
        decays.append(1.0 - jnp.exp2(-5.0 - 7.0 * index / (HEADS - 1)))

    def project(i):
        span = pl.ds(2 * i * total, 2 * total)
        with jax.named_scope("weight_wait"):
            settle(weights.at[:, span], weight_sem.at[i])
        both = dot(tokens[...], weights[:, span]).astype(jnp.bfloat16).astype(jnp.float32)
        return both[:, :total], both[:, total:]

    with jax.named_scope("small_wait"):
        small[1].wait()
    query, key = project(0)
    lanes = columns.shape[1]
    for i, (x, scale) in enumerate([(query, 1.0), (key, width ** (-0.5))]):
        turned = rotated(x, cosine, sine, width // 2) * scale
        padded = jnp.concatenate([turned, jnp.zeros((lanes - rows, total), jnp.float32)], 0)
        columns[i * total : (i + 1) * total, :] = jnp.transpose(padded).astype(jnp.bfloat16)
    value, gate = project(1)
    for head in range(heads):
        values[head] = value[:, head * width : (head + 1) * width]

    source_lane = lax.broadcasted_iota(jnp.int32, (lanes, 2 * lanes), 0)
    target_lane = lax.broadcasted_iota(jnp.int32, (lanes, 2 * lanes), 1)
    offset = jnp.where(target_lane >= lanes, 1, 0)
    buffers = [spread_even, spread_odd]

    def widen(i, pair):
        pick = jnp.where(source_lane == offset + (i * chunk + 2 * pair), 1.0, 0.0)
        buffers[i % 2][pair] = dot(columns[...], pick.astype(jnp.bfloat16))

    for pair in range(chunk // 2):
        widen(0, pair)
    for i in range(chunks):
        base = i * chunk
        piece = pl.ds(base, chunk)
        with jax.named_scope("state_wait"):
            pltpu.make_async_copy(state_in.at[piece], state.at[piece], state_sem.at[i]).wait()
        wide = buffers[i % 2]
        for at in range(chunk):
            if i + 1 < chunks and at % 2 == 0:
                widen(i + 1, at // 2)
            lane = (at % 2) * lanes
            for head in range(heads):
                low, high = head * width, (head + 1) * width
                q_cols = wide[at // 2, low:high, lane : lane + width]
                k_cols = wide[at // 2, total + low : total + high, lane : lane + width]
                v_row = values[head, base + at : base + at + 1, :]
                new = decays[head] * state[base + at, head] + k_cols * v_row
                state[base + at, head] = new
                carried[head, base + at : base + at + 1, :] = jnp.sum(
                    q_cols * new, 0, keepdims=True
                )
        fetch(state.at[piece], state_out.at[piece], out_sem)
    parts = []
    for head in range(heads):
        result = carried[head]
        scale = lax.rsqrt(jnp.mean(result * result, -1, keepdims=True) + GROUP_EPS)
        parts.append(result * scale)
    mixed[...] = (jnp.concatenate(parts, 1) * silu(gate)).astype(mixed.dtype)
    with jax.named_scope("state_drain"):
        settle(state, out_sem)


def retain_kernel(tokens, lengths, weights, state):
    rows, heads, width = state.shape[0], state.shape[1], state.shape[2]
    chunk, lanes = 8, 128
    cols = heads * width
    wide = pltpu.VMEM((chunk // 2, 2 * cols, 2 * lanes), jnp.float32)
    return pl.pallas_call(
        functools.partial(retain_body, chunk),
        out_shape=[
            jax.ShapeDtypeStruct((rows, cols), jnp.bfloat16),
            jax.ShapeDtypeStruct(state.shape, state.dtype),
        ],
        in_specs=[ANY] * 7,
        out_specs=[VMEM, ANY],
        compiler_params=pltpu.CompilerParams(vmem_limit_bytes=55200 * 2**10),
        scratch_shapes=[
            pltpu.VMEM(tokens.shape, tokens.dtype),
            pltpu.VMEM(lengths.shape, lengths.dtype),
            pltpu.VMEM((tokens.shape[1], 4 * cols), jnp.bfloat16),
            pltpu.VMEM(state.shape, state.dtype),
            pltpu.VMEM((2 * cols, lanes), jnp.bfloat16),
            wide,
            wide,
            pltpu.VMEM((heads, rows, width), jnp.float32),
            pltpu.VMEM((heads, rows, width), jnp.float32),
            pltpu.SemaphoreType.DMA((2,)),
            pltpu.SemaphoreType.DMA((2,)),
            pltpu.SemaphoreType.DMA((rows // chunk,)),
            pltpu.SemaphoreType.DMA,
        ],
    )(tokens, lengths, *weights, state)


def mixer_body(
    dims,
    mixed_in,
    tokens_in,
    routes_in,
    route_weights_in,
    first_gain_in,
    side_switch_in,
    out_in,
    gate_in,
    up_in,
    down_in,
    shared_gate_in,
    shared_up_in,
    shared_down_in,
    side_gate_in,
    side_up_in,
    side_down_in,
    output,
    own_tokens,
    first_gain,
    side_switch,
    mixed_all,
    route_all,
    weight_all,
    rows_all,
    normed,
    info,
    info_cols,
    hidden_all,
    pair_out,
    pair_in,
    line_out,
    line_in,
    total,
    side_out,
    side_in,
    late_all,
    stats,
    out_w,
    gate_up_w,
    down_w,
    shared_w,
    shared_down_w,
    side_w,
    side_down_w,
    small_sem,
    weight_sem,
    send_sem,
    recv_sem,
    row_sem,
    back_sem,
):
    chips, tps, capacity, groups = dims
    steps = chips
    rows, cols = own_tokens.shape
    model = cols * tps
    half = cols // 2
    experts, hidden_width = gate_in.shape[0], gate_in.shape[2]
    slots = experts * capacity
    pair_slots = hidden_all.shape[2]
    side_width = side_gate_in.shape[0]
    side_rows = side_gate_in.shape[1]
    shared_width = shared_gate_in.shape[1]
    tp = lax.axis_index("tp")
    ep = lax.axis_index("ep")
    eps = 2 * chips
    chip, core = ep // 2, lax.rem(ep, 2)
    partner = (chip * 2 + 1 - core, tp)
    low, high = lax.rem(tp, 2), tp // 2
    tp_x = high * 2 + 1 - low
    tp_y = (1 - high) * 2 + low
    tp_d = (1 - high) * 2 + 1 - low
    plane = [(ep, tp_x), (ep, tp_y), (ep, tp_d)]

    def chip_at(step):
        if step == 0:
            return chip
        if step == 1:
            return chip + 1 - 2 * lax.rem(chip, 2)
        if step == 2:
            return lax.rem(chip + 2, 4)
        return 3 - chip

    def group_at(step, at):
        return chip_at(step) * 2 + (core if at == 0 else 1 - core)

    line = [(group_at(step, 0), tp) for step in range(steps)]
    others = [(group_at(s, at), tp) for s in range(steps) for at in range(2) if s + at > 0]
    peers = plane + others
    barrier = pltpu.get_barrier_semaphore()
    for peer in peers:
        pl.semaphore_signal(barrier, inc=1, device_id=peer, device_id_type=DEVICE)

    own_mixed = mixed_all.at[tp]
    own_slice = pl.ds(pl.multiple_of(tp * cols, cols), cols)
    fetch(routes_in, route_all.at[ep], small_sem.at[1])
    fetch(route_weights_in, weight_all.at[ep], small_sem.at[2])
    fetch(tokens_in.at[:, own_slice], own_tokens, small_sem.at[3])
    fetch(out_in, out_w, weight_sem.at[0])
    MIXED, ROUTE, WEIGHT, SIDE, LATE, STAT, HIDDEN = 0, 1, 2, 3, 4, 5, 6

    def push(source, target, sent, received, peer):
        send(source, target, sent, received, peer)

    with jax.named_scope("small_wait"):
        settle(route_all.at[ep], small_sem.at[1])
        settle(weight_all.at[ep], small_sem.at[2])
    fetch(first_gain_in, first_gain, small_sem.at[4])
    fetch(side_switch_in, side_switch, small_sem.at[5])
    for e in range(experts):
        fetch(gate_in.at[e], gate_up_w.at[e, :, pl.ds(0, hidden_width)], weight_sem.at[1])
        fetch(up_in.at[e], gate_up_w.at[e, :, pl.ds(hidden_width, hidden_width)], weight_sem.at[1])
    fetch(side_gate_in, side_w.at[pl.ds(0, side_width)], weight_sem.at[2])
    fetch(side_up_in, side_w.at[pl.ds(side_width, side_width)], weight_sem.at[2])
    fetch(shared_gate_in, shared_w.at[:, pl.ds(0, shared_width)], weight_sem.at[3])
    fetch(shared_up_in, shared_w.at[:, pl.ds(shared_width, shared_width)], weight_sem.at[3])
    fetch(down_in, down_w, weight_sem.at[4])
    fetch(shared_down_in, shared_down_w, weight_sem.at[5])
    fetch(side_down_in, side_down_w, weight_sem.at[6])
    with jax.named_scope("enter"):
        pl.semaphore_wait(barrier, len(peers))

    for peer in plane:
        push(mixed_in, own_mixed, send_sem.at[MIXED], recv_sem.at[MIXED], peer)
    for peer in others:
        own = route_all.at[ep]
        push(own, own, send_sem.at[ROUTE], recv_sem.at[ROUTE], peer)
        own = weight_all.at[ep]
        push(own, own, send_sem.at[WEIGHT], recv_sem.at[WEIGHT], peer)

    mixed_all[tp] = mixed_in[...]
    with jax.named_scope("out_wait"):
        settle(own_tokens, small_sem.at[3])
        settle(out_w, weight_sem.at[0])
    with jax.named_scope("mixed_wait"):
        settle(mixed_all.at[pl.ds(0, tps - 1)], recv_sem.at[MIXED])
    heads_all = jnp.concatenate([mixed_all[t] for t in range(tps)], 1)
    pre_first = RESIDUAL_SCALE * own_tokens[...].astype(jnp.float32) + dot(heads_all, out_w[...])
    for part in range(2):
        rows_all[ep, 2 * tp + part] = pre_first[:, part * half : (part + 1) * half].astype(
            jnp.bfloat16
        )

    def block(step, index):
        return rows_all.at[group_at(step, 0), pl.ds(2 * index, 2)]

    def piece(step, index, part):
        return rows_all.at[group_at(step, 0), 2 * index + part]

    def push_rows(ref, step, kind, peer):
        sent = send_sem.at[8] if kind == 5 else send_sem.at[7]
        push(ref, ref, sent, row_sem.at[step, kind], peer)

    def came(ref, step, kind):
        settle(ref, row_sem.at[step, kind])

    def spread(step):
        ref = block(step, tp)
        if step > 0:
            came(ref, step, 0)
        for i, peer in enumerate(plane):
            push_rows(ref, step, 1 + i, peer)
        push_rows(ref, step, 5, partner)

    def relay(step):
        for i, index in enumerate([tp_x, tp_y]):
            came(block(step, index), step, 1 + i)
            push_rows(block(step, index), step, 5, partner)

    def corner(step):
        came(block(step, tp_d), step, 3)
        push_rows(block(step, tp_d), step, 5, partner)

    def arrive(step):
        came(rows_all.at[group_at(step, 1)], step, 5)

    with jax.named_scope("spread0"):
        spread(0)
        for step in range(1, steps):
            push_rows_to = line[step]
            push(block(0, tp), block(0, tp), send_sem.at[7], row_sem.at[step, 0], push_rows_to)

    with jax.named_scope("route_wait"):
        settle(route_all.at[pl.ds(0, eps - 1)], recv_sem.at[ROUTE])
        settle(weight_all.at[pl.ds(0, eps - 1)], recv_sem.at[WEIGHT])
    wide = experts * rows

    def expert_of(index):
        return sum(jnp.where(index >= e * rows, 1, 0) for e in range(1, experts))

    group_lane = expert_of(lax.broadcasted_iota(jnp.int32, (1, wide), 1))
    expert_lane = ep * experts + group_lane
    info[...] = jnp.zeros_like(info)
    for g in range(eps):
        ids = jnp.concatenate([route_all[g]] * experts, 1)
        hits = ids == expert_lane
        scales = jnp.concatenate([weight_all[g]] * experts, 1)
        info[g : g + 1, 0:wide] = jnp.sum(jnp.where(hits, 1.0, 0.0), 0, keepdims=True)
        info[eps + g : eps + g + 1, 0:wide] = jnp.sum(
            jnp.where(hits, scales, 0.0), 0, keepdims=True
        )
    member = info[0:eps, 0:wide]
    sooner = lax.broadcasted_iota(jnp.int32, (wide, wide), 0)
    later = lax.broadcasted_iota(jnp.int32, (wide, wide), 1)
    earlier = jnp.where(
        (sooner < later) & (expert_of(sooner) == expert_of(later)), 1.0, 0.0
    ).astype(jnp.bfloat16)
    before = dot(member.astype(jnp.bfloat16), earlier)
    start = (group_lane * capacity).astype(jnp.float32)
    info[0:eps, 0:wide] = jnp.where(member > 0.5, before + start, -1.0)
    info_cols[...] = jnp.transpose(info[...])
    settle(first_gain, small_sem.at[4])

    def column(index):
        lane = lax.broadcasted_iota(jnp.int32, (wide, info_cols.shape[1]), 1)
        picked = jnp.where(lane == index, info_cols[0:wide, :], 0.0)
        return jnp.sum(picked, 1, keepdims=True)

    side_span = pl.ds(pl.multiple_of(ep * side_rows, side_rows), side_rows)

    def blocks(group):
        return [(step, at) for step in groups[group] for at in range(2)]

    def group_rows(group):
        return slice(2 * groups[group][0] * rows, 2 * (groups[group][-1] + 1) * rows)

    def group_steps(group):
        return pl.ds(groups[group][0], len(groups[group]))

    def norm_step(step, at):
        g, base = group_at(step, at), (2 * step + at) * rows
        sums = jnp.zeros((rows, half), jnp.float32)
        squares = jnp.zeros((rows, half), jnp.float32)
        for part in range(2 * tps):
            x = rows_all[g, part].astype(jnp.float32)
            sums = sums + x
            squares = squares + x * x
        mean = jnp.sum(sums, 1, keepdims=True) / model
        square = jnp.sum(squares, 1, keepdims=True) / model
        scale = lax.rsqrt(square - mean * mean + NORM_EPS)
        for part in range(2 * tps):
            span = slice(part * half, (part + 1) * half)
            x = rows_all[g, part].astype(jnp.float32)
            y = (x - mean) * scale * first_gain[:, span]
            normed[base : base + rows, span] = y.astype(jnp.bfloat16)

    def side_step(group):
        if group == 0:
            settle(side_w, weight_sem.at[2])
        partial = lax.dot_general(
            normed[group_rows(group), side_span],
            side_w[...],
            (((1,), (1,)), ((), ())),
            preferred_element_type=jnp.float32,
        ).astype(jnp.bfloat16)
        for i, (step, at) in enumerate(blocks(group)):
            n = 2 * step + at
            side_out[n] = partial[i * rows : (i + 1) * rows]
            if n > 0:
                peer = (group_at(step, at), tp)
                push(
                    side_out.at[n],
                    side_in.at[n],
                    send_sem.at[SIDE],
                    recv_sem.at[SIDE],
                    peer,
                )

    def expert_step(group):
        if group == 0:
            settle(gate_up_w, weight_sem.at[1])
        members = blocks(group)
        stacks = [[] for _ in members]
        scales = [column(eps + group_at(step, at)) for step, at in members]
        for e in range(experts):
            both = dot(normed[group_rows(group), :], gate_up_w[e])
            hidden = silu(both[:, :hidden_width]) * both[:, hidden_width:]
            for i in range(len(members)):
                mine = hidden[i * rows : (i + 1) * rows] * scales[i][e * rows : (e + 1) * rows]
                stacks[i].append(mine.astype(jnp.bfloat16))
        number = lax.broadcasted_iota(jnp.int32, (pair_slots, 2 * wide), 0).astype(jnp.float32)
        for i, step in enumerate(groups[group]):
            near = info[pl.ds(group_at(step, 0), 1), 0:wide]
            far = info[pl.ds(group_at(step, 1), 1), 0:wide]
            far = jnp.where(far < 0.0, -1.0, far + slots)
            slot_row = jnp.concatenate([near, far], 1)
            table = jnp.where(number == slot_row, 1.0, 0.0).astype(jnp.bfloat16)
            stack = jnp.concatenate(stacks[2 * i] + stacks[2 * i + 1], 0)
            hidden_all[tp, step] = dot(table, stack).astype(jnp.bfloat16)
        own = hidden_all.at[tp, group_steps(group)]
        for peer in plane:
            push(own, own, send_sem.at[HIDDEN], recv_sem.at[HIDDEN + group], peer)

    def down_step(group):
        with jax.named_scope("hidden_wait"):
            arrived = hidden_all.at[pl.ds(0, tps - 1), group_steps(group)]
            settle(arrived, recv_sem.at[HIDDEN + group])
        if group == 0:
            settle(down_w, weight_sem.at[4])
        spread_rows = []
        number = lax.broadcasted_iota(jnp.int32, (wide, pair_slots), 1).astype(jnp.float32)
        for step in groups[group]:
            packed = jnp.concatenate([hidden_all[t, step] for t in range(tps)], 1)
            for at in range(2):
                slot = column(group_at(step, at))
                if at == 1:
                    slot = jnp.where(slot < 0.0, -1.0, slot + slots)
                table = jnp.where(number == slot, 1.0, 0.0).astype(jnp.bfloat16)
                spread_rows.append(dot(table, packed).astype(jnp.bfloat16))
        result = None
        for e in range(experts):
            mine = jnp.concatenate([r[e * rows : (e + 1) * rows] for r in spread_rows], 0)
            term = dot(mine, down_w[e])
            result = term if result is None else result + term
        for i, (step, at) in enumerate(blocks(group)):
            part = result[i * rows : (i + 1) * rows]
            if at == 0:
                total[step] = part
            else:
                pair_out[step] = part.astype(jnp.bfloat16)
        both = group_steps(group)
        push(
            pair_out.at[both],
            pair_in.at[both],
            send_sem.at[9],
            back_sem.at[group],
            partner,
        )

    def return_step(group):
        both = group_steps(group)
        with jax.named_scope("pair_wait"):
            settle(pair_in.at[both], back_sem.at[group])
        for step in groups[group]:
            mine = total[step] + pair_in[step].astype(jnp.float32)
            if step == 0:
                total[step] = mine
                continue
            line_out[step] = mine.astype(jnp.bfloat16)
            push(
                line_out.at[step],
                line_in.at[step],
                send_sem.at[10],
                back_sem.at[steps + step],
                line[step],
            )

    def own_shared():
        settle(shared_w, weight_sem.at[3])
        both = dot(normed[0:rows, :], shared_w[...])
        hidden = silu(both[:, :shared_width]) * both[:, shared_width:]
        late_all[tp, :, 0:shared_width] = hidden.astype(jnp.bfloat16)

    def own_side():
        with jax.named_scope("side_wait"):
            settle(side_in.at[pl.ds(0, eps - 1)], recv_sem.at[SIDE])
        pre = side_out[0].astype(jnp.float32)
        for n in range(1, eps):
            pre = pre + side_in[n].astype(jnp.float32)
        act = silu(pre[:, :side_width]) * pre[:, side_width:]
        act = jnp.concatenate([act, jnp.zeros_like(act)], 1)
        late_all[tp, :, shared_width : shared_width + 2 * side_width] = act.astype(jnp.bfloat16)
        for peer in plane:
            push(late_all.at[tp], late_all.at[tp], send_sem.at[LATE], recv_sem.at[LATE], peer)

    def own_switch():
        settle(side_switch, small_sem.at[5])
        row = side_switch[...].astype(jnp.float32)
        product = normed[0:rows, :].astype(jnp.float32) * row
        logit = jnp.sum(product, 1, keepdims=True)
        return 1.0 / (1.0 + jnp.exp(-logit))

    def own_extra():
        settle(shared_down_w, weight_sem.at[5])
        settle(side_down_w, weight_sem.at[6])
        with jax.named_scope("late_wait"):
            settle(late_all.at[pl.ds(0, tps - 1)], recv_sem.at[LATE])
        shared = jnp.concatenate([late_all[t, :, :shared_width] for t in range(tps)], 1)
        shared = dot(shared, shared_down_w[...])
        side = None
        for t in range(tps):
            mine = late_all[t, :, shared_width : shared_width + side_width]
            term = dot(mine, side_down_w[t * side_width : (t + 1) * side_width, :])
            side = term if side is None else side + term
        return shared + switch * side

    with jax.named_scope("relay0"):
        relay(0)
    with jax.named_scope("spread1"):
        spread(1)
    with jax.named_scope("spread2"):
        spread(2)
    with jax.named_scope("corner0"):
        corner(0)
    with jax.named_scope("relay1"):
        relay(1)
    with jax.named_scope("spread3"):
        spread(3)
    with jax.named_scope("arrive0"):
        arrive(0)
    with jax.named_scope("norm_step0_0"):
        norm_step(0, 0)
    with jax.named_scope("norm_step0_1"):
        norm_step(0, 1)
    with jax.named_scope("relay2"):
        relay(2)
    with jax.named_scope("corner1"):
        corner(1)
    with jax.named_scope("relay3"):
        relay(3)
    with jax.named_scope("arrive1"):
        arrive(1)
    with jax.named_scope("norm_step1_0"):
        norm_step(1, 0)
    with jax.named_scope("norm_step1_1"):
        norm_step(1, 1)
    with jax.named_scope("side_step0"):
        side_step(0)
    with jax.named_scope("expert_step0"):
        expert_step(0)
    with jax.named_scope("corner2"):
        corner(2)
    with jax.named_scope("corner3"):
        corner(3)
    with jax.named_scope("arrive2"):
        arrive(2)
    with jax.named_scope("norm_step2_0"):
        norm_step(2, 0)
    with jax.named_scope("norm_step2_1"):
        norm_step(2, 1)
    with jax.named_scope("side_step1"):
        side_step(1)
    with jax.named_scope("expert_step1"):
        expert_step(1)
    with jax.named_scope("arrive3"):
        arrive(3)
    with jax.named_scope("norm_step3_0"):
        norm_step(3, 0)
    with jax.named_scope("norm_step3_1"):
        norm_step(3, 1)
    with jax.named_scope("side_step2"):
        side_step(2)
    with jax.named_scope("expert_step2"):
        expert_step(2)
    with jax.named_scope("down_step0"):
        down_step(0)
    with jax.named_scope("own_shared"):
        own_shared()
    with jax.named_scope("own_switch"):
        switch = own_switch()
    with jax.named_scope("return_step0"):
        return_step(0)
    with jax.named_scope("down_step1"):
        down_step(1)
    with jax.named_scope("own_side"):
        own_side()
    with jax.named_scope("return_step1"):
        return_step(1)
    with jax.named_scope("down_step2"):
        down_step(2)
    with jax.named_scope("return_step2"):
        return_step(2)
    with jax.named_scope("own_extra"):
        extra = own_extra()

    routed = total[0]
    for step in range(1, steps):
        with jax.named_scope("line_wait"):
            settle(line_in.at[step], back_sem.at[steps + step])
        routed = routed + line_in[step].astype(jnp.float32)
    own = normed[0:rows, own_slice].astype(jnp.float32)
    pre_second = RESIDUAL_SCALE * own + routed + extra
    stats[tp, 0:1, 0:rows] = line_of(jnp.sum(pre_second, 1, keepdims=True))
    stats[tp, 1:2, 0:rows] = line_of(jnp.sum(pre_second * pre_second, 1, keepdims=True))
    for peer in plane:
        push(stats.at[tp], stats.at[tp], send_sem.at[STAT], recv_sem.at[STAT], peer)
    with jax.named_scope("stat_wait"):
        settle(stats.at[pl.ds(0, tps - 1)], recv_sem.at[STAT])
    totals = stats[0]
    for t in range(1, tps):
        totals = totals + stats[t]
    mean = column_of(totals[0:1, 0:rows]) / model
    square = column_of(totals[1:2, 0:rows]) / model
    output[...] = (pre_second - mean) * lax.rsqrt(square - mean * mean + NORM_EPS)
    with jax.named_scope("drain"):
        settle(mixed_all.at[pl.ds(0, tps - 1)], send_sem.at[MIXED])
        settle(route_all.at[pl.ds(0, eps - 1)], send_sem.at[ROUTE])
        settle(weight_all.at[pl.ds(0, eps - 1)], send_sem.at[WEIGHT])
        settle(side_out.at[pl.ds(0, eps - 1)], send_sem.at[SIDE])
        settle(late_all.at[pl.ds(0, tps - 1)], send_sem.at[LATE])
        settle(stats.at[pl.ds(0, tps - 1)], send_sem.at[STAT])
        settle(hidden_all.at[pl.ds(0, tps - 1)], send_sem.at[HIDDEN])
        settle(rows_all.at[pl.ds(0, 5), pl.ds(0, 6)], send_sem.at[7])
        settle(rows_all.at[pl.ds(0, 4)], send_sem.at[8])
        settle(pair_out, send_sem.at[9])
        settle(line_out.at[pl.ds(0, steps - 1)], send_sem.at[10])


def mixer(mixed, tokens, routes, route_weights, first_gain, side_switch, weights):
    out_w, gate_w, up_w, down_w, shared_gate, _, shared_down, side_gate, _, side_down = weights
    eps, tps = lax.axis_size("ep"), lax.axis_size("tp")
    chips = eps // 2
    rows, model = tokens.shape
    cols = model // tps
    experts, _, hidden = gate_w.shape
    top = routes.shape[0]
    total = experts * eps
    capacity = (3 * rows * top + total - 1) // total
    slots = -(-2 * experts * capacity // 16) * 16
    groups = ((0, 1), (2,), (3,))
    wide = -(-experts * rows // 128) * 128
    side_width, side_rows = side_gate.shape
    shared = shared_gate.shape[1]
    bf16, f32 = jnp.bfloat16, jnp.float32
    dma = pltpu.SemaphoreType.DMA
    line = pltpu.VMEM((chips, rows, cols), bf16)
    sides = pltpu.VMEM((eps, rows, 2 * side_width), bf16)
    return pl.pallas_call(
        functools.partial(mixer_body, (chips, tps, capacity, groups)),
        out_shape=jax.ShapeDtypeStruct((rows, cols), f32),
        in_specs=[VMEM] + [ANY] * 15,
        out_specs=VMEM,
        scratch_shapes=[
            pltpu.VMEM((rows, cols), bf16),
            pltpu.VMEM(first_gain.shape, f32),
            pltpu.VMEM(side_switch.shape, bf16),
            pltpu.VMEM((tps,) + mixed.shape, bf16),
            pltpu.VMEM((eps, top, rows), jnp.int32),
            pltpu.VMEM((eps, top, rows), f32),
            pltpu.VMEM((eps, 2 * tps, rows, cols // 2), bf16),
            pltpu.VMEM((eps * rows, model), bf16),
            pltpu.VMEM((128, wide), f32),
            pltpu.VMEM((wide, 128), f32),
            pltpu.VMEM((tps, chips, slots, hidden), bf16),
            line,
            line,
            line,
            line,
            pltpu.VMEM((chips, rows, cols), f32),
            sides,
            sides,
            pltpu.VMEM((tps, rows, shared + 2 * side_width), bf16),
            pltpu.VMEM((tps, 8, 128), f32),
            pltpu.VMEM(out_w.shape, bf16),
            pltpu.VMEM((experts, model, 2 * hidden), bf16),
            pltpu.VMEM(down_w.shape, bf16),
            pltpu.VMEM((model, 2 * shared), bf16),
            pltpu.VMEM(shared_down.shape, bf16),
            pltpu.VMEM((2 * side_width, side_rows), bf16),
            pltpu.VMEM(side_down.shape, bf16),
            dma((6,)),
            dma((7,)),
            dma((11,)),
            dma((6 + len(groups),)),
            dma((chips, 6)),
            dma((2 * chips,)),
        ],
        compiler_params=pltpu.CompilerParams(
            collective_id=0, has_side_effects=True, vmem_limit_bytes=54900 * 2**10
        ),
    )(mixed, tokens, routes, route_weights, first_gain, side_switch, *weights)


def streamed_device(
    tokens,
    retention_state,
    lengths,
    query_weight,
    key_weight,
    value_weight,
    gate_weight,
    out_weight,
    first_gain,
    routing,
    route_weight,
    expert_gate,
    expert_up,
    expert_down,
    shared_gate,
    shared_up,
    shared_down,
    side_gate,
    side_up,
    side_down,
    side_switch,
    second_gain,
):
    rows = tokens.shape[0]
    mixed, new_state = retain_kernel(
        tokens,
        lengths.reshape(1, rows),
        [query_weight, key_weight, value_weight, gate_weight],
        retention_state,
    )
    normed = mixer(
        mixed,
        tokens,
        routing.T,
        route_weight.T,
        first_gain.reshape(1, -1),
        side_switch,
        [
            out_weight,
            expert_gate,
            expert_up,
            expert_down,
            shared_gate,
            shared_up,
            shared_down,
            side_gate.T,
            side_up.T,
            side_down,
        ],
    )
    output = (normed * second_gain[None, :]).astype(jnp.bfloat16)
    return (output, new_state)


def staged_device(
    tokens,
    retention_state,
    lengths,
    query_weight,
    key_weight,
    value_weight,
    gate_weight,
    out_weight,
    first_gain,
    routing,
    route_weight,
    expert_gate,
    expert_up,
    expert_down,
    shared_gate,
    shared_up,
    shared_down,
    side_gate,
    side_up,
    side_down,
    side_switch,
    second_gain,
):
    seq_rows = tokens.shape[0]
    model_width = tokens.shape[1]
    head_count = retention_state.shape[1]
    col_count = out_weight.shape[1]
    ep_count = lax.axis_size("ep")
    tp_rank = lax.axis_index("tp")
    ep_rank = lax.axis_index("ep")
    col_start = tp_rank * col_count
    side_width = side_gate.shape[1]
    side_part = jnp.concatenate([side_gate, side_up], 1)
    side_both, every_route, every_weight, *projections = first(
        [side_part, routing.T, route_weight.T],
        tokens,
        [query_weight, key_weight, value_weight, gate_weight],
        0,
    )
    side_both = side_both.reshape(model_width, 2 * side_width)
    mixed_heads, new_state = retain(
        retention_state, lengths, projections, tp_rank * head_count
    )
    (every_mixed,) = gather([mixed_heads], "tp", 1)
    mixing = jnp.dot(
        side_by_side(every_mixed),
        out_weight,
        preferred_element_type=jnp.float32,
    )
    own_cols = lax.dynamic_slice_in_dim(tokens, col_start, col_count, 1).astype(jnp.float32)
    pre_first = RESIDUAL_SCALE * own_cols + mixing
    first_sum, first_square = row_moments(pre_first, 2)
    row_mean = first_sum / model_width
    square = first_square / model_width
    own_gain = lax.dynamic_slice_in_dim(first_gain, col_start, col_count, 0)
    normed_cols = (
        (pre_first - row_mean) * lax.rsqrt(square - row_mean * row_mean + NORM_EPS) * own_gain
    ).astype(jnp.bfloat16)
    every_rows = spread(normed_cols, 3)
    normed_full = lax.dynamic_index_in_dim(every_rows, ep_rank, 0, keepdims=False)
    every_rows = every_rows.reshape(ep_count * seq_rows, model_width)

    local_experts = expert_gate.shape[0]
    top_count = routing.shape[1]
    expert_count = local_experts * ep_count
    capacity = (3 * seq_rows * top_count + expert_count - 1) // expert_count
    total_rows = ep_count * seq_rows
    route_all = jnp.transpose(every_route, (1, 0, 2)).reshape(top_count, total_rows)
    weight_all = jnp.transpose(every_weight, (1, 0, 2)).reshape(top_count, total_rows)
    local_ids = ep_rank * local_experts + jnp.arange(local_experts, dtype=jnp.int32)
    named = route_all[None, :, :] == local_ids[:, None, None]
    member = jnp.any(named, 1)
    pair_weight = jnp.sum(jnp.where(named, weight_all[None, :, :], 0.0), 1)
    index = jnp.arange(total_rows, dtype=jnp.int32)
    group = index // seq_rows
    earlier = ((index[:, None] < index[None, :]) & (group[:, None] == group[None, :])).astype(
        jnp.bfloat16
    )
    before = jnp.dot(
        member.astype(jnp.bfloat16), earlier, preferred_element_type=jnp.float32
    ).astype(jnp.int32)
    slot = jnp.where(member, group[None, :] * capacity + before, -1)
    slot_total = ep_count * capacity
    hit = slot[:, None, :] == jnp.arange(slot_total, dtype=jnp.int32)[None, :, None]
    table = hit.astype(jnp.bfloat16).reshape(local_experts * slot_total, total_rows)
    slot_weight = jnp.sum(jnp.where(hit, pair_weight[:, None, :], 0.0), -1, keepdims=True)
    chosen = (
        jnp.dot(table, every_rows, preferred_element_type=jnp.float32)
        .astype(jnp.bfloat16)
        .reshape(local_experts, slot_total, model_width)
    )
    gate_part = jnp.einsum("jcd,jdf->jcf", chosen, expert_gate, preferred_element_type=jnp.float32)
    up_part = jnp.einsum("jcd,jdf->jcf", chosen, expert_up, preferred_element_type=jnp.float32)
    hidden = (jax.nn.silu(gate_part) * up_part * slot_weight).astype(jnp.bfloat16)

    side_pre = jnp.dot(normed_full, side_both, preferred_element_type=jnp.float32)
    side_hidden = (jax.nn.silu(side_pre[:, :side_width]) * side_pre[:, side_width:]).astype(
        jnp.bfloat16
    )
    shared_hidden = (
        jax.nn.silu(jnp.dot(normed_full, shared_gate, preferred_element_type=jnp.float32))
        * jnp.dot(normed_full, shared_up, preferred_element_type=jnp.float32)
    ).astype(jnp.bfloat16)
    hidden_blocks, shared_blocks, side_blocks = gather(
        [hidden.reshape(local_experts * slot_total, -1), shared_hidden, side_hidden], "tp", 4
    )
    hidden_all = side_by_side(hidden_blocks).reshape(local_experts, slot_total, -1)
    result = (
        jnp.einsum("jcf,jfd->jcd", hidden_all, expert_down, preferred_element_type=jnp.float32)
        .astype(jnp.bfloat16)
        .reshape(local_experts * slot_total, col_count)
    )
    summed = (
        lax.dot_general(
            table, result, (((0,), (0,)), ((), ())), preferred_element_type=jnp.float32
        )
        .astype(jnp.bfloat16)
        .reshape(ep_count, seq_rows, col_count)
    )
    returned = scatter(summed, 5)
    routed = jnp.sum(returned.astype(jnp.float32), 0)
    shared_out = jnp.dot(
        side_by_side(shared_blocks), shared_down, preferred_element_type=jnp.float32
    )
    side_out = jnp.dot(side_by_side(side_blocks), side_down, preferred_element_type=jnp.float32)
    switch = jax.nn.sigmoid(
        jnp.sum(normed_full.astype(jnp.float32) * side_switch.astype(jnp.float32)[None, :], -1)
    )
    pre_second = (
        RESIDUAL_SCALE * normed_cols.astype(jnp.float32)
        + routed
        + shared_out
        + switch[:, None] * side_out
    )
    second_sum, second_square = row_moments(pre_second, 6)
    mean_second = second_sum / model_width
    square_second = second_square / model_width
    output = (
        (pre_second - mean_second)
        * lax.rsqrt(square_second - mean_second * mean_second + NORM_EPS)
        * second_gain
    ).astype(jnp.bfloat16)
    return (output, new_state)


def on_device(*arrays):
    tokens, state, expert_gate, side_gate = arrays[0], arrays[1], arrays[11], arrays[17]
    eps, tps = lax.axis_size("ep"), lax.axis_size("tp")
    rows, model = tokens.shape
    fits = (
        eps == 8
        and tps == 4
        and rows % 16 == 0
        and model % (256 * tps) == 0
        and state.shape[1] * state.shape[2] % 128 == 0
        and expert_gate.shape[2] % 128 == 0
        and side_gate.shape[0] % 128 == 0
        and side_gate.shape[1] == 64
    )
    return (streamed_device if fits else staged_device)(*arrays)


def solution(mesh):
    return jax.shard_map(
        on_device,
        mesh=mesh,
        in_specs=(
            P("ep", None),
            P("ep", "tp", None, None),
            P("ep"),
            P(None, "tp"),
            P(None, "tp"),
            P(None, "tp"),
            P(None, "tp"),
            P(None, "tp"),
            P(),
            P("ep", None),
            P("ep", None),
            P("ep", None, "tp"),
            P("ep", None, "tp"),
            P("ep", None, "tp"),
            P(None, "tp"),
            P(None, "tp"),
            P(None, "tp"),
            P("ep", "tp"),
            P("ep", "tp"),
            P(None, "tp"),
            P(),
            P("tp"),
        ),
        out_specs=(P("ep", "tp"), P("ep", "tp", None, None)),
        check_vma=False,
    )
```

```python
import functools

import jax
import jax.numpy as jnp
from jax import lax
from jax.experimental import pallas as pl
from jax.experimental.pallas import tpu as pltpu
from jax.sharding import PartitionSpec as P

HEADS = 16


RESIDUAL_SCALE = 2.0**0.25
NORM_EPS = 1e-05
GROUP_EPS = 1e-06
ROPE_BASE = 10000.0


def rotate(vector, positions):
    half_width = vector.shape[-1] // 2
    frequency = ROPE_BASE ** (-jnp.arange(half_width, dtype=jnp.float32) / half_width)
    angles = positions.astype(jnp.float32)[:, None, None] * frequency[None, None, :]
    cosine = jnp.cos(angles)
    sine_part = jnp.sin(angles)
    first_half = vector[..., :half_width]
    second_half = vector[..., half_width:]
    return jnp.concatenate(
        [
            first_half * cosine - second_half * sine_part,
            second_half * cosine + first_half * sine_part,
        ],
        -1,
    )


def retain(
    retention_state,
    lengths,
    projections,
    first_head,
):
    row_count = retention_state.shape[0]
    head_count = retention_state.shape[1]
    head_width = retention_state.shape[2]

    query_rows, key_part, value_part, gate_part = [part.astype(jnp.float32) for part in projections]
    queries = rotate(query_rows.reshape(row_count, head_count, head_width), lengths)
    key_rows = rotate(
        key_part.reshape(row_count, head_count, head_width), lengths
    ) * head_width ** (-0.5)
    values = value_part.reshape(row_count, head_count, head_width)
    gate_act = gate_part
    head_index = (first_head + jnp.arange(head_count)).astype(jnp.float32)
    decays = 1.0 - 2.0 ** (-5.0 - 7.0 * head_index / (HEADS - 1))
    own_term = jnp.sum(queries * key_rows, -1, keepdims=True) * values
    carried = decays[None, :, None] * jnp.sum(queries[:, :, :, None] * retention_state, 2)
    result = own_term + carried
    new_state = (
        decays[None, :, None, None] * retention_state
        + key_rows[:, :, :, None] * values[:, :, None, :]
    )
    normed = result * lax.rsqrt(jnp.mean(result * result, -1, keepdims=True) + GROUP_EPS)
    mixed_heads = (
        normed.reshape(row_count, head_count * head_width) * jax.nn.silu(gate_act)
    ).astype(jnp.bfloat16)
    return (mixed_heads, new_state)


VMEM = pl.BlockSpec(memory_space=pltpu.VMEM)
DEVICE = pl.DeviceIdType.MESH


def enter(peers):
    barrier = pltpu.get_barrier_semaphore()
    for peer in peers:
        pl.semaphore_signal(barrier, inc=1, device_id=peer, device_id_type=DEVICE)
    pl.semaphore_wait(barrier, len(peers))


def send(source, target, send_sem, recv_sem, peer):
    copy = pltpu.make_async_remote_copy(
        src_ref=source,
        dst_ref=target,
        send_sem=send_sem,
        recv_sem=recv_sem,
        device_id=peer,
        device_id_type=DEVICE,
    )
    copy.start()
    return copy


def on_axis(axis, index):
    if axis == "ep":
        return (index, lax.axis_index("tp"))
    return (lax.axis_index("ep"), index)


def gather_body(axis, count, parts, *refs):
    sources, targets = refs[:parts], refs[parts : 2 * parts]
    send_sem, recv_sem, local_sem = refs[2 * parts :]
    me = lax.axis_index(axis)
    others = [lax.rem(me + step, count) for step in range(1, count)]
    locals_ = []
    for part in range(parts):
        own = pltpu.make_async_copy(sources[part], targets[part].at[me], local_sem.at[part])
        own.start()
        locals_.append(own)
    enter([on_axis(axis, other) for other in others])
    copies = []
    for step, other in enumerate(others):
        for part in range(parts):
            copies.append(
                send(
                    sources[part],
                    targets[part].at[me],
                    send_sem.at[step, part],
                    recv_sem.at[step, part],
                    on_axis(axis, other),
                )
            )
    for copy in locals_:
        copy.wait()
    for copy in copies:
        copy.wait()


def gather(arrays, axis, ident):
    count, parts = lax.axis_size(axis), len(arrays)
    return pl.pallas_call(
        functools.partial(gather_body, axis, count, parts),
        out_shape=[jax.ShapeDtypeStruct((count,) + a.shape, a.dtype) for a in arrays],
        in_specs=[VMEM] * parts,
        out_specs=[VMEM] * parts,
        scratch_shapes=[
            pltpu.SemaphoreType.DMA((count - 1, parts)),
            pltpu.SemaphoreType.DMA((count - 1, parts)),
            pltpu.SemaphoreType.DMA((parts,)),
        ],
        compiler_params=pltpu.CompilerParams(collective_id=ident, has_side_effects=True),
    )(*arrays)


def scatter_body(count, source, target, send_sem, recv_sem, local_sem):
    me = lax.axis_index("ep")
    others = [lax.rem(me + step, count) for step in range(1, count)]
    own = pltpu.make_async_copy(source.at[me], target.at[me], local_sem)
    own.start()
    enter([on_axis("ep", other) for other in others])
    copies = [
        send(
            source.at[other],
            target.at[me],
            send_sem.at[step],
            recv_sem.at[step],
            on_axis("ep", other),
        )
        for step, other in enumerate(others)
    ]
    own.wait()
    for copy in copies:
        copy.wait()


def scatter(array, ident):
    count = array.shape[0]
    return pl.pallas_call(
        functools.partial(scatter_body, count),
        out_shape=jax.ShapeDtypeStruct(array.shape, array.dtype),
        in_specs=[VMEM],
        out_specs=VMEM,
        scratch_shapes=[
            pltpu.SemaphoreType.DMA((count - 1,)),
            pltpu.SemaphoreType.DMA((count - 1,)),
            pltpu.SemaphoreType.DMA,
        ],
        compiler_params=pltpu.CompilerParams(collective_id=ident, has_side_effects=True),
    )(array)


def first_body(count, *refs):
    parts = 3
    sources, (tokens, *weights) = refs[:parts], refs[parts : parts + 5]
    targets = refs[parts + 5 : 2 * parts + 5]
    results = refs[2 * parts + 5 : 2 * parts + 9]
    send_sem, recv_sem, local_sem = refs[2 * parts + 9 :]
    chips = count // 2
    me = lax.axis_index("ep")
    chip, core = me // 2, lax.rem(me, 2)
    partner = on_axis("ep", chip * 2 + 1 - core)
    line = [lax.rem(chip + step, chips) * 2 + core for step in range(1, chips)]
    senders = [lax.rem(chip + chips - step, chips) * 2 + core for step in range(1, chips)]
    locals_ = []
    for part in range(parts):
        own = pltpu.make_async_copy(sources[part], targets[part].at[me], local_sem.at[part])
        own.start()
        locals_.append(own)
    enter([on_axis("ep", other) for other in line] + [partner])
    direct, copies = [], []
    for step, other in enumerate(line):
        for part in range(parts):
            direct.append(
                send(
                    sources[part],
                    targets[part].at[me],
                    send_sem.at[step, part],
                    recv_sem.at[step, part],
                    on_axis("ep", other),
                )
            )
    for part in range(parts):
        copies.append(
            send(
                sources[part],
                targets[part].at[me],
                send_sem.at[chips - 1, part],
                recv_sem.at[chips - 1, part],
                partner,
            )
        )
    for weight, result in zip(weights, results):
        result[...] = jnp.dot(
            tokens[...], weight[...], preferred_element_type=jnp.float32
        ).astype(result.dtype)
    for step, sender in enumerate(senders):
        for part in range(parts):
            direct[step * parts + part].wait_recv()
            copies.append(
                send(
                    targets[part].at[sender],
                    targets[part].at[sender],
                    send_sem.at[chips + step, part],
                    recv_sem.at[chips + step, part],
                    partner,
                )
            )
    for copy in locals_:
        copy.wait()
    for copy in direct:
        copy.wait_send()
    for copy in copies:
        copy.wait()


def first(arrays, tokens, weights, ident):
    count, parts = lax.axis_size("ep"), len(arrays)
    rows = tokens.shape[0]
    return pl.pallas_call(
        functools.partial(first_body, count),
        out_shape=[jax.ShapeDtypeStruct((count,) + a.shape, a.dtype) for a in arrays]
        + [jax.ShapeDtypeStruct((rows, w.shape[1]), jnp.bfloat16) for w in weights],
        in_specs=[VMEM] * (parts + 5),
        out_specs=[VMEM] * (parts + 4),
        scratch_shapes=[
            pltpu.SemaphoreType.DMA((count - 1, parts)),
            pltpu.SemaphoreType.DMA((count - 1, parts)),
            pltpu.SemaphoreType.DMA((parts,)),
        ],
        compiler_params=pltpu.CompilerParams(collective_id=ident, has_side_effects=True),
    )(*arrays, tokens, *weights)


def spread_body(count, tp_count, source, target, send_sem, recv_sem, local_sem):
    chips, width = count // 2, source.shape[1]
    me, own_tp = lax.axis_index("ep"), lax.axis_index("tp")
    chip, core = me // 2, lax.rem(me, 2)
    partner = (chip * 2 + 1 - core, own_tp)

    def place(row, col):
        return target.at[row, :, pl.ds(pl.multiple_of(col * width, width), width)]

    def chip_at(step):
        return lax.rem(chip + chips + step, chips) * 2 + core

    def tp_at(step):
        return lax.rem(own_tp + tp_count + step, tp_count)

    own = pltpu.make_async_copy(source, place(me, own_tp), local_sem)
    own.start()
    line = [(chip_at(step), own_tp) for step in range(1, chips)]
    plane = [(me, tp_at(step)) for step in range(1, tp_count)]
    enter(line + plane + [partner])

    def pair(line_step, plane_step, to_partner):
        return (
            send_sem.at[to_partner, line_step, plane_step],
            recv_sem.at[to_partner, line_step, plane_step],
        )

    direct, planar, copies = [], {}, []
    for step in range(1, chips):
        direct.append(send(source, place(me, own_tp), *pair(step, 0, 0), line[step - 1]))
    for step in range(1, tp_count):
        planar[(0, step)] = send(source, place(me, own_tp), *pair(0, step, 0), plane[step - 1])
    copies.append(send(source, place(me, own_tp), *pair(0, 0, 1), partner))
    for line_step in range(1, chips):
        direct[line_step - 1].wait_recv()
        block = place(chip_at(-line_step), own_tp)
        for step in range(1, tp_count):
            planar[(line_step, step)] = send(
                block, block, *pair(line_step, step, 0), plane[step - 1]
            )
        copies.append(send(block, block, *pair(line_step, 0, 1), partner))
    for line_step in range(chips):
        for step in range(1, tp_count):
            planar[(line_step, step)].wait_recv()
            block = place(chip_at(-line_step), tp_at(-step))
            copies.append(send(block, block, *pair(line_step, step, 1), partner))
    own.wait()
    for copy in direct:
        copy.wait_send()
    for copy in planar.values():
        copy.wait_send()
    for copy in copies:
        copy.wait()


def spread(block, ident):
    count, tp_count = lax.axis_size("ep"), lax.axis_size("tp")
    rows, width = block.shape
    return pl.pallas_call(
        functools.partial(spread_body, count, tp_count),
        out_shape=jax.ShapeDtypeStruct((count, rows, width * tp_count), block.dtype),
        in_specs=[VMEM],
        out_specs=VMEM,
        scratch_shapes=[
            pltpu.SemaphoreType.DMA((2, count // 2, tp_count)),
            pltpu.SemaphoreType.DMA((2, count // 2, tp_count)),
            pltpu.SemaphoreType.DMA,
        ],
        compiler_params=pltpu.CompilerParams(collective_id=ident, has_side_effects=True),
    )(block)


def side_by_side(gathered):
    return jnp.concatenate([gathered[i] for i in range(gathered.shape[0])], -1)


def row_moments(values, ident):
    sums = jnp.stack([jnp.sum(values, -1), jnp.sum(values * values, -1)])
    (every,) = gather([sums], "tp", ident)
    totals = jnp.sum(every, 0)
    return totals[0][:, None], totals[1][:, None]


ANY = pl.BlockSpec(memory_space=pl.ANY)


def dot(a, b):
    return jnp.dot(a, b, preferred_element_type=jnp.float32)


def silu(x):
    return x / (1.0 + jnp.exp(-x))


def fetch(source, target, sem):
    copy = pltpu.make_async_copy(source, target, sem)
    copy.start()
    return copy


def settle(ref, sem):
    pltpu.make_async_copy(ref, ref, sem).wait()


def on_diagonal(rows):
    row = lax.broadcasted_iota(jnp.int32, (rows, rows), 0)
    return row == lax.broadcasted_iota(jnp.int32, (rows, rows), 1)


def column_of(line):
    return jnp.sum(jnp.where(on_diagonal(line.shape[1]), line, 0.0), 1, keepdims=True)


def line_of(column):
    return jnp.sum(jnp.where(on_diagonal(column.shape[0]), column, 0.0), 0, keepdims=True)


def rotated(x, cosine, sine, half):
    width = x.shape[1]
    lane = lax.broadcasted_iota(jnp.int32, x.shape, 1)
    first = (lane & (2 * half - 1)) < half
    later = pltpu.roll(x, width - half, 1)
    sooner = pltpu.roll(x, half, 1)
    return x * cosine + jnp.where(first, -later, sooner) * sine


def retain_body(
    chunk,
    tokens_in,
    lengths_in,
    query_in,
    key_in,
    value_in,
    gate_in,
    state_in,
    mixed,
    state_out,
    tokens,
    lengths,
    weights,
    state,
    columns,
    spread_even,
    spread_odd,
    values,
    carried,
    small_sem,
    weight_sem,
    state_sem,
    out_sem,
):
    rows, heads, width = state.shape[0], state.shape[1], state.shape[2]
    total = heads * width
    chunks = rows // chunk
    small = [
        fetch(source, target, small_sem.at[i])
        for i, (source, target) in enumerate(
            [(lengths_in, lengths), (tokens_in, tokens)]
        )
    ]
    for i, source in enumerate([query_in, key_in, value_in, gate_in]):
        fetch(source, weights.at[:, pl.ds(i * total, total)], weight_sem.at[i // 2])

    with jax.named_scope("small_wait"):
        small[0].wait()
    for i in range(chunks):
        piece = pl.ds(i * chunk, chunk)
        fetch(state_in.at[piece], state.at[piece], state_sem.at[i])
    position = column_of(lengths[...].astype(jnp.float32))
    lane = lax.broadcasted_iota(jnp.int32, (1, total), 1) & (width // 2 - 1)
    frequency = jnp.zeros((1, total), jnp.float32)
    for i in range(width // 2):
        frequency = jnp.where(lane == i, ROPE_BASE ** (-i / (width // 2)), frequency)
    angles = position * frequency
    cosine, sine = jnp.cos(angles), jnp.sin(angles)
    first_head = lax.axis_index("tp") * heads
    decays = []
    for head in range(heads):
        index = jnp.full((1, width), first_head + head, jnp.int32).astype(jnp.float32)
        decays.append(1.0 - jnp.exp2(-5.0 - 7.0 * index / (HEADS - 1)))

    def project(i):
        span = pl.ds(2 * i * total, 2 * total)
        with jax.named_scope("weight_wait"):
            settle(weights.at[:, span], weight_sem.at[i])
        both = dot(tokens[...], weights[:, span]).astype(jnp.bfloat16).astype(jnp.float32)
        return both[:, :total], both[:, total:]

    with jax.named_scope("small_wait"):
        small[1].wait()
    query, key = project(0)
    value, gate = project(1)
    lanes = columns.shape[1]
    for i, (x, scale) in enumerate([(query, 1.0), (key, width ** (-0.5))]):
        turned = rotated(x, cosine, sine, width // 2) * scale
        padded = jnp.concatenate([turned, jnp.zeros((lanes - rows, total), jnp.float32)], 0)
        columns[i * total : (i + 1) * total, :] = jnp.transpose(padded).astype(jnp.bfloat16)
    for head in range(heads):
        values[head] = value[:, head * width : (head + 1) * width]

    source_lane = lax.broadcasted_iota(jnp.int32, (lanes, 2 * lanes), 0)
    target_lane = lax.broadcasted_iota(jnp.int32, (lanes, 2 * lanes), 1)
    offset = jnp.where(target_lane >= lanes, 1, 0)
    buffers = [spread_even, spread_odd]

    def widen(i, pair, half):
        pick = jnp.where(source_lane == offset + (i * chunk + 2 * pair), 1.0, 0.0)
        span = slice(half * total, (half + 1) * total)
        buffers[i % 2][pair, span] = dot(columns[span, :], pick.astype(jnp.bfloat16))

    for pair in range(chunk):
        widen(0, pair // 2, pair % 2)
    for i in range(chunks):
        base = i * chunk
        piece = pl.ds(base, chunk)
        with jax.named_scope("state_wait"):
            pltpu.make_async_copy(state_in.at[piece], state.at[piece], state_sem.at[i]).wait()
        wide = buffers[i % 2]
        for at in range(chunk):
            if i + 1 < chunks:
                widen(i + 1, at // 2, at % 2)
            if at == chunk // 2:
                part = pl.ds(base, chunk // 2)
                fetch(state.at[part], state_out.at[part], out_sem)
            lane = (at % 2) * lanes
            for head in range(heads):
                low, high = head * width, (head + 1) * width
                q_cols = wide[at // 2, low:high, lane : lane + width]
                k_cols = wide[at // 2, total + low : total + high, lane : lane + width]
                v_row = values[head, base + at : base + at + 1, :]
                new = decays[head] * state[base + at, head] + k_cols * v_row
                state[base + at, head] = new
                carried[head, base + at : base + at + 1, :] = jnp.sum(
                    q_cols * new, 0, keepdims=True
                )
        part = pl.ds(base + chunk // 2, chunk // 2)
        fetch(state.at[part], state_out.at[part], out_sem)
    parts = []
    for head in range(heads):
        result = carried[head]
        scale = lax.rsqrt(jnp.mean(result * result, -1, keepdims=True) + GROUP_EPS)
        parts.append(result * scale)
    mixed[...] = (jnp.concatenate(parts, 1) * silu(gate)).astype(mixed.dtype)
    with jax.named_scope("state_drain"):
        settle(state, out_sem)


def retain_kernel(tokens, lengths, weights, state):
    rows, heads, width = state.shape[0], state.shape[1], state.shape[2]
    chunk, lanes = 8, 128
    cols = heads * width
    wide = pltpu.VMEM((chunk // 2, 2 * cols, 2 * lanes), jnp.float32)
    return pl.pallas_call(
        functools.partial(retain_body, chunk),
        out_shape=[
            jax.ShapeDtypeStruct((rows, cols), jnp.bfloat16),
            jax.ShapeDtypeStruct(state.shape, state.dtype),
        ],
        in_specs=[ANY] * 7,
        out_specs=[VMEM, ANY],
        compiler_params=pltpu.CompilerParams(vmem_limit_bytes=55200 * 2**10),
        scratch_shapes=[
            pltpu.VMEM(tokens.shape, tokens.dtype),
            pltpu.VMEM(lengths.shape, lengths.dtype),
            pltpu.VMEM((tokens.shape[1], 4 * cols), jnp.bfloat16),
            pltpu.VMEM(state.shape, state.dtype),
            pltpu.VMEM((2 * cols, lanes), jnp.bfloat16),
            wide,
            wide,
            pltpu.VMEM((heads, rows, width), jnp.float32),
            pltpu.VMEM((heads, rows, width), jnp.float32),
            pltpu.SemaphoreType.DMA((2,)),
            pltpu.SemaphoreType.DMA((2,)),
            pltpu.SemaphoreType.DMA((rows // chunk,)),
            pltpu.SemaphoreType.DMA,
        ],
    )(tokens, lengths, *weights, state)


def mixer_body(
    dims,
    mixed_in,
    tokens_in,
    routes_in,
    route_weights_in,
    first_gain_in,
    side_switch_in,
    out_in,
    gate_in,
    up_in,
    down_in,
    shared_gate_in,
    shared_up_in,
    shared_down_in,
    side_gate_in,
    side_up_in,
    side_down_in,
    output,
    own_tokens,
    first_gain,
    side_switch,
    mixed_all,
    route_all,
    weight_all,
    rows_all,
    normed,
    info,
    info_cols,
    hidden_all,
    pair_out,
    pair_in,
    line_out,
    line_in,
    total,
    side_out,
    side_in,
    late_all,
    stats,
    out_w,
    gate_up_w,
    down_w,
    shared_w,
    shared_down_w,
    side_w,
    side_down_w,
    small_sem,
    weight_sem,
    send_sem,
    recv_sem,
    row_sem,
    back_sem,
):
    chips, tps, capacity, groups = dims
    steps = chips
    rows, cols = own_tokens.shape
    model = cols * tps
    half = cols // 2
    experts, hidden_width = gate_in.shape[0], gate_in.shape[2]
    slots = experts * capacity
    pair_slots = hidden_all.shape[2]
    side_width = side_gate_in.shape[0]
    side_rows = side_gate_in.shape[1]
    shared_width = shared_gate_in.shape[1]
    tp = lax.axis_index("tp")
    ep = lax.axis_index("ep")
    eps = 2 * chips
    chip, core = ep // 2, lax.rem(ep, 2)
    partner = (chip * 2 + 1 - core, tp)
    low, high = lax.rem(tp, 2), tp // 2
    tp_x = high * 2 + 1 - low
    tp_y = (1 - high) * 2 + low
    tp_d = (1 - high) * 2 + 1 - low
    plane = [(ep, tp_x), (ep, tp_y), (ep, tp_d)]

    def chip_at(step):
        if step == 0:
            return chip
        if step == 1:
            return chip + 1 - 2 * lax.rem(chip, 2)
        if step == 2:
            return lax.rem(chip + 2, 4)
        return 3 - chip

    def group_at(step, at):
        return chip_at(step) * 2 + (core if at == 0 else 1 - core)

    line = [(group_at(step, 0), tp) for step in range(steps)]
    others = [(group_at(s, at), tp) for s in range(steps) for at in range(2) if s + at > 0]
    peers = plane + others
    barrier = pltpu.get_barrier_semaphore()
    for peer in peers:
        pl.semaphore_signal(barrier, inc=1, device_id=peer, device_id_type=DEVICE)

    own_mixed = mixed_all.at[tp]
    own_slice = pl.ds(pl.multiple_of(tp * cols, cols), cols)
    fetch(routes_in, route_all.at[ep], small_sem.at[1])
    fetch(route_weights_in, weight_all.at[ep], small_sem.at[2])
    fetch(tokens_in.at[:, own_slice], own_tokens, small_sem.at[3])
    fetch(out_in, out_w, weight_sem.at[0])
    MIXED, ROUTE, WEIGHT, SIDE, LATE, STAT, HIDDEN = 0, 1, 2, 3, 4, 5, 6

    def push(source, target, sent, received, peer):
        send(source, target, sent, received, peer)

    with jax.named_scope("small_wait"):
        settle(route_all.at[ep], small_sem.at[1])
        settle(weight_all.at[ep], small_sem.at[2])
    fetch(first_gain_in, first_gain, small_sem.at[4])
    fetch(side_switch_in, side_switch, small_sem.at[5])
    for e in range(experts):
        fetch(gate_in.at[e], gate_up_w.at[e, :, pl.ds(0, hidden_width)], weight_sem.at[1])
        fetch(up_in.at[e], gate_up_w.at[e, :, pl.ds(hidden_width, hidden_width)], weight_sem.at[1])
    fetch(side_gate_in, side_w.at[pl.ds(0, side_width)], weight_sem.at[2])
    fetch(side_up_in, side_w.at[pl.ds(side_width, side_width)], weight_sem.at[2])
    fetch(shared_gate_in, shared_w.at[:, pl.ds(0, shared_width)], weight_sem.at[3])
    fetch(shared_up_in, shared_w.at[:, pl.ds(shared_width, shared_width)], weight_sem.at[3])
    fetch(down_in, down_w, weight_sem.at[4])
    fetch(shared_down_in, shared_down_w, weight_sem.at[5])
    fetch(side_down_in, side_down_w, weight_sem.at[6])
    with jax.named_scope("enter"):
        pl.semaphore_wait(barrier, len(peers))

    for peer in plane:
        push(mixed_in, own_mixed, send_sem.at[MIXED], recv_sem.at[MIXED], peer)
    for peer in others:
        own = route_all.at[ep]
        push(own, own, send_sem.at[ROUTE], recv_sem.at[ROUTE], peer)
        own = weight_all.at[ep]
        push(own, own, send_sem.at[WEIGHT], recv_sem.at[WEIGHT], peer)

    mixed_all[tp] = mixed_in[...]
    with jax.named_scope("out_wait"):
        settle(own_tokens, small_sem.at[3])
        settle(out_w, weight_sem.at[0])
    with jax.named_scope("mixed_wait"):
        settle(mixed_all.at[pl.ds(0, tps - 1)], recv_sem.at[MIXED])
    heads_all = jnp.concatenate([mixed_all[t] for t in range(tps)], 1)
    pre_first = RESIDUAL_SCALE * own_tokens[...].astype(jnp.float32) + dot(heads_all, out_w[...])
    for part in range(2):
        rows_all[ep, 2 * tp + part] = pre_first[:, part * half : (part + 1) * half].astype(
            jnp.bfloat16
        )

    def block(step, index):
        return rows_all.at[group_at(step, 0), pl.ds(2 * index, 2)]

    def piece(step, index, part):
        return rows_all.at[group_at(step, 0), 2 * index + part]

    def push_rows(ref, step, kind, peer):
        sent = send_sem.at[8] if kind == 5 else send_sem.at[7]
        push(ref, ref, sent, row_sem.at[step, kind], peer)

    def came(ref, step, kind):
        settle(ref, row_sem.at[step, kind])

    def spread(step):
        ref = block(step, tp)
        if step > 0:
            came(ref, step, 0)
        for i, peer in enumerate(plane):
            push_rows(ref, step, 1 + i, peer)
        push_rows(ref, step, 5, partner)

    def relay(step):
        for i, index in enumerate([tp_x, tp_y]):
            came(block(step, index), step, 1 + i)
            push_rows(block(step, index), step, 5, partner)

    def corner(step):
        came(block(step, tp_d), step, 3)
        push_rows(block(step, tp_d), step, 5, partner)

    def arrive(step):
        came(rows_all.at[group_at(step, 1)], step, 5)

    with jax.named_scope("spread0"):
        spread(0)
        for step in range(1, steps):
            push_rows_to = line[step]
            push(block(0, tp), block(0, tp), send_sem.at[7], row_sem.at[step, 0], push_rows_to)

    with jax.named_scope("route_wait"):
        settle(route_all.at[pl.ds(0, eps - 1)], recv_sem.at[ROUTE])
        settle(weight_all.at[pl.ds(0, eps - 1)], recv_sem.at[WEIGHT])
    wide = experts * rows

    def expert_of(index):
        return sum(jnp.where(index >= e * rows, 1, 0) for e in range(1, experts))

    group_lane = expert_of(lax.broadcasted_iota(jnp.int32, (1, wide), 1))
    expert_lane = ep * experts + group_lane
    info[...] = jnp.zeros_like(info)
    for g in range(eps):
        ids = jnp.concatenate([route_all[g]] * experts, 1)
        hits = ids == expert_lane
        scales = jnp.concatenate([weight_all[g]] * experts, 1)
        info[g : g + 1, 0:wide] = jnp.sum(jnp.where(hits, 1.0, 0.0), 0, keepdims=True)
        info[eps + g : eps + g + 1, 0:wide] = jnp.sum(
            jnp.where(hits, scales, 0.0), 0, keepdims=True
        )
    member = info[0:eps, 0:wide]
    sooner = lax.broadcasted_iota(jnp.int32, (wide, wide), 0)
    later = lax.broadcasted_iota(jnp.int32, (wide, wide), 1)
    earlier = jnp.where(
        (sooner < later) & (expert_of(sooner) == expert_of(later)), 1.0, 0.0
    ).astype(jnp.bfloat16)
    before = dot(member.astype(jnp.bfloat16), earlier)
    start = (group_lane * capacity).astype(jnp.float32)
    info[0:eps, 0:wide] = jnp.where(member > 0.5, before + start, -1.0)
    info_cols[...] = jnp.transpose(info[...])
    settle(first_gain, small_sem.at[4])

    def column(index):
        lane = lax.broadcasted_iota(jnp.int32, (wide, info_cols.shape[1]), 1)
        picked = jnp.where(lane == index, info_cols[0:wide, :], 0.0)
        return jnp.sum(picked, 1, keepdims=True)

    side_span = pl.ds(pl.multiple_of(ep * side_rows, side_rows), side_rows)

    def blocks(group):
        return [(step, at) for step in groups[group] for at in range(2)]

    def group_rows(group):
        return slice(2 * groups[group][0] * rows, 2 * (groups[group][-1] + 1) * rows)

    def group_steps(group):
        return pl.ds(groups[group][0], len(groups[group]))

    def norm_step(step, at):
        g, base = group_at(step, at), (2 * step + at) * rows
        sums = jnp.zeros((rows, half), jnp.float32)
        squares = jnp.zeros((rows, half), jnp.float32)
        for part in range(2 * tps):
            x = rows_all[g, part].astype(jnp.float32)
            sums = sums + x
            squares = squares + x * x
        mean = jnp.sum(sums, 1, keepdims=True) / model
        square = jnp.sum(squares, 1, keepdims=True) / model
        scale = lax.rsqrt(square - mean * mean + NORM_EPS)
        for part in range(2 * tps):
            span = slice(part * half, (part + 1) * half)
            x = rows_all[g, part].astype(jnp.float32)
            y = (x - mean) * scale * first_gain[:, span]
            normed[base : base + rows, span] = y.astype(jnp.bfloat16)

    def side_step(group):
        if group == 0:
            settle(side_w, weight_sem.at[2])
        partial = lax.dot_general(
            normed[group_rows(group), side_span],
            side_w[...],
            (((1,), (1,)), ((), ())),
            preferred_element_type=jnp.float32,
        ).astype(jnp.bfloat16)
        for i, (step, at) in enumerate(blocks(group)):
            n = 2 * step + at
            side_out[n] = partial[i * rows : (i + 1) * rows]
            if n > 0:
                peer = (group_at(step, at), tp)
                push(
                    side_out.at[n],
                    side_in.at[n],
                    send_sem.at[SIDE],
                    recv_sem.at[SIDE],
                    peer,
                )

    def expert_step(group):
        if group == 0:
            settle(gate_up_w, weight_sem.at[1])
        members = blocks(group)
        stacks = [[] for _ in members]
        scales = [column(eps + group_at(step, at)) for step, at in members]
        for e in range(experts):
            both = dot(normed[group_rows(group), :], gate_up_w[e])
            hidden = silu(both[:, :hidden_width]) * both[:, hidden_width:]
            for i in range(len(members)):
                mine = hidden[i * rows : (i + 1) * rows] * scales[i][e * rows : (e + 1) * rows]
                stacks[i].append(mine.astype(jnp.bfloat16))
        number = lax.broadcasted_iota(jnp.int32, (pair_slots, 2 * wide), 0).astype(jnp.float32)
        for i, step in enumerate(groups[group]):
            near = info[pl.ds(group_at(step, 0), 1), 0:wide]
            far = info[pl.ds(group_at(step, 1), 1), 0:wide]
            far = jnp.where(far < 0.0, -1.0, far + slots)
            slot_row = jnp.concatenate([near, far], 1)
            table = jnp.where(number == slot_row, 1.0, 0.0).astype(jnp.bfloat16)
            stack = jnp.concatenate(stacks[2 * i] + stacks[2 * i + 1], 0)
            hidden_all[tp, step] = dot(table, stack).astype(jnp.bfloat16)
        own = hidden_all.at[tp, group_steps(group)]
        for peer in plane:
            push(own, own, send_sem.at[HIDDEN], recv_sem.at[HIDDEN + group], peer)

    def down_step(group):
        with jax.named_scope("hidden_wait"):
            arrived = hidden_all.at[pl.ds(0, tps - 1), group_steps(group)]
            settle(arrived, recv_sem.at[HIDDEN + group])
        if group == 0:
            settle(down_w, weight_sem.at[4])
        spread_rows = []
        number = lax.broadcasted_iota(jnp.int32, (wide, pair_slots), 1).astype(jnp.float32)
        for step in groups[group]:
            packed = jnp.concatenate([hidden_all[t, step] for t in range(tps)], 1)
            for at in range(2):
                slot = column(group_at(step, at))
                if at == 1:
                    slot = jnp.where(slot < 0.0, -1.0, slot + slots)
                table = jnp.where(number == slot, 1.0, 0.0).astype(jnp.bfloat16)
                spread_rows.append(dot(table, packed).astype(jnp.bfloat16))
        result = None
        for e in range(experts):
            mine = jnp.concatenate([r[e * rows : (e + 1) * rows] for r in spread_rows], 0)
            term = dot(mine, down_w[e])
            result = term if result is None else result + term
        for i, (step, at) in enumerate(blocks(group)):
            part = result[i * rows : (i + 1) * rows]
            if at == 0:
                total[step] = part
            else:
                pair_out[step] = part.astype(jnp.bfloat16)
        both = group_steps(group)
        push(
            pair_out.at[both],
            pair_in.at[both],
            send_sem.at[9],
            back_sem.at[group],
            partner,
        )

    def return_step(group):
        both = group_steps(group)
        with jax.named_scope("pair_wait"):
            settle(pair_in.at[both], back_sem.at[group])
        for step in groups[group]:
            mine = total[step] + pair_in[step].astype(jnp.float32)
            if step == 0:
                total[step] = mine
                continue
            line_out[step] = mine.astype(jnp.bfloat16)
            push(
                line_out.at[step],
                line_in.at[step],
                send_sem.at[10],
                back_sem.at[steps + step],
                line[step],
            )

    def own_shared():
        settle(shared_w, weight_sem.at[3])
        both = dot(normed[0:rows, :], shared_w[...])
        hidden = silu(both[:, :shared_width]) * both[:, shared_width:]
        late_all[tp, :, 0:shared_width] = hidden.astype(jnp.bfloat16)

    def own_side():
        with jax.named_scope("side_wait"):
            settle(side_in.at[pl.ds(0, eps - 1)], recv_sem.at[SIDE])
        pre = side_out[0].astype(jnp.float32)
        for n in range(1, eps):
            pre = pre + side_in[n].astype(jnp.float32)
        act = silu(pre[:, :side_width]) * pre[:, side_width:]
        act = jnp.concatenate([act, jnp.zeros_like(act)], 1)
        late_all[tp, :, shared_width : shared_width + 2 * side_width] = act.astype(jnp.bfloat16)
        for peer in plane:
            push(late_all.at[tp], late_all.at[tp], send_sem.at[LATE], recv_sem.at[LATE], peer)

    def own_switch():
        settle(side_switch, small_sem.at[5])
        row = side_switch[...].astype(jnp.float32)
        product = normed[0:rows, :].astype(jnp.float32) * row
        logit = jnp.sum(product, 1, keepdims=True)
        return 1.0 / (1.0 + jnp.exp(-logit))

    def own_extra():
        settle(shared_down_w, weight_sem.at[5])
        settle(side_down_w, weight_sem.at[6])
        with jax.named_scope("late_wait"):
            settle(late_all.at[pl.ds(0, tps - 1)], recv_sem.at[LATE])
        shared = jnp.concatenate([late_all[t, :, :shared_width] for t in range(tps)], 1)
        shared = dot(shared, shared_down_w[...])
        side = None
        for t in range(tps):
            mine = late_all[t, :, shared_width : shared_width + side_width]
            term = dot(mine, side_down_w[t * side_width : (t + 1) * side_width, :])
            side = term if side is None else side + term
        return shared + switch * side

    with jax.named_scope("relay0"):
        relay(0)
    with jax.named_scope("spread1"):
        spread(1)
    with jax.named_scope("corner0"):
        corner(0)
    with jax.named_scope("spread2"):
        spread(2)
    with jax.named_scope("relay1"):
        relay(1)
    with jax.named_scope("arrive0"):
        arrive(0)
    with jax.named_scope("norm_step0_0"):
        norm_step(0, 0)
    with jax.named_scope("norm_step0_1"):
        norm_step(0, 1)
    with jax.named_scope("side_step0"):
        side_step(0)
    with jax.named_scope("expert_step0"):
        expert_step(0)
    with jax.named_scope("corner1"):
        corner(1)
    with jax.named_scope("spread3"):
        spread(3)
    with jax.named_scope("relay2"):
        relay(2)
    with jax.named_scope("arrive1"):
        arrive(1)
    with jax.named_scope("norm_step1_0"):
        norm_step(1, 0)
    with jax.named_scope("norm_step1_1"):
        norm_step(1, 1)
    with jax.named_scope("side_step1"):
        side_step(1)
    with jax.named_scope("expert_step1"):
        expert_step(1)
    with jax.named_scope("corner2"):
        corner(2)
    with jax.named_scope("relay3"):
        relay(3)
    with jax.named_scope("arrive2"):
        arrive(2)
    with jax.named_scope("norm_step2_0"):
        norm_step(2, 0)
    with jax.named_scope("norm_step2_1"):
        norm_step(2, 1)
    with jax.named_scope("side_step2"):
        side_step(2)
    with jax.named_scope("expert_step2"):
        expert_step(2)
    with jax.named_scope("corner3"):
        corner(3)
    with jax.named_scope("arrive3"):
        arrive(3)
    with jax.named_scope("norm_step3_0"):
        norm_step(3, 0)
    with jax.named_scope("norm_step3_1"):
        norm_step(3, 1)
    with jax.named_scope("side_step3"):
        side_step(3)
    with jax.named_scope("expert_step3"):
        expert_step(3)
    with jax.named_scope("down_step0"):
        down_step(0)
    with jax.named_scope("down_step1"):
        down_step(1)
    with jax.named_scope("own_shared"):
        own_shared()
    with jax.named_scope("own_switch"):
        switch = own_switch()
    with jax.named_scope("return_step0"):
        return_step(0)
    with jax.named_scope("return_step1"):
        return_step(1)
    with jax.named_scope("down_step2"):
        down_step(2)
    with jax.named_scope("own_side"):
        own_side()
    with jax.named_scope("return_step2"):
        return_step(2)
    with jax.named_scope("down_step3"):
        down_step(3)
    with jax.named_scope("return_step3"):
        return_step(3)
    with jax.named_scope("own_extra"):
        extra = own_extra()

    routed = total[0]
    for step in range(1, steps):
        with jax.named_scope("line_wait"):
            settle(line_in.at[step], back_sem.at[steps + step])
        routed = routed + line_in[step].astype(jnp.float32)
    own = normed[0:rows, own_slice].astype(jnp.float32)
    pre_second = RESIDUAL_SCALE * own + routed + extra
    stats[tp, 0:1, 0:rows] = line_of(jnp.sum(pre_second, 1, keepdims=True))
    stats[tp, 1:2, 0:rows] = line_of(jnp.sum(pre_second * pre_second, 1, keepdims=True))
    for peer in plane:
        push(stats.at[tp], stats.at[tp], send_sem.at[STAT], recv_sem.at[STAT], peer)
    with jax.named_scope("stat_wait"):
        settle(stats.at[pl.ds(0, tps - 1)], recv_sem.at[STAT])
    totals = stats[0]
    for t in range(1, tps):
        totals = totals + stats[t]
    mean = column_of(totals[0:1, 0:rows]) / model
    square = column_of(totals[1:2, 0:rows]) / model
    output[...] = (pre_second - mean) * lax.rsqrt(square - mean * mean + NORM_EPS)
    with jax.named_scope("drain"):
        settle(mixed_all.at[pl.ds(0, tps - 1)], send_sem.at[MIXED])
        settle(route_all.at[pl.ds(0, eps - 1)], send_sem.at[ROUTE])
        settle(weight_all.at[pl.ds(0, eps - 1)], send_sem.at[WEIGHT])
        settle(side_out.at[pl.ds(0, eps - 1)], send_sem.at[SIDE])
        settle(late_all.at[pl.ds(0, tps - 1)], send_sem.at[LATE])
        settle(stats.at[pl.ds(0, tps - 1)], send_sem.at[STAT])
        settle(hidden_all.at[pl.ds(0, tps - 1)], send_sem.at[HIDDEN])
        settle(rows_all.at[pl.ds(0, 5), pl.ds(0, 6)], send_sem.at[7])
        settle(rows_all.at[pl.ds(0, 4)], send_sem.at[8])
        settle(pair_out, send_sem.at[9])
        settle(line_out.at[pl.ds(0, steps - 1)], send_sem.at[10])


def mixer(mixed, tokens, routes, route_weights, first_gain, side_switch, weights):
    out_w, gate_w, up_w, down_w, shared_gate, _, shared_down, side_gate, _, side_down = weights
    eps, tps = lax.axis_size("ep"), lax.axis_size("tp")
    chips = eps // 2
    rows, model = tokens.shape
    cols = model // tps
    experts, _, hidden = gate_w.shape
    top = routes.shape[0]
    total = experts * eps
    capacity = (3 * rows * top + total - 1) // total
    slots = -(-2 * experts * capacity // 16) * 16
    groups = ((0,), (1,), (2,), (3,))
    wide = -(-experts * rows // 128) * 128
    side_width, side_rows = side_gate.shape
    shared = shared_gate.shape[1]
    bf16, f32 = jnp.bfloat16, jnp.float32
    dma = pltpu.SemaphoreType.DMA
    line = pltpu.VMEM((chips, rows, cols), bf16)
    sides = pltpu.VMEM((eps, rows, 2 * side_width), bf16)
    return pl.pallas_call(
        functools.partial(mixer_body, (chips, tps, capacity, groups)),
        out_shape=jax.ShapeDtypeStruct((rows, cols), f32),
        in_specs=[VMEM] + [ANY] * 15,
        out_specs=VMEM,
        scratch_shapes=[
            pltpu.VMEM((rows, cols), bf16),
            pltpu.VMEM(first_gain.shape, f32),
            pltpu.VMEM(side_switch.shape, bf16),
            pltpu.VMEM((tps,) + mixed.shape, bf16),
            pltpu.VMEM((eps, top, rows), jnp.int32),
            pltpu.VMEM((eps, top, rows), f32),
            pltpu.VMEM((eps, 2 * tps, rows, cols // 2), bf16),
            pltpu.VMEM((eps * rows, model), bf16),
            pltpu.VMEM((128, wide), f32),
            pltpu.VMEM((wide, 128), f32),
            pltpu.VMEM((tps, chips, slots, hidden), bf16),
            line,
            line,
            line,
            line,
            pltpu.VMEM((chips, rows, cols), f32),
            sides,
            sides,
            pltpu.VMEM((tps, rows, shared + 2 * side_width), bf16),
            pltpu.VMEM((tps, 8, 128), f32),
            pltpu.VMEM(out_w.shape, bf16),
            pltpu.VMEM((experts, model, 2 * hidden), bf16),
            pltpu.VMEM(down_w.shape, bf16),
            pltpu.VMEM((model, 2 * shared), bf16),
            pltpu.VMEM(shared_down.shape, bf16),
            pltpu.VMEM((2 * side_width, side_rows), bf16),
            pltpu.VMEM(side_down.shape, bf16),
            dma((6,)),
            dma((7,)),
            dma((11,)),
            dma((6 + len(groups),)),
            dma((chips, 6)),
            dma((2 * chips,)),
        ],
        compiler_params=pltpu.CompilerParams(
            collective_id=0, has_side_effects=True, vmem_limit_bytes=54900 * 2**10
        ),
    )(mixed, tokens, routes, route_weights, first_gain, side_switch, *weights)


def streamed_device(
    tokens,
    retention_state,
    lengths,
    query_weight,
    key_weight,
    value_weight,
    gate_weight,
    out_weight,
    first_gain,
    routing,
    route_weight,
    expert_gate,
    expert_up,
    expert_down,
    shared_gate,
    shared_up,
    shared_down,
    side_gate,
    side_up,
    side_down,
    side_switch,
    second_gain,
):
    rows = tokens.shape[0]
    mixed, new_state = retain_kernel(
        tokens,
        lengths.reshape(1, rows),
        [query_weight, key_weight, value_weight, gate_weight],
        retention_state,
    )
    normed = mixer(
        mixed,
        tokens,
        routing.T,
        route_weight.T,
        first_gain.reshape(1, -1),
        side_switch,
        [
            out_weight,
            expert_gate,
            expert_up,
            expert_down,
            shared_gate,
            shared_up,
            shared_down,
            side_gate.T,
            side_up.T,
            side_down,
        ],
    )
    output = (normed * second_gain[None, :]).astype(jnp.bfloat16)
    return (output, new_state)


def staged_device(
    tokens,
    retention_state,
    lengths,
    query_weight,
    key_weight,
    value_weight,
    gate_weight,
    out_weight,
    first_gain,
    routing,
    route_weight,
    expert_gate,
    expert_up,
    expert_down,
    shared_gate,
    shared_up,
    shared_down,
    side_gate,
    side_up,
    side_down,
    side_switch,
    second_gain,
):
    seq_rows = tokens.shape[0]
    model_width = tokens.shape[1]
    head_count = retention_state.shape[1]
    col_count = out_weight.shape[1]
    ep_count = lax.axis_size("ep")
    tp_rank = lax.axis_index("tp")
    ep_rank = lax.axis_index("ep")
    col_start = tp_rank * col_count
    side_width = side_gate.shape[1]
    side_part = jnp.concatenate([side_gate, side_up], 1)
    side_both, every_route, every_weight, *projections = first(
        [side_part, routing.T, route_weight.T],
        tokens,
        [query_weight, key_weight, value_weight, gate_weight],
        0,
    )
    side_both = side_both.reshape(model_width, 2 * side_width)
    mixed_heads, new_state = retain(
        retention_state, lengths, projections, tp_rank * head_count
    )
    (every_mixed,) = gather([mixed_heads], "tp", 1)
    mixing = jnp.dot(
        side_by_side(every_mixed),
        out_weight,
        preferred_element_type=jnp.float32,
    )
    own_cols = lax.dynamic_slice_in_dim(tokens, col_start, col_count, 1).astype(jnp.float32)
    pre_first = RESIDUAL_SCALE * own_cols + mixing
    first_sum, first_square = row_moments(pre_first, 2)
    row_mean = first_sum / model_width
    square = first_square / model_width
    own_gain = lax.dynamic_slice_in_dim(first_gain, col_start, col_count, 0)
    normed_cols = (
        (pre_first - row_mean) * lax.rsqrt(square - row_mean * row_mean + NORM_EPS) * own_gain
    ).astype(jnp.bfloat16)
    every_rows = spread(normed_cols, 3)
    normed_full = lax.dynamic_index_in_dim(every_rows, ep_rank, 0, keepdims=False)
    every_rows = every_rows.reshape(ep_count * seq_rows, model_width)

    local_experts = expert_gate.shape[0]
    top_count = routing.shape[1]
    expert_count = local_experts * ep_count
    capacity = (3 * seq_rows * top_count + expert_count - 1) // expert_count
    total_rows = ep_count * seq_rows
    route_all = jnp.transpose(every_route, (1, 0, 2)).reshape(top_count, total_rows)
    weight_all = jnp.transpose(every_weight, (1, 0, 2)).reshape(top_count, total_rows)
    local_ids = ep_rank * local_experts + jnp.arange(local_experts, dtype=jnp.int32)
    named = route_all[None, :, :] == local_ids[:, None, None]
    member = jnp.any(named, 1)
    pair_weight = jnp.sum(jnp.where(named, weight_all[None, :, :], 0.0), 1)
    index = jnp.arange(total_rows, dtype=jnp.int32)
    group = index // seq_rows
    earlier = ((index[:, None] < index[None, :]) & (group[:, None] == group[None, :])).astype(
        jnp.bfloat16
    )
    before = jnp.dot(
        member.astype(jnp.bfloat16), earlier, preferred_element_type=jnp.float32
    ).astype(jnp.int32)
    slot = jnp.where(member, group[None, :] * capacity + before, -1)
    slot_total = ep_count * capacity
    hit = slot[:, None, :] == jnp.arange(slot_total, dtype=jnp.int32)[None, :, None]
    table = hit.astype(jnp.bfloat16).reshape(local_experts * slot_total, total_rows)
    slot_weight = jnp.sum(jnp.where(hit, pair_weight[:, None, :], 0.0), -1, keepdims=True)
    chosen = (
        jnp.dot(table, every_rows, preferred_element_type=jnp.float32)
        .astype(jnp.bfloat16)
        .reshape(local_experts, slot_total, model_width)
    )
    gate_part = jnp.einsum("jcd,jdf->jcf", chosen, expert_gate, preferred_element_type=jnp.float32)
    up_part = jnp.einsum("jcd,jdf->jcf", chosen, expert_up, preferred_element_type=jnp.float32)
    hidden = (jax.nn.silu(gate_part) * up_part * slot_weight).astype(jnp.bfloat16)

    side_pre = jnp.dot(normed_full, side_both, preferred_element_type=jnp.float32)
    side_hidden = (jax.nn.silu(side_pre[:, :side_width]) * side_pre[:, side_width:]).astype(
        jnp.bfloat16
    )
    shared_hidden = (
        jax.nn.silu(jnp.dot(normed_full, shared_gate, preferred_element_type=jnp.float32))
        * jnp.dot(normed_full, shared_up, preferred_element_type=jnp.float32)
    ).astype(jnp.bfloat16)
    hidden_blocks, shared_blocks, side_blocks = gather(
        [hidden.reshape(local_experts * slot_total, -1), shared_hidden, side_hidden], "tp", 4
    )
    hidden_all = side_by_side(hidden_blocks).reshape(local_experts, slot_total, -1)
    result = (
        jnp.einsum("jcf,jfd->jcd", hidden_all, expert_down, preferred_element_type=jnp.float32)
        .astype(jnp.bfloat16)
        .reshape(local_experts * slot_total, col_count)
    )
    summed = (
        lax.dot_general(
            table, result, (((0,), (0,)), ((), ())), preferred_element_type=jnp.float32
        )
        .astype(jnp.bfloat16)
        .reshape(ep_count, seq_rows, col_count)
    )
    returned = scatter(summed, 5)
    routed = jnp.sum(returned.astype(jnp.float32), 0)
    shared_out = jnp.dot(
        side_by_side(shared_blocks), shared_down, preferred_element_type=jnp.float32
    )
    side_out = jnp.dot(side_by_side(side_blocks), side_down, preferred_element_type=jnp.float32)
    switch = jax.nn.sigmoid(
        jnp.sum(normed_full.astype(jnp.float32) * side_switch.astype(jnp.float32)[None, :], -1)
    )
    pre_second = (
        RESIDUAL_SCALE * normed_cols.astype(jnp.float32)
        + routed
        + shared_out
        + switch[:, None] * side_out
    )
    second_sum, second_square = row_moments(pre_second, 6)
    mean_second = second_sum / model_width
    square_second = second_square / model_width
    output = (
        (pre_second - mean_second)
        * lax.rsqrt(square_second - mean_second * mean_second + NORM_EPS)
        * second_gain
    ).astype(jnp.bfloat16)
    return (output, new_state)


def on_device(*arrays):
    tokens, state, expert_gate, side_gate = arrays[0], arrays[1], arrays[11], arrays[17]
    eps, tps = lax.axis_size("ep"), lax.axis_size("tp")
    rows, model = tokens.shape
    fits = (
        eps == 8
        and tps == 4
        and rows % 16 == 0
        and model % (256 * tps) == 0
        and state.shape[1] * state.shape[2] % 128 == 0
        and expert_gate.shape[2] % 128 == 0
        and side_gate.shape[0] % 128 == 0
        and side_gate.shape[1] == 64
    )
    return (streamed_device if fits else staged_device)(*arrays)


def solution(mesh):
    return jax.shard_map(
        on_device,
        mesh=mesh,
        in_specs=(
            P("ep", None),
            P("ep", "tp", None, None),
            P("ep"),
            P(None, "tp"),
            P(None, "tp"),
            P(None, "tp"),
            P(None, "tp"),
            P(None, "tp"),
            P(),
            P("ep", None),
            P("ep", None),
            P("ep", None, "tp"),
            P("ep", None, "tp"),
            P("ep", None, "tp"),
            P(None, "tp"),
            P(None, "tp"),
            P(None, "tp"),
            P("ep", "tp"),
            P("ep", "tp"),
            P(None, "tp"),
            P(),
            P("tp"),
        ),
        out_specs=(P("ep", "tp"), P("ep", "tp", None, None)),
        check_vma=False,
    )
```

```python
import functools

import jax
import jax.numpy as jnp
from jax import lax
from jax.experimental import pallas as pl
from jax.experimental.pallas import tpu as pltpu
from jax.sharding import PartitionSpec as P

HEADS = 16


RESIDUAL_SCALE = 2.0**0.25
NORM_EPS = 1e-05
GROUP_EPS = 1e-06
ROPE_BASE = 10000.0


def rotate(vector, positions):
    half_width = vector.shape[-1] // 2
    frequency = ROPE_BASE ** (-jnp.arange(half_width, dtype=jnp.float32) / half_width)
    angles = positions.astype(jnp.float32)[:, None, None] * frequency[None, None, :]
    cosine = jnp.cos(angles)
    sine_part = jnp.sin(angles)
    first_half = vector[..., :half_width]
    second_half = vector[..., half_width:]
    return jnp.concatenate(
        [
            first_half * cosine - second_half * sine_part,
            second_half * cosine + first_half * sine_part,
        ],
        -1,
    )


def retain(
    retention_state,
    lengths,
    projections,
    first_head,
):
    row_count = retention_state.shape[0]
    head_count = retention_state.shape[1]
    head_width = retention_state.shape[2]

    query_rows, key_part, value_part, gate_part = [part.astype(jnp.float32) for part in projections]
    queries = rotate(query_rows.reshape(row_count, head_count, head_width), lengths)
    key_rows = rotate(
        key_part.reshape(row_count, head_count, head_width), lengths
    ) * head_width ** (-0.5)
    values = value_part.reshape(row_count, head_count, head_width)
    gate_act = gate_part
    head_index = (first_head + jnp.arange(head_count)).astype(jnp.float32)
    decays = 1.0 - 2.0 ** (-5.0 - 7.0 * head_index / (HEADS - 1))
    own_term = jnp.sum(queries * key_rows, -1, keepdims=True) * values
    carried = decays[None, :, None] * jnp.sum(queries[:, :, :, None] * retention_state, 2)
    result = own_term + carried
    new_state = (
        decays[None, :, None, None] * retention_state
        + key_rows[:, :, :, None] * values[:, :, None, :]
    )
    normed = result * lax.rsqrt(jnp.mean(result * result, -1, keepdims=True) + GROUP_EPS)
    mixed_heads = (
        normed.reshape(row_count, head_count * head_width) * jax.nn.silu(gate_act)
    ).astype(jnp.bfloat16)
    return (mixed_heads, new_state)


VMEM = pl.BlockSpec(memory_space=pltpu.VMEM)
DEVICE = pl.DeviceIdType.MESH


def enter(peers):
    barrier = pltpu.get_barrier_semaphore()
    for peer in peers:
        pl.semaphore_signal(barrier, inc=1, device_id=peer, device_id_type=DEVICE)
    pl.semaphore_wait(barrier, len(peers))


def send(source, target, send_sem, recv_sem, peer):
    copy = pltpu.make_async_remote_copy(
        src_ref=source,
        dst_ref=target,
        send_sem=send_sem,
        recv_sem=recv_sem,
        device_id=peer,
        device_id_type=DEVICE,
    )
    copy.start()
    return copy


def on_axis(axis, index):
    if axis == "ep":
        return (index, lax.axis_index("tp"))
    return (lax.axis_index("ep"), index)


def gather_body(axis, count, parts, *refs):
    sources, targets = refs[:parts], refs[parts : 2 * parts]
    send_sem, recv_sem, local_sem = refs[2 * parts :]
    me = lax.axis_index(axis)
    others = [lax.rem(me + step, count) for step in range(1, count)]
    locals_ = []
    for part in range(parts):
        own = pltpu.make_async_copy(sources[part], targets[part].at[me], local_sem.at[part])
        own.start()
        locals_.append(own)
    enter([on_axis(axis, other) for other in others])
    copies = []
    for step, other in enumerate(others):
        for part in range(parts):
            copies.append(
                send(
                    sources[part],
                    targets[part].at[me],
                    send_sem.at[step, part],
                    recv_sem.at[step, part],
                    on_axis(axis, other),
                )
            )
    for copy in locals_:
        copy.wait()
    for copy in copies:
        copy.wait()


def gather(arrays, axis, ident):
    count, parts = lax.axis_size(axis), len(arrays)
    return pl.pallas_call(
        functools.partial(gather_body, axis, count, parts),
        out_shape=[jax.ShapeDtypeStruct((count,) + a.shape, a.dtype) for a in arrays],
        in_specs=[VMEM] * parts,
        out_specs=[VMEM] * parts,
        scratch_shapes=[
            pltpu.SemaphoreType.DMA((count - 1, parts)),
            pltpu.SemaphoreType.DMA((count - 1, parts)),
            pltpu.SemaphoreType.DMA((parts,)),
        ],
        compiler_params=pltpu.CompilerParams(collective_id=ident, has_side_effects=True),
    )(*arrays)


def scatter_body(count, source, target, send_sem, recv_sem, local_sem):
    me = lax.axis_index("ep")
    others = [lax.rem(me + step, count) for step in range(1, count)]
    own = pltpu.make_async_copy(source.at[me], target.at[me], local_sem)
    own.start()
    enter([on_axis("ep", other) for other in others])
    copies = [
        send(
            source.at[other],
            target.at[me],
            send_sem.at[step],
            recv_sem.at[step],
            on_axis("ep", other),
        )
        for step, other in enumerate(others)
    ]
    own.wait()
    for copy in copies:
        copy.wait()


def scatter(array, ident):
    count = array.shape[0]
    return pl.pallas_call(
        functools.partial(scatter_body, count),
        out_shape=jax.ShapeDtypeStruct(array.shape, array.dtype),
        in_specs=[VMEM],
        out_specs=VMEM,
        scratch_shapes=[
            pltpu.SemaphoreType.DMA((count - 1,)),
            pltpu.SemaphoreType.DMA((count - 1,)),
            pltpu.SemaphoreType.DMA,
        ],
        compiler_params=pltpu.CompilerParams(collective_id=ident, has_side_effects=True),
    )(array)


def first_body(count, *refs):
    parts = 3
    sources, (tokens, *weights) = refs[:parts], refs[parts : parts + 5]
    targets = refs[parts + 5 : 2 * parts + 5]
    results = refs[2 * parts + 5 : 2 * parts + 9]
    send_sem, recv_sem, local_sem = refs[2 * parts + 9 :]
    chips = count // 2
    me = lax.axis_index("ep")
    chip, core = me // 2, lax.rem(me, 2)
    partner = on_axis("ep", chip * 2 + 1 - core)
    line = [lax.rem(chip + step, chips) * 2 + core for step in range(1, chips)]
    senders = [lax.rem(chip + chips - step, chips) * 2 + core for step in range(1, chips)]
    locals_ = []
    for part in range(parts):
        own = pltpu.make_async_copy(sources[part], targets[part].at[me], local_sem.at[part])
        own.start()
        locals_.append(own)
    enter([on_axis("ep", other) for other in line] + [partner])
    direct, copies = [], []
    for step, other in enumerate(line):
        for part in range(parts):
            direct.append(
                send(
                    sources[part],
                    targets[part].at[me],
                    send_sem.at[step, part],
                    recv_sem.at[step, part],
                    on_axis("ep", other),
                )
            )
    for part in range(parts):
        copies.append(
            send(
                sources[part],
                targets[part].at[me],
                send_sem.at[chips - 1, part],
                recv_sem.at[chips - 1, part],
                partner,
            )
        )
    for weight, result in zip(weights, results):
        result[...] = jnp.dot(
            tokens[...], weight[...], preferred_element_type=jnp.float32
        ).astype(result.dtype)
    for step, sender in enumerate(senders):
        for part in range(parts):
            direct[step * parts + part].wait_recv()
            copies.append(
                send(
                    targets[part].at[sender],
                    targets[part].at[sender],
                    send_sem.at[chips + step, part],
                    recv_sem.at[chips + step, part],
                    partner,
                )
            )
    for copy in locals_:
        copy.wait()
    for copy in direct:
        copy.wait_send()
    for copy in copies:
        copy.wait()


def first(arrays, tokens, weights, ident):
    count, parts = lax.axis_size("ep"), len(arrays)
    rows = tokens.shape[0]
    return pl.pallas_call(
        functools.partial(first_body, count),
        out_shape=[jax.ShapeDtypeStruct((count,) + a.shape, a.dtype) for a in arrays]
        + [jax.ShapeDtypeStruct((rows, w.shape[1]), jnp.bfloat16) for w in weights],
        in_specs=[VMEM] * (parts + 5),
        out_specs=[VMEM] * (parts + 4),
        scratch_shapes=[
            pltpu.SemaphoreType.DMA((count - 1, parts)),
            pltpu.SemaphoreType.DMA((count - 1, parts)),
            pltpu.SemaphoreType.DMA((parts,)),
        ],
        compiler_params=pltpu.CompilerParams(collective_id=ident, has_side_effects=True),
    )(*arrays, tokens, *weights)


def spread_body(count, tp_count, source, target, send_sem, recv_sem, local_sem):
    chips, width = count // 2, source.shape[1]
    me, own_tp = lax.axis_index("ep"), lax.axis_index("tp")
    chip, core = me // 2, lax.rem(me, 2)
    partner = (chip * 2 + 1 - core, own_tp)

    def place(row, col):
        return target.at[row, :, pl.ds(pl.multiple_of(col * width, width), width)]

    def chip_at(step):
        return lax.rem(chip + chips + step, chips) * 2 + core

    def tp_at(step):
        return lax.rem(own_tp + tp_count + step, tp_count)

    own = pltpu.make_async_copy(source, place(me, own_tp), local_sem)
    own.start()
    line = [(chip_at(step), own_tp) for step in range(1, chips)]
    plane = [(me, tp_at(step)) for step in range(1, tp_count)]
    enter(line + plane + [partner])

    def pair(line_step, plane_step, to_partner):
        return (
            send_sem.at[to_partner, line_step, plane_step],
            recv_sem.at[to_partner, line_step, plane_step],
        )

    direct, planar, copies = [], {}, []
    for step in range(1, chips):
        direct.append(send(source, place(me, own_tp), *pair(step, 0, 0), line[step - 1]))
    for step in range(1, tp_count):
        planar[(0, step)] = send(source, place(me, own_tp), *pair(0, step, 0), plane[step - 1])
    copies.append(send(source, place(me, own_tp), *pair(0, 0, 1), partner))
    for line_step in range(1, chips):
        direct[line_step - 1].wait_recv()
        block = place(chip_at(-line_step), own_tp)
        for step in range(1, tp_count):
            planar[(line_step, step)] = send(
                block, block, *pair(line_step, step, 0), plane[step - 1]
            )
        copies.append(send(block, block, *pair(line_step, 0, 1), partner))
    for line_step in range(chips):
        for step in range(1, tp_count):
            planar[(line_step, step)].wait_recv()
            block = place(chip_at(-line_step), tp_at(-step))
            copies.append(send(block, block, *pair(line_step, step, 1), partner))
    own.wait()
    for copy in direct:
        copy.wait_send()
    for copy in planar.values():
        copy.wait_send()
    for copy in copies:
        copy.wait()


def spread(block, ident):
    count, tp_count = lax.axis_size("ep"), lax.axis_size("tp")
    rows, width = block.shape
    return pl.pallas_call(
        functools.partial(spread_body, count, tp_count),
        out_shape=jax.ShapeDtypeStruct((count, rows, width * tp_count), block.dtype),
        in_specs=[VMEM],
        out_specs=VMEM,
        scratch_shapes=[
            pltpu.SemaphoreType.DMA((2, count // 2, tp_count)),
            pltpu.SemaphoreType.DMA((2, count // 2, tp_count)),
            pltpu.SemaphoreType.DMA,
        ],
        compiler_params=pltpu.CompilerParams(collective_id=ident, has_side_effects=True),
    )(block)


def side_by_side(gathered):
    return jnp.concatenate([gathered[i] for i in range(gathered.shape[0])], -1)


def row_moments(values, ident):
    sums = jnp.stack([jnp.sum(values, -1), jnp.sum(values * values, -1)])
    (every,) = gather([sums], "tp", ident)
    totals = jnp.sum(every, 0)
    return totals[0][:, None], totals[1][:, None]


ANY = pl.BlockSpec(memory_space=pl.ANY)


def dot(a, b):
    return jnp.dot(a, b, preferred_element_type=jnp.float32)


def silu(x):
    return x / (1.0 + jnp.exp(-x))


def fetch(source, target, sem):
    copy = pltpu.make_async_copy(source, target, sem)
    copy.start()
    return copy


def settle(ref, sem):
    pltpu.make_async_copy(ref, ref, sem).wait()


def on_diagonal(rows):
    row = lax.broadcasted_iota(jnp.int32, (rows, rows), 0)
    return row == lax.broadcasted_iota(jnp.int32, (rows, rows), 1)


def column_of(line):
    return jnp.sum(jnp.where(on_diagonal(line.shape[1]), line, 0.0), 1, keepdims=True)


def line_of(column):
    return jnp.sum(jnp.where(on_diagonal(column.shape[0]), column, 0.0), 0, keepdims=True)


def rotated(x, cosine, sine, half):
    width = x.shape[1]
    lane = lax.broadcasted_iota(jnp.int32, x.shape, 1)
    first = (lane & (2 * half - 1)) < half
    later = pltpu.roll(x, width - half, 1)
    sooner = pltpu.roll(x, half, 1)
    return x * cosine + jnp.where(first, -later, sooner) * sine


def retain_body(
    chunk,
    tokens_in,
    lengths_in,
    query_in,
    key_in,
    value_in,
    gate_in,
    state_in,
    mixed,
    state_out,
    tokens,
    lengths,
    weights,
    state,
    columns,
    query_columns,
    spread_even,
    spread_odd,
    values,
    carried,
    small_sem,
    weight_sem,
    state_sem,
    out_sem,
):
    rows, heads, width = state.shape[0], state.shape[1], state.shape[2]
    total = heads * width
    chunks = rows // chunk
    small = [
        fetch(source, target, small_sem.at[i])
        for i, (source, target) in enumerate(
            [(lengths_in, lengths), (tokens_in, tokens)]
        )
    ]
    for i, source in enumerate([query_in, key_in, value_in, gate_in]):
        fetch(source, weights.at[:, pl.ds(i * total, total)], weight_sem.at[i // 2])

    with jax.named_scope("small_wait"):
        small[0].wait()
    for i in range(chunks):
        piece = pl.ds(i * chunk, chunk)
        fetch(state_in.at[piece], state.at[piece], state_sem.at[i])
    position = column_of(lengths[...].astype(jnp.float32))
    lane = lax.broadcasted_iota(jnp.int32, (1, total), 1) & (width // 2 - 1)
    frequency = jnp.zeros((1, total), jnp.float32)
    for i in range(width // 2):
        frequency = jnp.where(lane == i, ROPE_BASE ** (-i / (width // 2)), frequency)
    angles = position * frequency
    cosine, sine = jnp.cos(angles), jnp.sin(angles)
    first_head = lax.axis_index("tp") * heads
    decays = []
    for head in range(heads):
        index = jnp.full((1, width), first_head + head, jnp.int32).astype(jnp.float32)
        decays.append(1.0 - jnp.exp2(-5.0 - 7.0 * index / (HEADS - 1)))

    def project(i):
        span = pl.ds(2 * i * total, 2 * total)
        with jax.named_scope("weight_wait"):
            settle(weights.at[:, span], weight_sem.at[i])
        both = dot(tokens[...], weights[:, span]).astype(jnp.bfloat16).astype(jnp.float32)
        return both[:, :total], both[:, total:]

    with jax.named_scope("small_wait"):
        small[1].wait()
    query, key = project(0)
    value, gate = project(1)
    lanes = columns.shape[1]

    def flipped(x):
        turned = rotated(x, cosine, sine, width // 2)
        padded = jnp.concatenate([turned, jnp.zeros((lanes - rows, total), jnp.float32)], 0)
        return jnp.transpose(padded)

    query_columns[...] = flipped(query)
    columns[...] = (flipped(key) * width ** (-0.5)).astype(jnp.bfloat16)
    for head in range(heads):
        values[head] = value[:, head * width : (head + 1) * width]

    source_lane = lax.broadcasted_iota(jnp.int32, (lanes, 2 * lanes), 0)
    target_lane = lax.broadcasted_iota(jnp.int32, (lanes, 2 * lanes), 1)
    offset = jnp.where(target_lane >= lanes, 1, 0)
    buffers = [spread_even, spread_odd]

    def widen(i, pair):
        pick = jnp.where(source_lane == offset + (i * chunk + 2 * pair), 1.0, 0.0)
        buffers[i % 2][pair] = dot(columns[...], pick.astype(jnp.bfloat16))

    for pair in range(chunk // 2):
        widen(0, pair)
    for i in range(chunks):
        base = i * chunk
        piece = pl.ds(base, chunk)
        with jax.named_scope("state_wait"):
            pltpu.make_async_copy(state_in.at[piece], state.at[piece], state_sem.at[i]).wait()
        wide = buffers[i % 2]
        for at in range(chunk):
            if i + 1 < chunks and at % 2 == 0:
                widen(i + 1, at // 2)
            if at == chunk // 2:
                part = pl.ds(base, chunk // 2)
                fetch(state.at[part], state_out.at[part], out_sem)
            lane = (at % 2) * lanes
            for head in range(heads):
                low, high = head * width, (head + 1) * width
                q_cols = query_columns[low:high, base + at : base + at + 1]
                k_cols = wide[at // 2, low:high, lane : lane + width]
                v_row = values[head, base + at : base + at + 1, :]
                new = decays[head] * state[base + at, head] + k_cols * v_row
                state[base + at, head] = new
                carried[head, base + at : base + at + 1, :] = jnp.sum(
                    q_cols * new, 0, keepdims=True
                )
        part = pl.ds(base + chunk // 2, chunk // 2)
        fetch(state.at[part], state_out.at[part], out_sem)
    parts = []
    for head in range(heads):
        result = carried[head]
        scale = lax.rsqrt(jnp.mean(result * result, -1, keepdims=True) + GROUP_EPS)
        parts.append(result * scale)
    mixed[...] = (jnp.concatenate(parts, 1) * silu(gate)).astype(mixed.dtype)
    with jax.named_scope("state_drain"):
        settle(state, out_sem)


def retain_kernel(tokens, lengths, weights, state):
    rows, heads, width = state.shape[0], state.shape[1], state.shape[2]
    chunk, lanes = 8, 128
    cols = heads * width
    wide = pltpu.VMEM((chunk // 2, cols, 2 * lanes), jnp.float32)
    return pl.pallas_call(
        functools.partial(retain_body, chunk),
        out_shape=[
            jax.ShapeDtypeStruct((rows, cols), jnp.bfloat16),
            jax.ShapeDtypeStruct(state.shape, state.dtype),
        ],
        in_specs=[ANY] * 7,
        out_specs=[VMEM, ANY],
        compiler_params=pltpu.CompilerParams(vmem_limit_bytes=55200 * 2**10),
        scratch_shapes=[
            pltpu.VMEM(tokens.shape, tokens.dtype),
            pltpu.VMEM(lengths.shape, lengths.dtype),
            pltpu.VMEM((tokens.shape[1], 4 * cols), jnp.bfloat16),
            pltpu.VMEM(state.shape, state.dtype),
            pltpu.VMEM((cols, lanes), jnp.bfloat16),
            pltpu.VMEM((cols, lanes), jnp.float32),
            wide,
            wide,
            pltpu.VMEM((heads, rows, width), jnp.float32),
            pltpu.VMEM((heads, rows, width), jnp.float32),
            pltpu.SemaphoreType.DMA((2,)),
            pltpu.SemaphoreType.DMA((2,)),
            pltpu.SemaphoreType.DMA((rows // chunk,)),
            pltpu.SemaphoreType.DMA,
        ],
    )(tokens, lengths, *weights, state)


def mixer_body(
    dims,
    mixed_in,
    tokens_in,
    routes_in,
    route_weights_in,
    first_gain_in,
    side_switch_in,
    out_in,
    gate_in,
    up_in,
    down_in,
    shared_gate_in,
    shared_up_in,
    shared_down_in,
    side_gate_in,
    side_up_in,
    side_down_in,
    output,
    own_tokens,
    first_gain,
    side_switch,
    mixed_all,
    route_all,
    weight_all,
    rows_all,
    normed,
    info,
    info_cols,
    hidden_all,
    pair_out,
    pair_in,
    line_out,
    line_in,
    total,
    side_out,
    side_in,
    late_all,
    stats,
    out_w,
    gate_up_w,
    down_w,
    shared_w,
    shared_down_w,
    side_w,
    side_down_w,
    small_sem,
    weight_sem,
    send_sem,
    recv_sem,
    row_sem,
    back_sem,
):
    chips, tps, capacity, groups = dims
    steps = chips
    downs = ((0, 1), (2,), (3,))
    rows, cols = own_tokens.shape
    model = cols * tps
    half = cols // 2
    experts, hidden_width = gate_in.shape[0], gate_in.shape[2]
    slots = experts * capacity
    pair_slots = hidden_all.shape[2]
    side_width = side_gate_in.shape[0]
    side_rows = side_gate_in.shape[1]
    shared_width = shared_gate_in.shape[1]
    tp = lax.axis_index("tp")
    ep = lax.axis_index("ep")
    eps = 2 * chips
    chip, core = ep // 2, lax.rem(ep, 2)
    partner = (chip * 2 + 1 - core, tp)
    low, high = lax.rem(tp, 2), tp // 2
    tp_x = high * 2 + 1 - low
    tp_y = (1 - high) * 2 + low
    tp_d = (1 - high) * 2 + 1 - low
    plane = [(ep, tp_x), (ep, tp_y), (ep, tp_d)]

    def chip_at(step):
        if step == 0:
            return chip
        if step == 1:
            return chip + 1 - 2 * lax.rem(chip, 2)
        if step == 2:
            return lax.rem(chip + 2, 4)
        return 3 - chip

    def group_at(step, at):
        return chip_at(step) * 2 + (core if at == 0 else 1 - core)

    line = [(group_at(step, 0), tp) for step in range(steps)]
    others = [(group_at(s, at), tp) for s in range(steps) for at in range(2) if s + at > 0]
    peers = plane + others
    barrier = pltpu.get_barrier_semaphore()
    for peer in peers:
        pl.semaphore_signal(barrier, inc=1, device_id=peer, device_id_type=DEVICE)

    own_mixed = mixed_all.at[tp]
    own_slice = pl.ds(pl.multiple_of(tp * cols, cols), cols)
    fetch(routes_in, route_all.at[ep], small_sem.at[1])
    fetch(route_weights_in, weight_all.at[ep], small_sem.at[2])
    fetch(tokens_in.at[:, own_slice], own_tokens, small_sem.at[3])
    fetch(out_in, out_w, weight_sem.at[0])
    MIXED, ROUTE, WEIGHT, SIDE, LATE, STAT, HIDDEN = 0, 1, 2, 3, 4, 5, 6

    def push(source, target, sent, received, peer):
        send(source, target, sent, received, peer)

    with jax.named_scope("small_wait"):
        settle(route_all.at[ep], small_sem.at[1])
        settle(weight_all.at[ep], small_sem.at[2])
    fetch(first_gain_in, first_gain, small_sem.at[4])
    fetch(side_switch_in, side_switch, small_sem.at[5])
    for e in range(experts):
        fetch(gate_in.at[e], gate_up_w.at[e, :, pl.ds(0, hidden_width)], weight_sem.at[1])
        fetch(up_in.at[e], gate_up_w.at[e, :, pl.ds(hidden_width, hidden_width)], weight_sem.at[1])
    fetch(side_gate_in, side_w.at[pl.ds(0, side_width)], weight_sem.at[2])
    fetch(side_up_in, side_w.at[pl.ds(side_width, side_width)], weight_sem.at[2])
    fetch(shared_gate_in, shared_w.at[:, pl.ds(0, shared_width)], weight_sem.at[3])
    fetch(shared_up_in, shared_w.at[:, pl.ds(shared_width, shared_width)], weight_sem.at[3])
    fetch(down_in, down_w, weight_sem.at[4])
    fetch(shared_down_in, shared_down_w, weight_sem.at[5])
    fetch(side_down_in, side_down_w, weight_sem.at[6])
    with jax.named_scope("enter"):
        pl.semaphore_wait(barrier, len(peers))

    for peer in plane:
        push(mixed_in, own_mixed, send_sem.at[MIXED], recv_sem.at[MIXED], peer)
    for peer in others:
        own = route_all.at[ep]
        push(own, own, send_sem.at[ROUTE], recv_sem.at[ROUTE], peer)
        own = weight_all.at[ep]
        push(own, own, send_sem.at[WEIGHT], recv_sem.at[WEIGHT], peer)

    mixed_all[tp] = mixed_in[...]
    with jax.named_scope("out_wait"):
        settle(own_tokens, small_sem.at[3])
        settle(out_w, weight_sem.at[0])
    with jax.named_scope("mixed_wait"):
        settle(mixed_all.at[pl.ds(0, tps - 1)], recv_sem.at[MIXED])
    heads_all = jnp.concatenate([mixed_all[t] for t in range(tps)], 1)
    pre_first = RESIDUAL_SCALE * own_tokens[...].astype(jnp.float32) + dot(heads_all, out_w[...])
    for part in range(2):
        rows_all[ep, 2 * tp + part] = pre_first[:, part * half : (part + 1) * half].astype(
            jnp.bfloat16
        )

    def block(step, index):
        return rows_all.at[group_at(step, 0), pl.ds(2 * index, 2)]

    def piece(step, index, part):
        return rows_all.at[group_at(step, 0), 2 * index + part]

    def push_rows(ref, step, kind, peer):
        sent = send_sem.at[8] if kind == 5 else send_sem.at[7]
        push(ref, ref, sent, row_sem.at[step, kind], peer)

    def came(ref, step, kind):
        settle(ref, row_sem.at[step, kind])

    def spread(step):
        ref = block(step, tp)
        if step > 0:
            came(ref, step, 0)
        for i, peer in enumerate(plane):
            push_rows(ref, step, 1 + i, peer)
        push_rows(ref, step, 5, partner)

    def relay(step):
        for i, index in enumerate([tp_x, tp_y]):
            came(block(step, index), step, 1 + i)
            push_rows(block(step, index), step, 5, partner)

    def corner(step):
        came(block(step, tp_d), step, 3)
        push_rows(block(step, tp_d), step, 5, partner)

    def arrive(step):
        came(rows_all.at[group_at(step, 1)], step, 5)

    with jax.named_scope("spread0"):
        spread(0)
        for step in range(1, steps):
            push_rows_to = line[step]
            push(block(0, tp), block(0, tp), send_sem.at[7], row_sem.at[step, 0], push_rows_to)

    with jax.named_scope("route_wait"):
        settle(route_all.at[pl.ds(0, eps - 1)], recv_sem.at[ROUTE])
        settle(weight_all.at[pl.ds(0, eps - 1)], recv_sem.at[WEIGHT])
    wide = experts * rows

    def expert_of(index):
        return sum(jnp.where(index >= e * rows, 1, 0) for e in range(1, experts))

    group_lane = expert_of(lax.broadcasted_iota(jnp.int32, (1, wide), 1))
    expert_lane = ep * experts + group_lane
    info[...] = jnp.zeros_like(info)
    for g in range(eps):
        ids = jnp.concatenate([route_all[g]] * experts, 1)
        hits = ids == expert_lane
        scales = jnp.concatenate([weight_all[g]] * experts, 1)
        info[g : g + 1, 0:wide] = jnp.sum(jnp.where(hits, 1.0, 0.0), 0, keepdims=True)
        info[eps + g : eps + g + 1, 0:wide] = jnp.sum(
            jnp.where(hits, scales, 0.0), 0, keepdims=True
        )
    member = info[0:eps, 0:wide]
    sooner = lax.broadcasted_iota(jnp.int32, (wide, wide), 0)
    later = lax.broadcasted_iota(jnp.int32, (wide, wide), 1)
    earlier = jnp.where(
        (sooner < later) & (expert_of(sooner) == expert_of(later)), 1.0, 0.0
    ).astype(jnp.bfloat16)
    before = dot(member.astype(jnp.bfloat16), earlier)
    start = (group_lane * capacity).astype(jnp.float32)
    info[0:eps, 0:wide] = jnp.where(member > 0.5, before + start, -1.0)
    info_cols[...] = jnp.transpose(info[...])
    settle(first_gain, small_sem.at[4])

    def column(index):
        lane = lax.broadcasted_iota(jnp.int32, (wide, info_cols.shape[1]), 1)
        picked = jnp.where(lane == index, info_cols[0:wide, :], 0.0)
        return jnp.sum(picked, 1, keepdims=True)

    side_span = pl.ds(pl.multiple_of(ep * side_rows, side_rows), side_rows)

    def blocks(group):
        return [(step, at) for step in groups[group] for at in range(2)]

    def group_rows(group):
        return slice(2 * groups[group][0] * rows, 2 * (groups[group][-1] + 1) * rows)

    def group_steps(group):
        return pl.ds(groups[group][0], len(groups[group]))

    def norm_step(step, at):
        g, base = group_at(step, at), (2 * step + at) * rows
        sums = jnp.zeros((rows, half), jnp.float32)
        squares = jnp.zeros((rows, half), jnp.float32)
        for part in range(2 * tps):
            x = rows_all[g, part].astype(jnp.float32)
            sums = sums + x
            squares = squares + x * x
        mean = jnp.sum(sums, 1, keepdims=True) / model
        square = jnp.sum(squares, 1, keepdims=True) / model
        scale = lax.rsqrt(square - mean * mean + NORM_EPS)
        for part in range(2 * tps):
            span = slice(part * half, (part + 1) * half)
            x = rows_all[g, part].astype(jnp.float32)
            y = (x - mean) * scale * first_gain[:, span]
            normed[base : base + rows, span] = y.astype(jnp.bfloat16)

    def side_step(group):
        if group == 0:
            settle(side_w, weight_sem.at[2])
        partial = lax.dot_general(
            normed[group_rows(group), side_span],
            side_w[...],
            (((1,), (1,)), ((), ())),
            preferred_element_type=jnp.float32,
        ).astype(jnp.bfloat16)
        for i, (step, at) in enumerate(blocks(group)):
            n = 2 * step + at
            side_out[n] = partial[i * rows : (i + 1) * rows]
            if n > 0:
                peer = (group_at(step, at), tp)
                push(
                    side_out.at[n],
                    side_in.at[n],
                    send_sem.at[SIDE],
                    recv_sem.at[SIDE],
                    peer,
                )

    def expert_step(group):
        if group == 0:
            settle(gate_up_w, weight_sem.at[1])
        members = blocks(group)
        stacks = [[] for _ in members]
        scales = [column(eps + group_at(step, at)) for step, at in members]
        for e in range(experts):
            both = dot(normed[group_rows(group), :], gate_up_w[e])
            hidden = silu(both[:, :hidden_width]) * both[:, hidden_width:]
            for i in range(len(members)):
                mine = hidden[i * rows : (i + 1) * rows] * scales[i][e * rows : (e + 1) * rows]
                stacks[i].append(mine.astype(jnp.bfloat16))
        number = lax.broadcasted_iota(jnp.int32, (pair_slots, 2 * wide), 0).astype(jnp.float32)
        for i, step in enumerate(groups[group]):
            near = info[pl.ds(group_at(step, 0), 1), 0:wide]
            far = info[pl.ds(group_at(step, 1), 1), 0:wide]
            far = jnp.where(far < 0.0, -1.0, far + slots)
            slot_row = jnp.concatenate([near, far], 1)
            table = jnp.where(number == slot_row, 1.0, 0.0).astype(jnp.bfloat16)
            stack = jnp.concatenate(stacks[2 * i] + stacks[2 * i + 1], 0)
            hidden_all[tp, step] = dot(table, stack).astype(jnp.bfloat16)
        own = hidden_all.at[tp, group_steps(group)]
        for peer in plane:
            push(own, own, send_sem.at[HIDDEN], recv_sem.at[HIDDEN + group], peer)

    def down_step(index):
        members = [(step, at) for step in downs[index] for at in range(2)]
        both = pl.ds(downs[index][0], len(downs[index]))
        with jax.named_scope("hidden_wait"):
            for step in downs[index]:
                arrived = hidden_all.at[pl.ds(0, tps - 1), group_steps(step)]
                settle(arrived, recv_sem.at[HIDDEN + step])
        if index == 0:
            settle(down_w, weight_sem.at[4])
        spread_rows = []
        number = lax.broadcasted_iota(jnp.int32, (wide, pair_slots), 1).astype(jnp.float32)
        for step in downs[index]:
            packed = jnp.concatenate([hidden_all[t, step] for t in range(tps)], 1)
            for at in range(2):
                slot = column(group_at(step, at))
                if at == 1:
                    slot = jnp.where(slot < 0.0, -1.0, slot + slots)
                table = jnp.where(number == slot, 1.0, 0.0).astype(jnp.bfloat16)
                spread_rows.append(dot(table, packed).astype(jnp.bfloat16))
        result = None
        for e in range(experts):
            mine = jnp.concatenate([r[e * rows : (e + 1) * rows] for r in spread_rows], 0)
            term = dot(mine, down_w[e])
            result = term if result is None else result + term
        for i, (step, at) in enumerate(members):
            part = result[i * rows : (i + 1) * rows]
            if at == 0:
                total[step] = part
            else:
                pair_out[step] = part.astype(jnp.bfloat16)
        push(
            pair_out.at[both],
            pair_in.at[both],
            send_sem.at[9],
            back_sem.at[index],
            partner,
        )

    def return_step(index):
        both = pl.ds(downs[index][0], len(downs[index]))
        with jax.named_scope("pair_wait"):
            settle(pair_in.at[both], back_sem.at[index])
        for step in downs[index]:
            mine = total[step] + pair_in[step].astype(jnp.float32)
            if step == 0:
                total[step] = mine
                continue
            line_out[step] = mine.astype(jnp.bfloat16)
            push(
                line_out.at[step],
                line_in.at[step],
                send_sem.at[10],
                back_sem.at[steps + step],
                line[step],
            )

    def own_shared():
        settle(shared_w, weight_sem.at[3])
        both = dot(normed[0:rows, :], shared_w[...])
        hidden = silu(both[:, :shared_width]) * both[:, shared_width:]
        late_all[tp, :, 0:shared_width] = hidden.astype(jnp.bfloat16)

    def own_side():
        with jax.named_scope("side_wait"):
            settle(side_in.at[pl.ds(0, eps - 1)], recv_sem.at[SIDE])
        pre = side_out[0].astype(jnp.float32)
        for n in range(1, eps):
            pre = pre + side_in[n].astype(jnp.float32)
        act = silu(pre[:, :side_width]) * pre[:, side_width:]
        act = jnp.concatenate([act, jnp.zeros_like(act)], 1)
        late_all[tp, :, shared_width : shared_width + 2 * side_width] = act.astype(jnp.bfloat16)
        for peer in plane:
            push(late_all.at[tp], late_all.at[tp], send_sem.at[LATE], recv_sem.at[LATE], peer)

    def own_switch():
        settle(side_switch, small_sem.at[5])
        row = side_switch[...].astype(jnp.float32)
        product = normed[0:rows, :].astype(jnp.float32) * row
        logit = jnp.sum(product, 1, keepdims=True)
        return 1.0 / (1.0 + jnp.exp(-logit))

    def own_extra():
        settle(shared_down_w, weight_sem.at[5])
        settle(side_down_w, weight_sem.at[6])
        with jax.named_scope("late_wait"):
            settle(late_all.at[pl.ds(0, tps - 1)], recv_sem.at[LATE])
        shared = jnp.concatenate([late_all[t, :, :shared_width] for t in range(tps)], 1)
        shared = dot(shared, shared_down_w[...])
        side = None
        for t in range(tps):
            mine = late_all[t, :, shared_width : shared_width + side_width]
            term = dot(mine, side_down_w[t * side_width : (t + 1) * side_width, :])
            side = term if side is None else side + term
        return shared + switch * side

    with jax.named_scope("relay0"):
        relay(0)
    with jax.named_scope("spread1"):
        spread(1)
    with jax.named_scope("corner0"):
        corner(0)
    with jax.named_scope("spread2"):
        spread(2)
    with jax.named_scope("relay1"):
        relay(1)
    with jax.named_scope("arrive0"):
        arrive(0)
    with jax.named_scope("norm_step0_0"):
        norm_step(0, 0)
    with jax.named_scope("norm_step0_1"):
        norm_step(0, 1)
    with jax.named_scope("side_step0"):
        side_step(0)
    with jax.named_scope("expert_step0"):
        expert_step(0)
    with jax.named_scope("corner1"):
        corner(1)
    with jax.named_scope("spread3"):
        spread(3)
    with jax.named_scope("relay2"):
        relay(2)
    with jax.named_scope("arrive1"):
        arrive(1)
    with jax.named_scope("norm_step1_0"):
        norm_step(1, 0)
    with jax.named_scope("norm_step1_1"):
        norm_step(1, 1)
    with jax.named_scope("side_step1"):
        side_step(1)
    with jax.named_scope("expert_step1"):
        expert_step(1)
    with jax.named_scope("corner2"):
        corner(2)
    with jax.named_scope("own_shared"):
        own_shared()
    with jax.named_scope("own_switch"):
        switch = own_switch()
    with jax.named_scope("relay3"):
        relay(3)
    with jax.named_scope("arrive2"):
        arrive(2)
    with jax.named_scope("norm_step2_0"):
        norm_step(2, 0)
    with jax.named_scope("norm_step2_1"):
        norm_step(2, 1)
    with jax.named_scope("side_step2"):
        side_step(2)
    with jax.named_scope("expert_step2"):
        expert_step(2)
    with jax.named_scope("corner3"):
        corner(3)
    with jax.named_scope("arrive3"):
        arrive(3)
    with jax.named_scope("norm_step3_0"):
        norm_step(3, 0)
    with jax.named_scope("norm_step3_1"):
        norm_step(3, 1)
    with jax.named_scope("side_step3"):
        side_step(3)
    with jax.named_scope("expert_step3"):
        expert_step(3)
    with jax.named_scope("down_step0"):
        down_step(0)
    with jax.named_scope("return_step0"):
        return_step(0)
    with jax.named_scope("down_step1"):
        down_step(1)
    with jax.named_scope("own_side"):
        own_side()
    with jax.named_scope("down_step2"):
        down_step(2)
    with jax.named_scope("return_step1"):
        return_step(1)
    with jax.named_scope("return_step2"):
        return_step(2)
    with jax.named_scope("own_extra"):
        extra = own_extra()

    routed = total[0]
    for step in range(1, steps):
        with jax.named_scope("line_wait"):
            settle(line_in.at[step], back_sem.at[steps + step])
        routed = routed + line_in[step].astype(jnp.float32)
    own = normed[0:rows, own_slice].astype(jnp.float32)
    pre_second = RESIDUAL_SCALE * own + routed + extra
    stats[tp, 0:1, 0:rows] = line_of(jnp.sum(pre_second, 1, keepdims=True))
    stats[tp, 1:2, 0:rows] = line_of(jnp.sum(pre_second * pre_second, 1, keepdims=True))
    for peer in plane:
        push(stats.at[tp], stats.at[tp], send_sem.at[STAT], recv_sem.at[STAT], peer)
    with jax.named_scope("stat_wait"):
        settle(stats.at[pl.ds(0, tps - 1)], recv_sem.at[STAT])
    totals = stats[0]
    for t in range(1, tps):
        totals = totals + stats[t]
    mean = column_of(totals[0:1, 0:rows]) / model
    square = column_of(totals[1:2, 0:rows]) / model
    output[...] = (pre_second - mean) * lax.rsqrt(square - mean * mean + NORM_EPS)
    with jax.named_scope("drain"):
        settle(mixed_all.at[pl.ds(0, tps - 1)], send_sem.at[MIXED])
        settle(route_all.at[pl.ds(0, eps - 1)], send_sem.at[ROUTE])
        settle(weight_all.at[pl.ds(0, eps - 1)], send_sem.at[WEIGHT])
        settle(side_out.at[pl.ds(0, eps - 1)], send_sem.at[SIDE])
        settle(late_all.at[pl.ds(0, tps - 1)], send_sem.at[LATE])
        settle(stats.at[pl.ds(0, tps - 1)], send_sem.at[STAT])
        settle(hidden_all.at[pl.ds(0, tps - 1)], send_sem.at[HIDDEN])
        settle(rows_all.at[pl.ds(0, 5), pl.ds(0, 6)], send_sem.at[7])
        settle(rows_all.at[pl.ds(0, 4)], send_sem.at[8])
        settle(pair_out, send_sem.at[9])
        settle(line_out.at[pl.ds(0, steps - 1)], send_sem.at[10])


def mixer(mixed, tokens, routes, route_weights, first_gain, side_switch, weights):
    out_w, gate_w, up_w, down_w, shared_gate, _, shared_down, side_gate, _, side_down = weights
    eps, tps = lax.axis_size("ep"), lax.axis_size("tp")
    chips = eps // 2
    rows, model = tokens.shape
    cols = model // tps
    experts, _, hidden = gate_w.shape
    top = routes.shape[0]
    total = experts * eps
    capacity = (3 * rows * top + total - 1) // total
    slots = -(-2 * experts * capacity // 16) * 16
    groups = ((0,), (1,), (2,), (3,))
    wide = -(-experts * rows // 128) * 128
    side_width, side_rows = side_gate.shape
    shared = shared_gate.shape[1]
    bf16, f32 = jnp.bfloat16, jnp.float32
    dma = pltpu.SemaphoreType.DMA
    line = pltpu.VMEM((chips, rows, cols), bf16)
    sides = pltpu.VMEM((eps, rows, 2 * side_width), bf16)
    return pl.pallas_call(
        functools.partial(mixer_body, (chips, tps, capacity, groups)),
        out_shape=jax.ShapeDtypeStruct((rows, cols), f32),
        in_specs=[VMEM] + [ANY] * 15,
        out_specs=VMEM,
        scratch_shapes=[
            pltpu.VMEM((rows, cols), bf16),
            pltpu.VMEM(first_gain.shape, f32),
            pltpu.VMEM(side_switch.shape, bf16),
            pltpu.VMEM((tps,) + mixed.shape, bf16),
            pltpu.VMEM((eps, top, rows), jnp.int32),
            pltpu.VMEM((eps, top, rows), f32),
            pltpu.VMEM((eps, 2 * tps, rows, cols // 2), bf16),
            pltpu.VMEM((eps * rows, model), bf16),
            pltpu.VMEM((128, wide), f32),
            pltpu.VMEM((wide, 128), f32),
            pltpu.VMEM((tps, chips, slots, hidden), bf16),
            line,
            line,
            line,
            line,
            pltpu.VMEM((chips, rows, cols), f32),
            sides,
            sides,
            pltpu.VMEM((tps, rows, shared + 2 * side_width), bf16),
            pltpu.VMEM((tps, 8, 128), f32),
            pltpu.VMEM(out_w.shape, bf16),
            pltpu.VMEM((experts, model, 2 * hidden), bf16),
            pltpu.VMEM(down_w.shape, bf16),
            pltpu.VMEM((model, 2 * shared), bf16),
            pltpu.VMEM(shared_down.shape, bf16),
            pltpu.VMEM((2 * side_width, side_rows), bf16),
            pltpu.VMEM(side_down.shape, bf16),
            dma((6,)),
            dma((7,)),
            dma((11,)),
            dma((6 + len(groups),)),
            dma((chips, 6)),
            dma((2 * chips,)),
        ],
        compiler_params=pltpu.CompilerParams(
            collective_id=0, has_side_effects=True, vmem_limit_bytes=54900 * 2**10
        ),
    )(mixed, tokens, routes, route_weights, first_gain, side_switch, *weights)


def streamed_device(
    tokens,
    retention_state,
    lengths,
    query_weight,
    key_weight,
    value_weight,
    gate_weight,
    out_weight,
    first_gain,
    routing,
    route_weight,
    expert_gate,
    expert_up,
    expert_down,
    shared_gate,
    shared_up,
    shared_down,
    side_gate,
    side_up,
    side_down,
    side_switch,
    second_gain,
):
    rows = tokens.shape[0]
    mixed, new_state = retain_kernel(
        tokens,
        lengths.reshape(1, rows),
        [query_weight, key_weight, value_weight, gate_weight],
        retention_state,
    )
    normed = mixer(
        mixed,
        tokens,
        routing.T,
        route_weight.T,
        first_gain.reshape(1, -1),
        side_switch,
        [
            out_weight,
            expert_gate,
            expert_up,
            expert_down,
            shared_gate,
            shared_up,
            shared_down,
            side_gate.T,
            side_up.T,
            side_down,
        ],
    )
    output = (normed * second_gain[None, :]).astype(jnp.bfloat16)
    return (output, new_state)


def staged_device(
    tokens,
    retention_state,
    lengths,
    query_weight,
    key_weight,
    value_weight,
    gate_weight,
    out_weight,
    first_gain,
    routing,
    route_weight,
    expert_gate,
    expert_up,
    expert_down,
    shared_gate,
    shared_up,
    shared_down,
    side_gate,
    side_up,
    side_down,
    side_switch,
    second_gain,
):
    seq_rows = tokens.shape[0]
    model_width = tokens.shape[1]
    head_count = retention_state.shape[1]
    col_count = out_weight.shape[1]
    ep_count = lax.axis_size("ep")
    tp_rank = lax.axis_index("tp")
    ep_rank = lax.axis_index("ep")
    col_start = tp_rank * col_count
    side_width = side_gate.shape[1]
    side_part = jnp.concatenate([side_gate, side_up], 1)
    side_both, every_route, every_weight, *projections = first(
        [side_part, routing.T, route_weight.T],
        tokens,
        [query_weight, key_weight, value_weight, gate_weight],
        0,
    )
    side_both = side_both.reshape(model_width, 2 * side_width)
    mixed_heads, new_state = retain(
        retention_state, lengths, projections, tp_rank * head_count
    )
    (every_mixed,) = gather([mixed_heads], "tp", 1)
    mixing = jnp.dot(
        side_by_side(every_mixed),
        out_weight,
        preferred_element_type=jnp.float32,
    )
    own_cols = lax.dynamic_slice_in_dim(tokens, col_start, col_count, 1).astype(jnp.float32)
    pre_first = RESIDUAL_SCALE * own_cols + mixing
    first_sum, first_square = row_moments(pre_first, 2)
    row_mean = first_sum / model_width
    square = first_square / model_width
    own_gain = lax.dynamic_slice_in_dim(first_gain, col_start, col_count, 0)
    normed_cols = (
        (pre_first - row_mean) * lax.rsqrt(square - row_mean * row_mean + NORM_EPS) * own_gain
    ).astype(jnp.bfloat16)
    every_rows = spread(normed_cols, 3)
    normed_full = lax.dynamic_index_in_dim(every_rows, ep_rank, 0, keepdims=False)
    every_rows = every_rows.reshape(ep_count * seq_rows, model_width)

    local_experts = expert_gate.shape[0]
    top_count = routing.shape[1]
    expert_count = local_experts * ep_count
    capacity = (3 * seq_rows * top_count + expert_count - 1) // expert_count
    total_rows = ep_count * seq_rows
    route_all = jnp.transpose(every_route, (1, 0, 2)).reshape(top_count, total_rows)
    weight_all = jnp.transpose(every_weight, (1, 0, 2)).reshape(top_count, total_rows)
    local_ids = ep_rank * local_experts + jnp.arange(local_experts, dtype=jnp.int32)
    named = route_all[None, :, :] == local_ids[:, None, None]
    member = jnp.any(named, 1)
    pair_weight = jnp.sum(jnp.where(named, weight_all[None, :, :], 0.0), 1)
    index = jnp.arange(total_rows, dtype=jnp.int32)
    group = index // seq_rows
    earlier = ((index[:, None] < index[None, :]) & (group[:, None] == group[None, :])).astype(
        jnp.bfloat16
    )
    before = jnp.dot(
        member.astype(jnp.bfloat16), earlier, preferred_element_type=jnp.float32
    ).astype(jnp.int32)
    slot = jnp.where(member, group[None, :] * capacity + before, -1)
    slot_total = ep_count * capacity
    hit = slot[:, None, :] == jnp.arange(slot_total, dtype=jnp.int32)[None, :, None]
    table = hit.astype(jnp.bfloat16).reshape(local_experts * slot_total, total_rows)
    slot_weight = jnp.sum(jnp.where(hit, pair_weight[:, None, :], 0.0), -1, keepdims=True)
    chosen = (
        jnp.dot(table, every_rows, preferred_element_type=jnp.float32)
        .astype(jnp.bfloat16)
        .reshape(local_experts, slot_total, model_width)
    )
    gate_part = jnp.einsum("jcd,jdf->jcf", chosen, expert_gate, preferred_element_type=jnp.float32)
    up_part = jnp.einsum("jcd,jdf->jcf", chosen, expert_up, preferred_element_type=jnp.float32)
    hidden = (jax.nn.silu(gate_part) * up_part * slot_weight).astype(jnp.bfloat16)

    side_pre = jnp.dot(normed_full, side_both, preferred_element_type=jnp.float32)
    side_hidden = (jax.nn.silu(side_pre[:, :side_width]) * side_pre[:, side_width:]).astype(
        jnp.bfloat16
    )
    shared_hidden = (
        jax.nn.silu(jnp.dot(normed_full, shared_gate, preferred_element_type=jnp.float32))
        * jnp.dot(normed_full, shared_up, preferred_element_type=jnp.float32)
    ).astype(jnp.bfloat16)
    hidden_blocks, shared_blocks, side_blocks = gather(
        [hidden.reshape(local_experts * slot_total, -1), shared_hidden, side_hidden], "tp", 4
    )
    hidden_all = side_by_side(hidden_blocks).reshape(local_experts, slot_total, -1)
    result = (
        jnp.einsum("jcf,jfd->jcd", hidden_all, expert_down, preferred_element_type=jnp.float32)
        .astype(jnp.bfloat16)
        .reshape(local_experts * slot_total, col_count)
    )
    summed = (
        lax.dot_general(
            table, result, (((0,), (0,)), ((), ())), preferred_element_type=jnp.float32
        )
        .astype(jnp.bfloat16)
        .reshape(ep_count, seq_rows, col_count)
    )
    returned = scatter(summed, 5)
    routed = jnp.sum(returned.astype(jnp.float32), 0)
    shared_out = jnp.dot(
        side_by_side(shared_blocks), shared_down, preferred_element_type=jnp.float32
    )
    side_out = jnp.dot(side_by_side(side_blocks), side_down, preferred_element_type=jnp.float32)
    switch = jax.nn.sigmoid(
        jnp.sum(normed_full.astype(jnp.float32) * side_switch.astype(jnp.float32)[None, :], -1)
    )
    pre_second = (
        RESIDUAL_SCALE * normed_cols.astype(jnp.float32)
        + routed
        + shared_out
        + switch[:, None] * side_out
    )
    second_sum, second_square = row_moments(pre_second, 6)
    mean_second = second_sum / model_width
    square_second = second_square / model_width
    output = (
        (pre_second - mean_second)
        * lax.rsqrt(square_second - mean_second * mean_second + NORM_EPS)
        * second_gain
    ).astype(jnp.bfloat16)
    return (output, new_state)


def on_device(*arrays):
    tokens, state, expert_gate, side_gate = arrays[0], arrays[1], arrays[11], arrays[17]
    eps, tps = lax.axis_size("ep"), lax.axis_size("tp")
    rows, model = tokens.shape
    fits = (
        eps == 8
        and tps == 4
        and rows % 16 == 0
        and model % (256 * tps) == 0
        and state.shape[1] * state.shape[2] % 128 == 0
        and expert_gate.shape[2] % 128 == 0
        and side_gate.shape[0] % 128 == 0
        and side_gate.shape[1] == 64
    )
    return (streamed_device if fits else staged_device)(*arrays)


def solution(mesh):
    return jax.shard_map(
        on_device,
        mesh=mesh,
        in_specs=(
            P("ep", None),
            P("ep", "tp", None, None),
            P("ep"),
            P(None, "tp"),
            P(None, "tp"),
            P(None, "tp"),
            P(None, "tp"),
            P(None, "tp"),
            P(),
            P("ep", None),
            P("ep", None),
            P("ep", None, "tp"),
            P("ep", None, "tp"),
            P("ep", None, "tp"),
            P(None, "tp"),
            P(None, "tp"),
            P(None, "tp"),
            P("ep", "tp"),
            P("ep", "tp"),
            P(None, "tp"),
            P(),
            P("tp"),
        ),
        out_specs=(P("ep", "tp"), P("ep", "tp", None, None)),
        check_vma=False,
    )
```
